32 devices in a mesh: grp: 2 (over y), fs: 4 (over z), tp: 4 (over x, core).
Axes of the slice: x: 2, y: 2, z: 4, core: 2. Of those that a mesh axis runs over, the one named last changes fastest.
Arguments:
- tokens: bfloat16 [3072, 2048], P(('grp', 'fs')), parts along dimension 0, may hold values from -3 to 3
- gate_weight: bfloat16 [2048, 5120], P('fs', 'tp'), may hold values from -0.125 to 0.125
- up_weight: bfloat16 [2048, 5120], P('fs', 'tp'), may hold values from -0.125 to 0.125
- down_weight: bfloat16 [5120, 2048], P('tp', 'fs'), may hold values from -0.078125 to 0.078125
- pool_weight: bfloat16 [512, 4, 512], P('fs', None, 'tp'), may hold values from -0.375 to 0.375
- pool_bias: float32 [4, 512], replicated, may hold values from -3 to 3
- pool_scale: float32 [2048], replicated, may hold values from 0.1 to 1.9
- gain_first: float32 [2048], replicated, may hold values from 0.1 to 1.9
- gain_mix: float32 [2048], replicated, may hold values from 0.1 to 1.9
- gain_second: float32 [2048], replicated, may hold values from 0.1 to 1.9
Outputs:
- result: bfloat16 [3072, 2048], P(('grp', 'fs')), parts along dimension 0
The draws below stay inside these ranges and needn't reach their ends.
There are 2 independent parts, one for each index of `grp`. The reference program is written for one: setup_inputs(seed, part) draws one part's arguments, and reference() takes and returns one part's arrays. A program takes and returns all parts, laid end to end along the dimension named above; an argument that names none is the same for every part. Nothing has to cross between parts.
All inputs are finite; a program needn't handle non-finite values.
Results may differ from the reference program's by a relative error of at most 0.018.
Values may be sent and summed in bfloat16 or wider, within the bound.
A program may use at most 64 MiB of HBM per device.

```python
import jax
import jax.numpy as jnp
from jax import lax

D = 2048
FF = 5120
TOK_DEV = 384
TOKENS = 1536
N_FS = 4
N_TP = 4


def level_of(stream_key, extent, split, least, high):
    level, own = 1.0, jax.random.fold_in(stream_key, 6)
    for dim, blocks in split:
        heights = jnp.exp(jax.random.uniform(jax.random.fold_in(own, dim), (blocks,), jnp.float32, least / len(split), high / len(split)))
        level = level * jnp.repeat(heights, extent[dim] // blocks).reshape([-1 if axis == dim else 1 for axis in range(len(extent))])
    return level


def normal_values(stream_key, dims, spread, bound, pieces=(), kind=jnp.bfloat16):
    loudness = level_of(stream_key, dims, pieces, -0.22, 0.18) if pieces else 1.0
    values = jax.random.normal(stream_key, dims, jnp.float32) * spread * loudness
    return jnp.minimum(jnp.maximum(values, -bound), bound).astype(kind)


def setup_inputs(seed: int = 0, part: int = 0) -> dict:
    splits = jax.random.split(jax.random.key(seed), 11)
    part_keys = jax.random.split(jax.random.fold_in(splits[10], part), 11)
    return {
        "tokens": normal_values(part_keys[0], (TOKENS, D), 0.5, 3.0, ((0, 4),)),
        "gate_weight": normal_values(splits[1], (D, FF), D ** -0.5, 0.125, ((0, 4), (1, 4))),
        "up_weight": normal_values(splits[2], (D, FF), D ** -0.5, 0.125, ((0, 4), (1, 4))),
        "down_weight": normal_values(splits[3], (FF, D), FF ** -0.5, 0.078125, ((0, 4), (1, 4))),
        "pool_weight": normal_values(splits[4], (D // 4, 4, D // 4), (D // 8) ** -0.5, 0.375, ((0, 4), (2, 4))),
        "pool_bias": normal_values(splits[5], (4, D // 4), 0.5, 3.0, (), jnp.float32),
        "pool_scale": jnp.clip(1.0 + 0.18 * jax.random.normal(splits[6], (D,), jnp.float32), 0.1, 1.9),
        "gain_first": jnp.clip(1.0 + 0.18 * jax.random.normal(splits[7], (D,), jnp.float32), 0.1, 1.9),
        "gain_mix": jnp.clip(1.0 + 0.18 * jax.random.normal(splits[8], (D,), jnp.float32), 0.1, 1.9),
        "gain_second": jnp.clip(1.0 + 0.18 * jax.random.normal(splits[9], (D,), jnp.float32), 0.1, 1.9),
    }


eps = 1e-06
pool_spans = (2, 4, 8, 16)

def rms_scale(values, gain_vec):
    fvalues = values.astype(jnp.float32)
    scaled = fvalues * lax.rsqrt(lax.optimization_barrier(jnp.mean(fvalues * fvalues, axis=-1, keepdims=True)) + eps)
    return (scaled * gain_vec).astype(jnp.bfloat16)

def ffn_hidden(normed, gate_weight, up_weight):
    gate_proj = jnp.dot(normed, gate_weight, preferred_element_type=jnp.float32)
    up_proj = jnp.dot(normed, up_weight, preferred_element_type=jnp.float32)
    return (jax.nn.silu(gate_proj) * up_proj).astype(jnp.bfloat16)

def down_sum(hidden, down_weight):
    block_width = FF // N_TP
    summed = jnp.zeros((hidden.shape[0], D), jnp.float32)
    for block_index in range(N_TP):
        lower_row = block_index * block_width
        partial_sum = jnp.dot(hidden[:, lower_row:lower_row + block_width], down_weight[lower_row:lower_row + block_width], preferred_element_type=jnp.float32)
        rounded = lax.optimization_barrier(partial_sum.astype(jnp.bfloat16))
        summed = summed + rounded.astype(jnp.float32)
    return summed

def pool_mix(normed, pool_weight, pool_bias, pool_scale):
    seq_len = normed.shape[0]
    group_width = D // 4
    grouped = normed.astype(jnp.float32).reshape(seq_len, 4, group_width)
    running = jnp.concatenate([jnp.zeros((1, 4, group_width), jnp.float32), jnp.cumsum(grouped, axis=0)], axis=0)
    position = jnp.arange(seq_len, dtype=jnp.int32)[:, None]
    spans = jnp.array(pool_spans, dtype=jnp.int32)[None, :]
    low_edge = jnp.clip(position - spans // 2, 0, seq_len)
    high_edge = jnp.clip(position - spans // 2 + spans, 0, seq_len)
    group_index = jnp.arange(4, dtype=jnp.int32)[None, :]
    counts = (high_edge - low_edge).astype(jnp.float32)[:, :, None]
    window_mean = (running[high_edge, group_index] - running[low_edge, group_index]) / counts
    deviation = (window_mean - grouped).astype(jnp.bfloat16)
    outputs = []
    for group_number in range(4):
        mapped = jnp.dot(deviation[:, group_number, :], pool_weight[:, group_number, :], preferred_element_type=jnp.float32)
        outputs.append(mapped + pool_bias[group_number])
    return jnp.concatenate(outputs, axis=-1) * pool_scale

def reference(tokens, gate_weight, up_weight, down_weight, pool_weight, pool_bias, pool_scale, gain_first, gain_mix, gain_second):

    def one_sequence(seq_rows):
        first_normed = rms_scale(seq_rows, gain_first)
        first_hidden = ffn_hidden(first_normed, gate_weight, up_weight)
        after_first = (seq_rows.astype(jnp.float32) + 0.5 * down_sum(first_hidden, down_weight)).astype(jnp.bfloat16)
        mix_normed = rms_scale(after_first, gain_mix)
        mixed = pool_mix(mix_normed, pool_weight, pool_bias, pool_scale)
        after_mix = (after_first.astype(jnp.float32) + mixed).astype(jnp.bfloat16)
        second_normed = rms_scale(after_mix, gain_second)
        second_hidden = ffn_hidden(second_normed, gate_weight, up_weight)
        return (after_mix.astype(jnp.float32) + 0.5 * down_sum(second_hidden, down_weight)).astype(jnp.bfloat16)
    sequences = tokens.reshape(N_FS, TOK_DEV, D)
    return lax.map(one_sequence, sequences).reshape(TOKENS, D)
```

```python
import functools

import jax
import jax.numpy as jnp
from jax import lax
from jax.experimental import pallas as pl
from jax.experimental.pallas import tpu as pltpu
from jax.sharding import PartitionSpec as P

eps = 1e-06
pool_spans = (2, 4, 8, 16)
pad_width = 8
MESH = pl.DeviceIdType.MESH


def rms_scale(values, gain_vec):
    fvalues = values.astype(jnp.float32)
    scaled = fvalues * lax.rsqrt(jnp.mean(fvalues * fvalues, axis=-1, keepdims=True) + eps)
    return (scaled * gain_vec).astype(jnp.bfloat16)


def ffn_hidden(normed, gate_full, up_full):
    gate_proj = jnp.dot(normed, gate_full, preferred_element_type=jnp.float32)
    up_proj = jnp.dot(normed, up_full, preferred_element_type=jnp.float32)
    return (jax.nn.silu(gate_proj) * up_proj).astype(jnp.bfloat16)


def pool_block(padded, offset, seq_len, pool_full, pool_bias, pool_scale):
    n_tokens = padded.shape[0] - 2 * pad_width
    group_width = pool_full.shape[0]
    position = offset + lax.iota(jnp.int32, n_tokens)
    column_pos = offset - pad_width + lax.iota(jnp.int32, padded.shape[0])
    center = padded[pad_width : pad_width + n_tokens].astype(jnp.float32)
    outputs = []
    for group_number, window_span in enumerate(pool_spans):
        low_edge = jnp.clip(position - window_span // 2, 0, seq_len)
        high_edge = jnp.clip(position - window_span // 2 + window_span, 0, seq_len)
        band_mask = (
            (column_pos[None, :] >= low_edge[:, None]) & (column_pos[None, :] < high_edge[:, None])
        ).astype(jnp.bfloat16)
        lower_col = group_number * group_width
        columns = padded[:, lower_col : lower_col + group_width]
        window_sum = jnp.dot(band_mask, columns, preferred_element_type=jnp.float32)
        window_mean = window_sum / (high_edge - low_edge).astype(jnp.float32)[:, None]
        deviation = (window_mean - center[:, lower_col : lower_col + group_width]).astype(
            jnp.bfloat16
        )
        mapped = jnp.dot(
            deviation, pool_full[:, group_number, :], preferred_element_type=jnp.float32
        )
        outputs.append(mapped + pool_bias[group_number])
    return jnp.concatenate(outputs, axis=-1) * pool_scale


def shards(
    tokens,
    gate_weight,
    up_weight,
    down_weight,
    pool_weight,
    pool_bias,
    pool_scale,
    gain_first,
    gain_mix,
    gain_second,
):
    gate_full, up_full, pool_half = (
        lax.all_gather(gate_weight, "fs", axis=0, tiled=True),
        lax.all_gather(up_weight, "fs", axis=0, tiled=True),
        lax.all_gather(pool_weight, "fs", axis=0, tiled=True),
    )
    down_full = lax.all_gather(down_weight, "fs", axis=1, tiled=True)
    pool_full = lax.all_gather(pool_half, "tp", axis=2, tiled=True)
    seq_len = tokens.shape[0]
    first_normed = rms_scale(tokens, gain_first)
    first_hidden = ffn_hidden(first_normed, gate_full, up_full)
    second_gate, second_up, second_down = (gate_full, up_full, down_full)
    first_branch = lax.psum(
        jnp.dot(first_hidden, down_full, preferred_element_type=jnp.float32).astype(jnp.bfloat16),
        "tp",
    ).astype(jnp.float32)
    after_first = (tokens.astype(jnp.float32) + 0.5 * first_branch).astype(jnp.bfloat16)
    mix_normed = rms_scale(after_first, gain_mix)
    padded = jnp.pad(mix_normed, ((pad_width, pad_width), (0, 0)))
    mixed = pool_block(padded, 0, seq_len, pool_full, pool_bias, pool_scale)
    after_mix = (after_first.astype(jnp.float32) + mixed).astype(jnp.bfloat16)
    second_normed = rms_scale(after_mix, gain_second)
    second_hidden = ffn_hidden(second_normed, second_gate, second_up)
    second_branch = lax.psum(
        jnp.dot(second_hidden, second_down, preferred_element_type=jnp.float32).astype(
            jnp.bfloat16
        ),
        "tp",
    ).astype(jnp.float32)
    return (after_mix.astype(jnp.float32) + 0.5 * second_branch).astype(jnp.bfloat16)


def fused_kernel(
    sizes, tok_ref, gate_ref, up_ref, down_ref, pool_ref, bias_ref, scale_ref, gain1_ref, gainm_ref, gain2_ref,
    out_ref,
    gu_full, down_full, pool_full, acc, normed, hidden, amix, res, guest, part0, rbuf0, xs0, xr0, xg0, lent,
    part1, rbuf1, xs1, xr1,
    zsend, zleft, zrecv, ysend, yrecv, tsend, trecv, lsem, asend, arecv, qsend, qrecv,
    csend, crecv, xsend, xrecv, gsend, grecv, fsend, frecv, osem,
):
    n, n_tp = sizes
    g, z, t = lax.axis_index("grp"), lax.axis_index("fs"), lax.axis_index("tp")
    core, side = lax.rem(t, 2), t // 2
    outer = (z == 0) | (z == n - 1)
    inner = (z > 0) & (z < n - 1)
    e = 1 - jnp.minimum(z, 1) * jnp.minimum(n - 1 - z, 1)
    pz = z + 1 - 2 * lax.rem(z, 2)
    mirror, far = n - 1 - z, n - 1 - pz
    y_peer, partner, inward = {"grp": 1 - g}, {"fs": pz}, {"fs": mirror}
    mate, x_peer = {"tp": t + 1 - 2 * core}, {"tp": lax.rem(t + 2, n_tp)}
    n_rows, width = tok_ref.shape
    d_loc, f_loc = gate_ref.shape
    groups, pool_rows, pool_cols = pool_ref.shape
    half_rows = n_rows // 2
    quarter = n_rows // n_tp
    block_cols = d_loc // 2
    n_blocks = 2 * n
    f32 = jnp.float32

    def remote(src, dst, s_sem, r_sem, dev):
        return pltpu.make_async_remote_copy(
            src_ref=src, dst_ref=dst, send_sem=s_sem, recv_sem=r_sem, device_id=dev, device_id_type=MESH
        )

    barrier = pltpu.get_barrier_semaphore()

    def greet(dev):
        pl.semaphore_signal(barrier, inc=1, device_id=dev, device_id_type=MESH)

    greet(y_peer)
    greet(partner)
    for off in range(1, n_tp):
        greet({"tp": lax.rem(t + off, n_tp)})

    @pl.when(inner)
    def _():
        greet(inward)

    pl.semaphore_wait(barrier, n_tp + 2 - e)

    counts = {"pool": 1, "gu": 8, "down": 4}
    first_key = {"pool": 0, "gu": 1, "down": 9}

    def each(name, act):
        if counts[name] == 1:
            act(0)
        else:
            pl.loop(0, counts[name])(act)

    def key(name, c):
        return first_key[name] + c

    def region(name, s, half, c):
        if name == "down":
            size = f_loc // 4
            return down_full.at[s, half, pl.ds(pl.multiple_of(c * size, 16), size), :]
        if name == "pool":
            size = pool_rows // 2
            rows = pl.ds(pl.multiple_of(s * pool_rows + half * size, 16), size)
            return pool_full.at[:, rows, pl.ds(pl.multiple_of(t * pool_cols, 128), pool_cols)]
        size = d_loc // 8
        rows = pl.ds(pl.multiple_of(s * d_loc + half * (d_loc // 2) + lax.rem(c, 4) * size, 16), size)
        return gu_full.at[c // 4, rows, :]

    def source(name, half, c):
        if name == "down":
            size = f_loc // 4
            cols = pl.ds(pl.multiple_of(half * block_cols, 128), block_cols)
            return down_ref.at[pl.ds(pl.multiple_of(c * size, 16), size), cols]
        if name == "pool":
            size = pool_rows // 2
            return pool_ref.at[:, pl.ds(pl.multiple_of(half * size, 16), size), :]
        size = d_loc // 8
        rows = pl.ds(pl.multiple_of(half * (d_loc // 2) + c * size, 16), size)
        return {"gate": gate_ref, "up": up_ref}[name].at[rows, :]

    def own_copy(name, c, half, s_sem, r_sem, dev):
        base = {"gate": 0, "up": 4}.get(name)
        k = key("gu", base + c) if base is not None else key(name, c)
        where = region("gu", z, half, base + c) if base is not None else region(name, z, half, c)
        return remote(source(name, half, c), where, s_sem.at[k], r_sem.at[z, k], dev)

    def own_partner(name, c):
        return own_copy(name, c, g, zsend.at[z], zrecv, partner)

    def own_inward(name, c):
        return own_copy(name, c, g, zleft, zrecv, inward)

    def own_direct(name, c):
        return own_copy(name, c, 1 - g, ysend.at[z], yrecv, partner)

    def passing(name, s, c, dev):
        there = region(name, s, g, c)
        return remote(there, there, zsend.at[s, key(name, c)], zrecv.at[s, key(name, c)], dev)

    def share(name, s, half, c):
        there = region(name, s, half, c)
        return remote(there, there, ysend.at[s, key(name, c)], yrecv.at[s, key(name, c)], y_peer)

    def settle(name, s, low=0, high=None):
        if counts[name] == 1:
            share(name, s, 1 - g, 0).wait_recv()
        else:
            pl.loop(low, counts[name] if high is None else high)(lambda c: share(name, s, 1 - g, c).wait_recv())

    def quarter_rows(tt):
        return pl.ds(pl.multiple_of((lax.rem(tt, 2) * (n_tp // 2) + tt // 2) * quarter, 16), quarter)

    def start_each(names, make):
        for name in names:
            pl.loop(0, 1 if name == "pool" else 4)(lambda c: make(name, c).start())

    tok_copy = remote(
        tok_ref.at[quarter_rows(t), :], guest.at[quarter_rows(t), :], asend.at[0], arecv.at[0], partner
    )

    @pl.when(outer)
    def _():
        tok_copy.start()
        start_each(("pool", "gate", "up"), own_partner)
        start_each(("pool", "gate", "up"), own_direct)
        start_each(("down",), own_partner)
        pl.loop(0, 2)(lambda c: own_direct("down", c).start())

    @pl.when(inner)
    def _():
        for name in ("pool", "gate", "up"):

            @pl.loop(0, 1 if name == "pool" else 4)
            def _(c):
                own_inward(name, c).start()
                own_partner(name, c).start()

    own_rows = pl.ds(pl.multiple_of(z * d_loc, 128), d_loc)
    own_pool = pool_full.at[
        :, pl.ds(pl.multiple_of(z * pool_rows, 16), pool_rows), pl.ds(pl.multiple_of(t * pool_cols, 128), pool_cols)
    ]
    local = [
        pltpu.make_async_copy(pool_ref, own_pool, lsem.at[0]),
        pltpu.make_async_copy(gate_ref, gu_full.at[0, own_rows, :], lsem.at[1]),
        pltpu.make_async_copy(up_ref, gu_full.at[1, own_rows, :], lsem.at[2]),
        pltpu.make_async_copy(down_ref.at[:, pl.ds(0, block_cols)], down_full.at[z, 0], lsem.at[3]),
        pltpu.make_async_copy(down_ref.at[:, pl.ds(block_cols, block_cols)], down_full.at[z, 1], lsem.at[4]),
    ]
    for copy in local:
        copy.start()

    def norm_rows(src, gain, base=0):
        @pl.loop(0, n_rows // 32)
        def _(r):
            values = src[pl.ds(pl.multiple_of(r * 32, 32), 32), :].astype(f32)
            scaled = values * lax.rsqrt(jnp.mean(values * values, axis=-1, keepdims=True) + eps)
            normed[pl.ds(pl.multiple_of(base + r * 32, 32), 32), :] = (scaled * gain[...]).astype(jnp.bfloat16)

    tile = 256

    def add_shard(w, s, first=False):
        k_cols = pl.ds(pl.multiple_of(s * d_loc, 128), d_loc)

        @pl.loop(0, f_loc // tile)
        def _(i):
            cols = pl.ds(pl.multiple_of(i * tile, tile), tile)
            product = jnp.dot(normed[:, k_cols], gu_full[w, k_cols, cols], preferred_element_type=f32)
            acc[w, :, cols] = product if first else acc[w, :, cols] + product

    def pool_copy(off, s, sender):
        cols = pl.ds(pl.multiple_of(sender * pool_cols, 128), pool_cols)
        there = pool_full.at[:, pl.ds(pl.multiple_of(s * pool_rows, 16), pool_rows), cols]
        return remote(there, there, tsend.at[off - 1, s], trecv.at[off - 1, s], {"tp": lax.rem(t + off, n_tp)})

    def spread_pool(s):
        for off in range(1, n_tp):
            pool_copy(off, s, t).start()

    def activate(gate_proj, up_proj):
        return (gate_proj / (1.0 + jnp.exp(-gate_proj)) * up_proj).astype(jnp.bfloat16)

    def guest_copy(off, sender):
        there = guest.at[quarter_rows(sender), :]
        return remote(there, there, qsend.at[off - 1, 0], qrecv.at[off - 1, 0], {"tp": lax.rem(t + off, n_tp)})

    def columns(place):
        s, half = place
        return pl.ds(pl.multiple_of(s * d_loc + half * block_cols, 128), block_cols)

    def first_place(j, at):
        here = [at, n - 1 - at, at + 1 - 2 * lax.rem(at, 2)]
        here.append(n - 1 - here[2])
        shard, half = ((0, 0), (0, 1), (1, 0), (1, 1), (2, 0), (3, 0), (2, 1), (3, 1))[j]
        return here[shard], g if half == 0 else 1 - g

    def second_place(j):
        here = [z, e * pz + (1 - e) * mirror, e * far + (1 - e) * pz, e * mirror + (1 - e) * far]
        return here[j // 2], g if j % 2 == 0 else 1 - g

    mine = pl.ds(pl.multiple_of(core * half_rows, 16), half_rows)
    other = pl.ds(pl.multiple_of((1 - core) * half_rows, 16), half_rows)

    def final_copy(phase, j, place, rows):
        there = res.at[phase, rows, columns(place)]
        return remote(there, there, fsend.at[phase, j], frecv.at[phase, j], mate)

    def pair_first(j):
        return remote(part0.at[j, 1 - core], rbuf0.at[j], csend.at[0, j], crecv.at[0, j], mate)

    def x_first(j):
        return remote(xs0.at[j, 0], xr0.at[j], xsend.at[0, j], xrecv.at[0, j], x_peer)

    kept = pl.ds(pl.multiple_of(side * quarter, 16), quarter)
    given = pl.ds(pl.multiple_of((1 - side) * quarter, 16), quarter)

    def x_guest(j):
        return remote(xs0.at[j, 1, given, :], xg0.at[j], gsend.at[j], grecv.at[j], x_peer)

    def lend_copy(j, at):
        cols = columns(first_place(j, at))
        return remote(lent.at[j], res.at[0, quarter_rows(t), cols], asend.at[1 + j], arecv.at[1 + j], partner)

    def lent_copy(j, off, sender):
        there = res.at[0, quarter_rows(sender), columns(first_place(j, pz))]
        return remote(
            there, there, qsend.at[off - 1, 1 + j], qrecv.at[off - 1, 1 + j], {"tp": lax.rem(t + off, n_tp)}
        )

    def from_mirror(name, c):
        passing(name, mirror, c, partner).wait_recv()
        passing(name, mirror, c, partner).start()
        share(name, mirror, g, c).start()

    def from_far(name, c):
        passing(name, far, c, partner).wait_recv()
        passing(name, far, c, partner).start()
        share(name, far, g, c).start()

    def from_partner(name, c):
        passing(name, pz, c, inward).wait_recv()
        passing(name, pz, c, inward).start()

    def down_mirror(c):
        passing("down", mirror, c, partner).wait_recv()
        share("down", mirror, g, c).start()

    def down_far(c):
        passing("down", far, c, partner).wait_recv()
        share("down", far, g, c).start()

    def down_partner(c, shared):
        from_partner("down", c)
        if shared:
            share("down", pz, g, c).start()

    def first_ffn():
        for copy in local:
            copy.wait()
        spread_pool(z)
        norm_rows(tok_ref, gain1_ref)
        tok_copy.wait_recv()
        for off in range(1, n_tp):
            guest_copy(off, t).start()
        from_mirror("pool", 0)
        from_mirror("gu", 0)
        from_mirror("gu", 1)
        from_partner("pool", 0)

        @pl.loop(0, 4)
        def _(m):
            from_mirror("gu", m + 2)
            from_partner("gu", m)

        for off in range(1, n_tp):
            guest_copy(off, lax.rem(t - off + n_tp, n_tp)).wait_recv()
        norm_rows(guest, gain1_ref, n_rows)
        from_mirror("gu", 6)
        from_partner("gu", 4)
        add_shard(0, z, True)
        from_mirror("gu", 7)
        from_partner("gu", 5)
        add_shard(1, z, True)
        settle("pool", mirror)
        spread_pool(mirror)
        from_far("pool", 0)
        from_far("gu", 0)
        from_partner("gu", 6)
        settle("gu", mirror, 0, 4)
        add_shard(0, mirror)
        from_far("gu", 1)
        from_partner("gu", 7)
        pl.loop(0, 4)(lambda c: own_inward("down", c).start())
        settle("gu", mirror, 4, 8)
        add_shard(1, mirror)
        pl.loop(2, 5)(lambda m: from_far("gu", m))
        settle("pool", far)
        spread_pool(far)
        settle("pool", pz)
        spread_pool(pz)
        settle("gu", far, 0, 4)
        add_shard(0, far)
        from_far("gu", 5)
        settle("gu", pz, 0, 4)
        add_shard(0, pz)
        pl.loop(6, 8)(lambda m: from_far("gu", m))
        settle("gu", far, 4, 8)
        add_shard(1, far)
        down_mirror(0)
        down_mirror(1)
        settle("gu", pz, 4, 8)
        add_shard(1, pz)
        down_mirror(2)

        @pl.loop(0, f_loc // tile)
        def _(i):
            cols = pl.ds(pl.multiple_of(i * tile, tile), tile)

            @pl.loop(0, 2 * n_rows // 128)
            def _(r):
                rows = pl.ds(pl.multiple_of(r * 128, 128), 128)
                hidden[rows, cols] = activate(acc[0, rows, cols], acc[1, rows, cols])

        def multiply(j):
            s, half = first_place(j, z)
            product = jnp.dot(hidden[...], down_full[s, half], preferred_element_type=f32).astype(jnp.bfloat16)
            for seq in range(2):
                for part in range(2):
                    row = seq * n_rows + part * half_rows
                    part0[j, part, seq] = product[row : row + half_rows]
            pair_first(j).start()

        def add_pair(j):
            pair_first(j).wait_recv()
            xs0[j] = (part0[j, core].astype(f32) + rbuf0[j].astype(f32)).astype(jnp.bfloat16)
            x_guest(j).start()
            x_first(j).start()

        def finish(j):
            place = first_place(j, z)
            cols = columns(place)
            x_guest(j).wait_recv()
            total = xs0[j, 1, kept, :].astype(f32) + xg0[j].astype(f32)
            lent[j] = (guest[quarter_rows(t), cols].astype(f32) + 0.5 * total).astype(jnp.bfloat16)
            lend_copy(j, z).start()
            x_first(j).wait_recv()
            total = xs0[j, 0].astype(f32) + xr0[j].astype(f32)
            res[0, mine, cols] = (tok_ref[mine, cols].astype(f32) + 0.5 * total).astype(jnp.bfloat16)
            final_copy(0, j, place, mine).start()

        down_partner(0, False)
        down_mirror(3)
        for j in range(n_blocks):
            if j == 2:
                down_partner(1, False)
                down_far(0)
                settle("down", mirror)
            if j == 4:
                down_partner(2, True)
                down_far(1)
                down_partner(3, True)
                down_far(2)
            if j == 5:
                down_far(3)
            if j == 6:
                settle("down", pz)
            if j == 7:
                settle("down", far)
            multiply(j)
            if j >= 1:
                add_pair(j - 1)
            if j >= 3:
                finish(j - 3)
            if j == 5:
                own_partner("down", 0).start()
            if j == 7:
                own_partner("down", 1).start()
        add_pair(n_blocks - 1)
        for j in range(n_blocks - 3, n_blocks):
            finish(j)
        own_partner("down", 2).start()
        own_partner("down", 3).start()
        pl.loop(0, 4)(lambda c: passing("down", mirror, c, partner).start())
        pl.loop(0, 4)(lambda c: passing("down", far, c, partner).start())
        for j in range(n_blocks):
            final_copy(0, j, first_place(j, z), other).wait_recv()

    def take(name, s, c):
        passing(name, s, c, partner).wait_recv()
        share(name, s, g, c).start()

    def collect():
        for copy in local:
            copy.wait()
        spread_pool(z)
        for s in (pz, far, mirror):
            take("pool", s, 0)
            pl.loop(0, 8)(lambda m: take("gu", s, m))
            settle("pool", s)
            spread_pool(s)

        def hand_out(j):
            lend_copy(j, pz).wait_recv()
            for off in range(1, n_tp):
                lent_copy(j, off, t).start()

        for j in range(n_blocks):
            hand_out(j)
            if j == 2:
                take("down", pz, 0)
            if j == 4:
                take("down", pz, 1)
        for s in (pz, far, mirror):
            settle("gu", s)
        for j in range(n_blocks):
            for off in range(1, n_tp):
                lent_copy(j, off, lax.rem(t - off + n_tp, n_tp)).wait_recv()

    pl.when(inner)(first_ffn)
    pl.when(outer)(collect)

    def when_outer(act):
        pl.when(outer)(act)

    norm_rows(res.at[0], gainm_ref)
    for off in range(1, n_tp):
        for s in range(n):
            pool_copy(off, s, lax.rem(t - off + n_tp, n_tp)).wait_recv()
    group_width = width // groups
    row_id = lax.broadcasted_iota(jnp.int32, (n_rows, n_rows), 0)
    col_id = lax.broadcasted_iota(jnp.int32, (n_rows, n_rows), 1)
    position = lax.broadcasted_iota(jnp.int32, (n_rows, 1), 0)
    own_seq = pl.ds(0, n_rows)
    for k, span in enumerate(pool_spans):
        low = row_id - span // 2
        band = jnp.where((col_id >= low) & (col_id < low + span), 1.0, 0.0).astype(jnp.bfloat16)
        first = jnp.maximum(position - span // 2, 0)
        last = jnp.minimum(position - span // 2 + span, n_rows)
        inverse = 1.0 / (last - first).astype(f32)
        cols = pl.ds(k * group_width, group_width)
        mean = jnp.dot(band, normed[own_seq, cols], preferred_element_type=f32) * inverse
        deviation = (mean - normed[own_seq, cols].astype(f32)).astype(jnp.bfloat16)
        mapped = jnp.dot(deviation, pool_full[k], preferred_element_type=f32) + bias_ref[pl.ds(k, 1), :]
        amix[:, cols] = (res[0, :, cols].astype(f32) + mapped * scale_ref[:, cols]).astype(jnp.bfloat16)
        if k % 2 == 1:
            when_outer(lambda: take("down", pz, 2 + k // 2))

    norm_rows(amix, gain2_ref)

    @pl.loop(0, f_loc // tile)
    def _(i):
        cols = pl.ds(pl.multiple_of(i * tile, tile), tile)
        gate_proj = jnp.dot(normed[own_seq, :], gu_full[0, :, cols], preferred_element_type=f32)
        up_proj = jnp.dot(normed[own_seq, :], gu_full[1, :, cols], preferred_element_type=f32)
        hidden[own_seq, cols] = activate(gate_proj, up_proj)

        @pl.when(outer & (i < 4))
        def _():
            take("down", far, i)

    def pair_copy(j):
        return remote(part1.at[j, other, :], rbuf1.at[j], csend.at[1, j], crecv.at[1, j], mate)

    def x_copy(j):
        return remote(xs1.at[j], xr1.at[j], xsend.at[1, j], xrecv.at[1, j], x_peer)

    def out_copy(j):
        cols = columns(second_place(j))
        return pltpu.make_async_copy(res.at[1, :, cols], out_ref.at[:, cols], osem.at[j])

    def multiply(j):
        s, half = second_place(j)
        part1[j] = jnp.dot(hidden[own_seq, :], down_full[s, half], preferred_element_type=f32).astype(jnp.bfloat16)
        pair_copy(j).start()

    def add_pair(j):
        pair_copy(j).wait_recv()
        xs1[j] = (part1[j, mine, :].astype(f32) + rbuf1[j].astype(f32)).astype(jnp.bfloat16)
        x_copy(j).start()

    def finish(j):
        x_copy(j).wait_recv()
        place = second_place(j)
        cols = columns(place)
        total = xs1[j].astype(f32) + xr1[j].astype(f32)
        res[1, mine, cols] = (amix[mine, cols].astype(f32) + 0.5 * total).astype(jnp.bfloat16)
        final_copy(1, j, place, mine).start()

    def emit(j):
        final_copy(1, j, second_place(j), other).wait_recv()
        out_copy(j).start()

    for j in range(n_blocks):
        if j == 3:
            when_outer(lambda: settle("down", pz))
        if j == 5:
            when_outer(lambda: settle("down", far))
        if 3 <= j < 7:
            when_outer(lambda: take("down", mirror, j - 3))
        if j == 7:
            when_outer(lambda: settle("down", mirror))
        multiply(j)
        if j >= 1:
            add_pair(j - 1)
        if j >= 3:
            finish(j - 3)
        if j >= 5:
            emit(j - 5)
    add_pair(n_blocks - 1)
    for j in range(n_blocks - 3, n_blocks):
        finish(j)
    for j in range(n_blocks - 5, n_blocks):
        emit(j)

    @pl.loop(0, n)
    def _(s):
        for off in range(1, n_tp):
            pool_copy(off, s, t).wait_send()

    for name in ("pool", "gate", "up", "down"):
        pl.loop(0, 1 if name == "pool" else 4)(lambda c: own_partner(name, c).wait_send())

    @pl.when(outer)
    def _():
        tok_copy.wait_send()
        for name in ("pool", "gate", "up", "down"):
            direct = {"pool": 1, "down": 2}.get(name, 4)
            pl.loop(0, direct)(lambda c: own_direct(name, c).wait_send())
        for s in (pz, far, mirror):
            for name in ("pool", "gu", "down"):
                each(name, lambda c: share(name, s, g, c).wait_send())
        for j in range(n_blocks):
            for off in range(1, n_tp):
                lent_copy(j, off, t).wait_send()

    @pl.when(inner)
    def _():
        for off in range(1, n_tp):
            guest_copy(off, t).wait_send()
        for name in ("pool", "gate", "up", "down"):
            pl.loop(0, 1 if name == "pool" else 4)(lambda c: own_inward(name, c).wait_send())
        for name in ("pool", "gu", "down"):
            each(name, lambda c: passing(name, pz, c, inward).wait_send())
            for s in (mirror, far):

                def sent(c):
                    passing(name, s, c, partner).wait_send()
                    share(name, s, g, c).wait_send()

                each(name, sent)
        pl.loop(2, 4)(lambda c: share("down", pz, g, c).wait_send())
        for j in range(n_blocks):
            pair_first(j).wait_send()
            x_first(j).wait_send()
            x_guest(j).wait_send()
            lend_copy(j, z).wait_send()
            final_copy(0, j, first_place(j, z), mine).wait_send()

    for j in range(n_blocks):
        pair_copy(j).wait_send()
        x_copy(j).wait_send()
        final_copy(1, j, second_place(j), mine).wait_send()
        out_copy(j).wait()


def fused_shards(
    n, n_tp, tokens, gate_weight, up_weight, down_weight, pool_weight, pool_bias, pool_scale,
    gain_first, gain_mix, gain_second,
):
    n_rows, width = tokens.shape
    d_loc, f_loc = gate_weight.shape
    groups = pool_weight.shape[1]
    pool = jnp.swapaxes(pool_weight, 0, 1)
    bf16, dma, vmem = jnp.bfloat16, pltpu.SemaphoreType.DMA, pltpu.VMEM
    in_vmem, anywhere = pl.BlockSpec(memory_space=pltpu.VMEM), pl.BlockSpec(memory_space=pl.ANY)
    half, quarter, block, blocks = n_rows // 2, n_rows // n_tp, d_loc // 2, 2 * n
    return pl.pallas_call(
        functools.partial(fused_kernel, (n, n_tp)),
        out_shape=jax.ShapeDtypeStruct((n_rows, width), bf16),
        in_specs=[in_vmem] + [anywhere] * 4 + [in_vmem] * 5,
        out_specs=anywhere,
        scratch_shapes=[
            vmem((2, n * d_loc, f_loc), bf16),
            vmem((n, 2, f_loc, block), bf16),
            vmem((groups, n * pool.shape[1], n_tp * pool.shape[2]), bf16),
            vmem((2, 2 * n_rows, f_loc), jnp.float32),
            vmem((2 * n_rows, width), bf16),
            vmem((2 * n_rows, f_loc), bf16),
            vmem((n_rows, width), bf16),
            vmem((2, n_rows, width), bf16),
            vmem((n_rows, width), bf16),
            vmem((blocks, 2, 2, half, block), bf16),
            vmem((blocks, 2, half, block), bf16),
            vmem((blocks, 2, half, block), bf16),
            vmem((blocks, half, block), bf16),
            vmem((blocks, quarter, block), bf16),
            vmem((blocks, quarter, block), bf16),
            vmem((blocks, n_rows, block), bf16),
            vmem((blocks, half, block), bf16),
            vmem((blocks, half, block), bf16),
            vmem((blocks, half, block), bf16),
            dma((n, 13)), dma((13,)), dma((n, 13)), dma((n, 13)), dma((n, 13)),
            dma((n_tp - 1, n)), dma((n_tp - 1, n)), dma((5,)),
            dma((1 + blocks,)), dma((1 + blocks,)), dma((n_tp - 1, 1 + blocks)), dma((n_tp - 1, 1 + blocks)),
            dma((2, blocks)), dma((2, blocks)), dma((2, blocks)), dma((2, blocks)), dma((blocks,)), dma((blocks,)),
            dma((2, blocks)), dma((2, blocks)), dma((blocks,)),
        ],
        compiler_params=pltpu.CompilerParams(
            collective_id=0, has_side_effects=True, vmem_limit_bytes=60 * 1024 * 1024
        ),
    )(
        tokens, gate_weight, up_weight, down_weight, pool, pool_bias, pool_scale.reshape(1, width),
        gain_first.reshape(1, width), gain_mix.reshape(1, width), gain_second.reshape(1, width),
    )


def layer(n_grp, n, n_tp, *args):
    n_rows, width = args[0].shape
    d_loc, f_loc = args[1].shape
    pool_rows, _, pool_cols = args[4].shape
    fits = n_grp == 2 and n_tp == 4 and n == 4 and n_rows % 64 == 0
    fits = fits and d_loc % 512 == 0 and f_loc % 256 == 0 and pool_rows % 32 == 0 and pool_cols % 128 == 0
    return fused_shards(n, n_tp, *args) if fits else shards(*args)


def solution(mesh):
    return jax.shard_map(
        functools.partial(layer, mesh.shape["grp"], mesh.shape["fs"], mesh.shape["tp"]),
        mesh=mesh,
        in_specs=(
            P(("grp", "fs"), None),
            P("fs", "tp"),
            P("fs", "tp"),
            P("tp", "fs"),
            P("fs", None, "tp"),
            P(),
            P(),
            P(),
            P(),
            P(),
        ),
        out_specs=P(("grp", "fs"), None),
        check_vma=False,
    )
```

```python
import functools

import jax
import jax.numpy as jnp
from jax import lax
from jax.experimental import pallas as pl
from jax.experimental.pallas import tpu as pltpu
from jax.sharding import PartitionSpec as P

eps = 1e-06
pool_spans = (2, 4, 8, 16)
pad_width = 8
MESH = pl.DeviceIdType.MESH


def rms_scale(values, gain_vec):
    fvalues = values.astype(jnp.float32)
    scaled = fvalues * lax.rsqrt(jnp.mean(fvalues * fvalues, axis=-1, keepdims=True) + eps)
    return (scaled * gain_vec).astype(jnp.bfloat16)


def ffn_hidden(normed, gate_full, up_full):
    gate_proj = jnp.dot(normed, gate_full, preferred_element_type=jnp.float32)
    up_proj = jnp.dot(normed, up_full, preferred_element_type=jnp.float32)
    return (jax.nn.silu(gate_proj) * up_proj).astype(jnp.bfloat16)


def pool_block(padded, offset, seq_len, pool_full, pool_bias, pool_scale):
    n_tokens = padded.shape[0] - 2 * pad_width
    group_width = pool_full.shape[0]
    position = offset + lax.iota(jnp.int32, n_tokens)
    column_pos = offset - pad_width + lax.iota(jnp.int32, padded.shape[0])
    center = padded[pad_width : pad_width + n_tokens].astype(jnp.float32)
    outputs = []
    for group_number, window_span in enumerate(pool_spans):
        low_edge = jnp.clip(position - window_span // 2, 0, seq_len)
        high_edge = jnp.clip(position - window_span // 2 + window_span, 0, seq_len)
        band_mask = (
            (column_pos[None, :] >= low_edge[:, None]) & (column_pos[None, :] < high_edge[:, None])
        ).astype(jnp.bfloat16)
        lower_col = group_number * group_width
        columns = padded[:, lower_col : lower_col + group_width]
        window_sum = jnp.dot(band_mask, columns, preferred_element_type=jnp.float32)
        window_mean = window_sum / (high_edge - low_edge).astype(jnp.float32)[:, None]
        deviation = (window_mean - center[:, lower_col : lower_col + group_width]).astype(
            jnp.bfloat16
        )
        mapped = jnp.dot(
            deviation, pool_full[:, group_number, :], preferred_element_type=jnp.float32
        )
        outputs.append(mapped + pool_bias[group_number])
    return jnp.concatenate(outputs, axis=-1) * pool_scale


def shards(
    tokens,
    gate_weight,
    up_weight,
    down_weight,
    pool_weight,
    pool_bias,
    pool_scale,
    gain_first,
    gain_mix,
    gain_second,
):
    gate_full, up_full, pool_half = (
        lax.all_gather(gate_weight, "fs", axis=0, tiled=True),
        lax.all_gather(up_weight, "fs", axis=0, tiled=True),
        lax.all_gather(pool_weight, "fs", axis=0, tiled=True),
    )
    down_full = lax.all_gather(down_weight, "fs", axis=1, tiled=True)
    pool_full = lax.all_gather(pool_half, "tp", axis=2, tiled=True)
    seq_len = tokens.shape[0]
    first_normed = rms_scale(tokens, gain_first)
    first_hidden = ffn_hidden(first_normed, gate_full, up_full)
    second_gate, second_up, second_down = (gate_full, up_full, down_full)
    first_branch = lax.psum(
        jnp.dot(first_hidden, down_full, preferred_element_type=jnp.float32).astype(jnp.bfloat16),
        "tp",
    ).astype(jnp.float32)
    after_first = (tokens.astype(jnp.float32) + 0.5 * first_branch).astype(jnp.bfloat16)
    mix_normed = rms_scale(after_first, gain_mix)
    padded = jnp.pad(mix_normed, ((pad_width, pad_width), (0, 0)))
    mixed = pool_block(padded, 0, seq_len, pool_full, pool_bias, pool_scale)
    after_mix = (after_first.astype(jnp.float32) + mixed).astype(jnp.bfloat16)
    second_normed = rms_scale(after_mix, gain_second)
    second_hidden = ffn_hidden(second_normed, second_gate, second_up)
    second_branch = lax.psum(
        jnp.dot(second_hidden, second_down, preferred_element_type=jnp.float32).astype(
            jnp.bfloat16
        ),
        "tp",
    ).astype(jnp.float32)
    return (after_mix.astype(jnp.float32) + 0.5 * second_branch).astype(jnp.bfloat16)


def fused_kernel(
    sizes, tok_ref, gate_ref, up_ref, down_ref, pool_ref, bias_ref, scale_ref, gain1_ref, gainm_ref, gain2_ref,
    out_ref,
    gu_full, down_full, pool_full, acc, normed, hidden, amix, res, guest, part0, rbuf0, xs0, xr0, xg0, lent,
    part1, rbuf1, xs1, xr1,
    zsend, zleft, zrecv, ysend, yrecv, tsend, trecv, lsem, asend, arecv, qsend, qrecv,
    csend, crecv, xsend, xrecv, gsend, grecv, fsend, frecv, osem,
):
    n, n_tp = sizes
    g, z, t = lax.axis_index("grp"), lax.axis_index("fs"), lax.axis_index("tp")
    core, side = lax.rem(t, 2), t // 2
    outer = (z == 0) | (z == n - 1)
    inner = (z > 0) & (z < n - 1)
    e = 1 - jnp.minimum(z, 1) * jnp.minimum(n - 1 - z, 1)
    pz = z + 1 - 2 * lax.rem(z, 2)
    mirror, far = n - 1 - z, n - 1 - pz
    y_peer, partner, inward = {"grp": 1 - g}, {"fs": pz}, {"fs": mirror}
    mate, x_peer = {"tp": t + 1 - 2 * core}, {"tp": lax.rem(t + 2, n_tp)}
    n_rows, width = tok_ref.shape
    d_loc, f_loc = gate_ref.shape
    groups, pool_rows, pool_cols = pool_ref.shape
    half_rows = n_rows // 2
    quarter = n_rows // n_tp
    block_cols = d_loc // 2
    n_blocks = 2 * n
    f32 = jnp.float32

    def remote(src, dst, s_sem, r_sem, dev):
        return pltpu.make_async_remote_copy(
            src_ref=src, dst_ref=dst, send_sem=s_sem, recv_sem=r_sem, device_id=dev, device_id_type=MESH
        )

    barrier = pltpu.get_barrier_semaphore()

    def greet(dev):
        pl.semaphore_signal(barrier, inc=1, device_id=dev, device_id_type=MESH)

    greet(y_peer)
    greet(partner)
    for off in range(1, n_tp):
        greet({"tp": lax.rem(t + off, n_tp)})

    @pl.when(inner)
    def _():
        greet(inward)

    pl.semaphore_wait(barrier, n_tp + 2 - e)

    counts = {"pool": 1, "gu": 8, "down": 8}
    first_key = {"pool": 0, "gu": 1, "down": 9}

    def each(name, act):
        if counts[name] == 1:
            act(0)
        else:
            pl.loop(0, counts[name])(act)

    kind = {"pool": 0, "gu": 1, "down": 2}

    def key(name, c):
        return first_key[name] + c

    def slot(s, at):
        return lax.rem(s - at + n, n) - 1

    def bulk(name, c):
        return 0 if name == "pool" else 3 if name == "down" else 1 + c // 4

    def region(name, s, half, c):
        if name == "down":
            size = f_loc // 8
            return down_full.at[s, half, pl.ds(pl.multiple_of(c * size, 16), size), :]
        if name == "pool":
            size = pool_rows // 2
            rows = pl.ds(pl.multiple_of(s * pool_rows + half * size, 16), size)
            return pool_full.at[:, rows, pl.ds(pl.multiple_of(t * pool_cols, 128), pool_cols)]
        size = d_loc // 8
        rows = pl.ds(pl.multiple_of(s * d_loc + half * (d_loc // 2) + lax.rem(c, 4) * size, 16), size)
        return gu_full.at[c // 4, rows, :]

    def whole(name, s, half):
        if name == "down":
            return down_full.at[s, half]
        if name == "pool":
            return region(name, s, half, 0)
        rows = pl.ds(pl.multiple_of(s * d_loc + half * (d_loc // 2), 16), d_loc // 2)
        return gu_full.at[:, rows, :] if name == "gu" else gu_full.at[0 if name == "gate" else 1, rows, :]

    def source(name, half, c):
        if name == "down":
            size = f_loc // 8
            cols = pl.ds(pl.multiple_of(half * block_cols, 128), block_cols)
            return down_ref.at[pl.ds(pl.multiple_of(c * size, 16), size), cols]
        if name == "pool":
            size = pool_rows // 2
            return pool_ref.at[:, pl.ds(pl.multiple_of(half * size, 16), size), :]
        size = d_loc // 8
        rows = pl.ds(pl.multiple_of(half * (d_loc // 2) + c * size, 16), size)
        return {"gate": gate_ref, "up": up_ref}[name].at[rows, :]

    def own_copy(name, c, half, s_sem, r_sem, dev):
        base = {"gate": 0, "up": 4}.get(name)
        name_of, at = ("gu", base + c) if base is not None else (name, c)
        where = region(name_of, z, half, at)
        return remote(source(name, half, c), where, s_sem.at[kind[name_of]], r_sem(name_of, at), dev)

    def own_partner(name, c):
        return own_copy(name, c, g, zsend.at[z], lambda nm, at: zrecv.at[slot(z, pz), key(nm, at)], partner)

    def own_inward(name, c):
        return own_copy(name, c, g, zleft, lambda nm, at: zrecv.at[slot(z, mirror), key(nm, at)], inward)

    def own_direct(name, c):
        return own_copy(name, c, 1 - g, ysend.at[z], lambda nm, at: yrecv.at[slot(z, pz), bulk(nm, at)], partner)

    def passing(name, s, c, dev):
        there = region(name, s, g, c)
        to = pz if dev is partner else mirror
        return remote(there, there, zsend.at[s, kind[name]], zrecv.at[slot(s, to), key(name, c)], dev)

    def arrival(name, s, c):
        there = region(name, s, g, c)
        return remote(there, there, zsend.at[s, kind[name]], zrecv.at[slot(s, z), key(name, c)], partner)

    def share(name, s, c):
        there = region(name, s, g, c)
        return remote(there, there, ysend.at[s, kind[name]], yrecv.at[slot(s, z), bulk(name, c)], y_peer)

    def settle(name, s):
        there = whole(name, s, 1 - g)
        where = {"pool": 0, "gate": 1, "up": 2, "down": 3}[name]
        remote(there, there, ysend.at[s, 0], yrecv.at[slot(s, z), where], y_peer).wait_recv()

    def sent(name, s, half, sems, dev):
        there = whole(name, s, half)
        return remote(there, there, sems.at[kind[name]], yrecv.at[0, 0], dev)

    kinds = ("pool", "gu", "down")

    def quarter_rows(tt):
        return pl.ds(pl.multiple_of((lax.rem(tt, 2) * (n_tp // 2) + tt // 2) * quarter, 16), quarter)

    own_counts = {"pool": 1, "gate": 4, "up": 4, "down": 8}

    def start_each(names, make):
        for name in names:
            pl.loop(0, own_counts[name])(lambda c: make(name, c).start())

    tok_copy = remote(
        tok_ref.at[quarter_rows(t), :], guest.at[quarter_rows(t), :], asend.at[0], arecv.at[0], partner
    )

    @pl.when(outer)
    def _():
        tok_copy.start()
        start_each(("pool", "gate", "up"), own_partner)
        start_each(("pool", "gate", "up"), own_direct)
        start_each(("down",), own_partner)
        start_each(("down",), own_direct)

    @pl.when(inner)
    def _():
        for name in ("pool", "gate", "up"):

            @pl.loop(0, own_counts[name])
            def _(c):
                own_inward(name, c).start()
                own_partner(name, c).start()

    own_rows = pl.ds(pl.multiple_of(z * d_loc, 128), d_loc)
    own_pool = pool_full.at[
        :, pl.ds(pl.multiple_of(z * pool_rows, 16), pool_rows), pl.ds(pl.multiple_of(t * pool_cols, 128), pool_cols)
    ]
    local = [
        pltpu.make_async_copy(pool_ref, own_pool, lsem.at[0]),
        pltpu.make_async_copy(gate_ref, gu_full.at[0, own_rows, :], lsem.at[1]),
        pltpu.make_async_copy(up_ref, gu_full.at[1, own_rows, :], lsem.at[2]),
        pltpu.make_async_copy(down_ref.at[:, pl.ds(0, block_cols)], down_full.at[z, 0], lsem.at[3]),
        pltpu.make_async_copy(down_ref.at[:, pl.ds(block_cols, block_cols)], down_full.at[z, 1], lsem.at[4]),
    ]
    for copy in local:
        copy.start()

    def norm_rows(src, gain, base=0):
        @pl.loop(0, n_rows // 32)
        def _(r):
            values = src[pl.ds(pl.multiple_of(r * 32, 32), 32), :].astype(f32)
            scaled = values * lax.rsqrt(jnp.mean(values * values, axis=-1, keepdims=True) + eps)
            normed[pl.ds(pl.multiple_of(base + r * 32, 32), 32), :] = (scaled * gain[...]).astype(jnp.bfloat16)

    tile = 256

    def add_shard(w, s, first=False):
        k_cols = pl.ds(pl.multiple_of(s * d_loc, 128), d_loc)

        @pl.loop(0, f_loc // tile)
        def _(i):
            cols = pl.ds(pl.multiple_of(i * tile, tile), tile)
            product = jnp.dot(normed[:, k_cols], gu_full[w, k_cols, cols], preferred_element_type=f32)
            acc[w, :, cols] = product if first else acc[w, :, cols] + product

    def pool_copy(off, s, sender):
        cols = pl.ds(pl.multiple_of(sender * pool_cols, 128), pool_cols)
        there = pool_full.at[:, pl.ds(pl.multiple_of(s * pool_rows, 16), pool_rows), cols]
        return remote(there, there, tsend.at[off - 1], trecv.at[off - 1], {"tp": lax.rem(t + off, n_tp)})

    def pool_all(off, sender):
        there = pool_full.at[:, :, pl.ds(pl.multiple_of(sender * pool_cols, 128), pool_cols)]
        return remote(there, there, tsend.at[off - 1], trecv.at[off - 1], {"tp": lax.rem(t + off, n_tp)})

    def spread_pool(s):
        for off in range(1, n_tp):
            pool_copy(off, s, t).start()

    def activate(gate_proj, up_proj):
        return (gate_proj / (1.0 + jnp.exp(-gate_proj)) * up_proj).astype(jnp.bfloat16)

    def guest_copy(off, sender):
        there = guest.at[quarter_rows(sender), :]
        return remote(there, there, qsend.at[off - 1], qrecv.at[off - 1], {"tp": lax.rem(t + off, n_tp)})

    def columns(place):
        s, half = place
        return pl.ds(pl.multiple_of(s * d_loc + half * block_cols, 128), block_cols)

    def first_place(j, at):
        here = [at, n - 1 - at, at + 1 - 2 * lax.rem(at, 2)]
        here.append(n - 1 - here[2])
        shard, half = ((0, 0), (0, 1), (1, 0), (1, 1), (2, 0), (3, 0), (2, 1), (3, 1))[j]
        return here[shard], g if half == 0 else 1 - g

    def second_place(j):
        here = [z, e * pz + (1 - e) * mirror, e * far + (1 - e) * pz, e * mirror + (1 - e) * far]
        return here[j // 2], g if j % 2 == 0 else 1 - g

    mine = pl.ds(pl.multiple_of(core * half_rows, 16), half_rows)
    other = pl.ds(pl.multiple_of((1 - core) * half_rows, 16), half_rows)

    def final_copy(phase, j, place, rows):
        there = res.at[phase, rows, columns(place)]
        return remote(there, there, fsend.at[phase], frecv.at[phase * (1 + j)], mate)

    def final_all(phase, rows):
        there = res.at[phase, rows, :]
        return remote(there, there, fsend.at[phase], frecv.at[0], mate)

    def pair_first(j):
        return remote(part0.at[j, 1 - core], rbuf0.at[j], csend.at[0], crecv.at[0, j], mate)

    def x_first(j):
        return remote(xs0.at[j, 0], xr0.at[j], xsend.at[0], xrecv.at[0, j], x_peer)

    kept = pl.ds(pl.multiple_of(side * quarter, 16), quarter)
    given = pl.ds(pl.multiple_of((1 - side) * quarter, 16), quarter)

    def x_guest(j):
        return remote(xs0.at[j, 1, given, :], xg0.at[j], gsend.at[0], grecv.at[j], x_peer)

    def lend_copy(j, at):
        cols = columns(first_place(j, at))
        return remote(lent.at[j], res.at[0, quarter_rows(t), cols], asend.at[1], arecv.at[1 + j], partner)

    def lent_copy(j, lane):
        owner = (t, t, lax.rem(t + 2, n_tp))[lane]
        there = res.at[0, quarter_rows(owner), columns(first_place(j, pz))]
        return remote(
            there, there, qsend.at[3 + lane], qrecv.at[3 + j if lane == 1 else 11 + lane // 2], x_peer if lane == 1 else mate
        )

    def lent_all(lane, owner):
        there = res.at[0, quarter_rows(owner), :]
        return remote(there, there, qsend.at[3 + lane], qrecv.at[11 + lane // 2], mate)

    def lent_arrival(j):
        lane = 1
        owner = lax.rem(t + 2, n_tp)
        there = res.at[0, quarter_rows(owner), columns(first_place(j, pz))]
        return remote(
            there, there, qsend.at[3 + lane], qrecv.at[3 + j if lane == 1 else 11 + lane // 2], x_peer if lane == 1 else mate
        )

    def from_mirror(name, c):
        arrival(name, mirror, c).wait_recv()
        passing(name, mirror, c, partner).start()
        share(name, mirror, c).start()

    def from_far(name, c):
        arrival(name, far, c).wait_recv()
        passing(name, far, c, partner).start()
        share(name, far, c).start()

    def from_partner(name, c):
        arrival(name, pz, c).wait_recv()
        passing(name, pz, c, inward).start()

    def keep_down(s, low):
        for c in range(low, low + 2):
            arrival("down", s, c).wait_recv()
            share("down", s, c).start()

    def down_mirror(c):
        keep_down(mirror, 2 * c)

    def down_far(c):
        keep_down(far, 2 * c)

    def down_partner(c):
        from_partner("down", 2 * c)
        from_partner("down", 2 * c + 1)

    def first_ffn():
        for copy in local:
            copy.wait()
        spread_pool(z)
        norm_rows(tok_ref, gain1_ref)
        tok_copy.wait_recv()
        for off in range(1, n_tp):
            guest_copy(off, t).start()
        from_mirror("pool", 0)
        from_mirror("gu", 0)
        from_mirror("gu", 1)
        from_partner("pool", 0)

        @pl.loop(0, 4)
        def _(m):
            from_mirror("gu", m + 2)
            from_partner("gu", m)

        for off in range(1, n_tp):
            guest_copy(off, lax.rem(t - off + n_tp, n_tp)).wait_recv()
        norm_rows(guest, gain1_ref, n_rows)
        from_mirror("gu", 6)
        from_partner("gu", 4)
        add_shard(0, z, True)
        from_mirror("gu", 7)
        from_partner("gu", 5)
        add_shard(1, z, True)
        from_partner("gu", 6)
        settle("pool", mirror)
        spread_pool(mirror)
        from_far("pool", 0)
        from_far("gu", 0)
        settle("gate", mirror)
        add_shard(0, mirror)
        from_partner("gu", 7)
        pl.loop(0, 8)(lambda c: own_inward("down", c).start())
        from_far("gu", 1)
        settle("up", mirror)
        add_shard(1, mirror)
        from_far("gu", 2)
        settle("pool", far)
        spread_pool(far)
        from_far("gu", 3)
        settle("pool", pz)
        spread_pool(pz)
        from_far("gu", 4)
        from_far("gu", 5)
        settle("gate", far)
        add_shard(0, far)
        from_far("gu", 6)
        settle("gate", pz)
        add_shard(0, pz)
        from_far("gu", 7)
        pl.loop(0, 4)(lambda c: own_partner("down", c).start())
        down_mirror(0)
        down_mirror(1)
        settle("up", far)
        add_shard(1, far)
        settle("up", pz)
        down_mirror(2)
        down_partner(0)
        add_shard(1, pz)

        @pl.loop(0, f_loc // tile)
        def _(i):
            cols = pl.ds(pl.multiple_of(i * tile, tile), tile)

            @pl.loop(0, 2 * n_rows // 128)
            def _(r):
                rows = pl.ds(pl.multiple_of(r * 128, 128), 128)
                hidden[rows, cols] = activate(acc[0, rows, cols], acc[1, rows, cols])

        def multiply(j):
            s, half = first_place(j, z)
            product = jnp.dot(hidden[...], down_full[s, half], preferred_element_type=f32).astype(jnp.bfloat16)
            for seq in range(2):
                for part in range(2):
                    row = seq * n_rows + part * half_rows
                    part0[j, part, seq] = product[row : row + half_rows]
            pair_first(j).start()

        def add_pair(j):
            pair_first(j).wait_recv()
            xs0[j] = (part0[j, core].astype(f32) + rbuf0[j].astype(f32)).astype(jnp.bfloat16)
            x_guest(j).start()
            x_first(j).start()

        def finish(j):
            place = first_place(j, z)
            cols = columns(place)
            x_guest(j).wait_recv()
            total = xs0[j, 1, kept, :].astype(f32) + xg0[j].astype(f32)
            lent[j] = (guest[quarter_rows(t), cols].astype(f32) + 0.5 * total).astype(jnp.bfloat16)
            lend_copy(j, z).start()
            x_first(j).wait_recv()
            total = xs0[j, 0].astype(f32) + xr0[j].astype(f32)
            res[0, mine, cols] = (tok_ref[mine, cols].astype(f32) + 0.5 * total).astype(jnp.bfloat16)
            final_copy(0, j, place, mine).start()

        down_mirror(3)
        down_partner(1)
        multiply(0)
        multiply(1)
        add_pair(0)
        down_far(0)
        down_partner(2)
        add_pair(1)
        settle("down", mirror)
        multiply(2)
        multiply(3)
        add_pair(2)
        down_partner(3)
        down_far(1)
        multiply(4)
        add_pair(3)
        down_far(2)
        add_pair(4)
        finish(0)
        finish(1)
        down_far(3)
        multiply(5)
        finish(2)
        add_pair(5)
        finish(3)
        pl.loop(4, 8)(lambda c: own_partner("down", c).start())
        settle("down", pz)
        multiply(6)
        finish(4)
        add_pair(6)
        settle("down", far)
        multiply(7)
        finish(5)
        add_pair(7)
        finish(6)
        finish(7)
        pl.loop(0, 8)(lambda c: passing("down", mirror, c, partner).start())
        pl.loop(0, 8)(lambda c: passing("down", far, c, partner).start())
        final_all(0, other).wait_recv()

    def take(name, s, c):
        arrival(name, s, c).wait_recv()
        share(name, s, c).start()

    def collect():
        for copy in local:
            copy.wait()
        spread_pool(z)
        for s in (pz, far, mirror):
            take("pool", s, 0)
            pl.loop(0, 8)(lambda m: take("gu", s, m))
            settle("pool", s)
            spread_pool(s)

        def hand_out(j):
            lend_copy(j, pz).wait_recv()
            lent_copy(j, 1).start()
            lent_copy(j, 0).start()

        def hand_on(j):
            lent_arrival(j).wait_recv()
            lent_copy(j, 2).start()

        for j in range(n_blocks):
            if j % 4 == 0:
                pl.loop(j, j + 4)(lambda c: take("down", pz, c))
            hand_out(j)
            if j >= 2:
                hand_on(j - 2)
        hand_on(n_blocks - 2)
        hand_on(n_blocks - 1)
        take("down", far, 0)
        t_mate = t + 1 - 2 * core
        lent_all(0, t_mate).wait_recv()
        lent_all(2, lax.rem(t_mate + 2, n_tp)).wait_recv()

    pl.when(inner)(first_ffn)
    pl.when(outer)(collect)

    def when_outer(act):
        pl.when(outer)(act)

    def take_down(s, low, high):
        @pl.when(outer)
        def _():
            for c in range(low, high):
                take("down", s, c)

    take_down(far, 1, 2)
    norm_rows(res.at[0], gainm_ref)
    take_down(far, 2, 3)
    for off in range(1, n_tp):
        pool_all(off, lax.rem(t - off + n_tp, n_tp)).wait_recv()
    group_width = width // groups
    row_id = lax.broadcasted_iota(jnp.int32, (n_rows, n_rows), 0)
    col_id = lax.broadcasted_iota(jnp.int32, (n_rows, n_rows), 1)
    position = lax.broadcasted_iota(jnp.int32, (n_rows, 1), 0)
    own_seq = pl.ds(0, n_rows)
    for k, span in enumerate(pool_spans):
        low = row_id - span // 2
        band = jnp.where((col_id >= low) & (col_id < low + span), 1.0, 0.0).astype(jnp.bfloat16)
        first = jnp.maximum(position - span // 2, 0)
        last = jnp.minimum(position - span // 2 + span, n_rows)
        inverse = 1.0 / (last - first).astype(f32)
        cols = pl.ds(k * group_width, group_width)
        mean = jnp.dot(band, normed[own_seq, cols], preferred_element_type=f32) * inverse
        deviation = (mean - normed[own_seq, cols].astype(f32)).astype(jnp.bfloat16)
        mapped = jnp.dot(deviation, pool_full[k], preferred_element_type=f32) + bias_ref[pl.ds(k, 1), :]
        amix[:, cols] = (res[0, :, cols].astype(f32) + mapped * scale_ref[:, cols]).astype(jnp.bfloat16)
        if k == 1:
            take_down(far, 3, 4)

    norm_rows(amix, gain2_ref)

    @pl.when(outer)
    def _():
        for s in (pz, far, mirror):
            settle("gate", s)
            settle("up", s)
        take("down", far, 4)

    @pl.loop(0, f_loc // tile)
    def _(i):
        cols = pl.ds(pl.multiple_of(i * tile, tile), tile)
        gate_proj = jnp.dot(normed[own_seq, :], gu_full[0, :, cols], preferred_element_type=f32)
        up_proj = jnp.dot(normed[own_seq, :], gu_full[1, :, cols], preferred_element_type=f32)
        hidden[own_seq, cols] = activate(gate_proj, up_proj)

        @pl.when(outer & (i % 2 == 0))
        def _():
            take("down", far, 5 + i // 2)

    def pair_copy(j):
        return remote(part1.at[j, other, :], rbuf1.at[j], csend.at[1], crecv.at[1, j], mate)

    def x_copy(j):
        return remote(xs1.at[j], xr1.at[j], xsend.at[1], xrecv.at[1, j], x_peer)

    def out_copy(j):
        cols = columns(second_place(j))
        return pltpu.make_async_copy(res.at[1, :, cols], out_ref.at[:, cols], osem.at[0])

    def multiply(j):
        s, half = second_place(j)
        part1[j] = jnp.dot(hidden[own_seq, :], down_full[s, half], preferred_element_type=f32).astype(jnp.bfloat16)
        pair_copy(j).start()

    def add_pair(j):
        pair_copy(j).wait_recv()
        xs1[j] = (part1[j, mine, :].astype(f32) + rbuf1[j].astype(f32)).astype(jnp.bfloat16)
        x_copy(j).start()

    def finish(j):
        x_copy(j).wait_recv()
        place = second_place(j)
        cols = columns(place)
        total = xs1[j].astype(f32) + xr1[j].astype(f32)
        res[1, mine, cols] = (amix[mine, cols].astype(f32) + 0.5 * total).astype(jnp.bfloat16)
        final_copy(1, j, place, mine).start()

    def emit(j):
        final_copy(1, j, second_place(j), other).wait_recv()
        out_copy(j).start()

    def drain_early():
        for off in range(1, n_tp):
            pool_all(off, t).wait_send()
        for name in kinds:
            sent(name, z, g, zsend.at[z], partner).wait_send()

        @pl.when(outer)
        def _():
            tok_copy.wait_send()
            for name in kinds:
                sent(name, z, 1 - g, ysend.at[z], partner).wait_send()
                for s in (pz, far, mirror):
                    if name != "down":
                        sent(name, s, g, ysend.at[s], y_peer).wait_send()
            sent("down", pz, g, ysend.at[pz], y_peer).wait_send()
            for lane in range(3):
                lent_all(lane, t).wait_send()

        @pl.when(inner)
        def _():
            for off in range(1, n_tp):
                guest_copy(off, t).wait_send()
            for name in kinds:
                sent(name, z, g, zleft, inward).wait_send()
                sent(name, pz, g, zsend.at[pz], inward).wait_send()
                for s in (mirror, far):
                    sent(name, s, g, ysend.at[s], y_peer).wait_send()
                    if name != "down":
                        sent(name, s, g, zsend.at[s], partner).wait_send()
            remote(rbuf0, rbuf0, csend.at[0], crecv.at[0, 0], mate).wait_send()
            remote(xr0, xr0, xsend.at[0], xrecv.at[0, 0], x_peer).wait_send()
            remote(xg0, xg0, gsend.at[0], grecv.at[0], x_peer).wait_send()
            remote(lent, lent, asend.at[1], arecv.at[1], partner).wait_send()
            final_all(0, mine).wait_send()

    multiply(0)
    take_down(mirror, 0, 1)
    multiply(1)
    add_pair(0)
    multiply(2)
    add_pair(1)
    take_down(mirror, 1, 2)
    when_outer(lambda: settle("down", pz))
    multiply(3)
    add_pair(2)
    take_down(mirror, 2, 3)
    multiply(4)
    add_pair(3)
    when_outer(lambda: settle("down", far))
    multiply(5)
    add_pair(4)
    take_down(mirror, 3, 4)
    finish(0)
    take_down(mirror, 4, 5)
    finish(1)
    add_pair(5)
    take_down(mirror, 5, 6)
    drain_early()
    finish(2)
    emit(0)
    take_down(mirror, 6, 7)
    finish(3)
    emit(1)
    take_down(mirror, 7, 8)
    multiply(6)
    emit(2)
    finish(4)
    add_pair(6)
    emit(3)
    when_outer(lambda: settle("down", mirror))
    multiply(7)
    finish(5)
    add_pair(7)
    emit(4)
    finish(6)
    emit(5)
    finish(7)
    emit(6)
    emit(7)

    @pl.when(outer)
    def _():
        for s in (far, mirror):
            sent("down", s, g, ysend.at[s], y_peer).wait_send()

    @pl.when(inner)
    def _():
        for s in (mirror, far):
            sent("down", s, g, zsend.at[s], partner).wait_send()

    remote(xr1, xr1, csend.at[1], crecv.at[1, 0], mate).wait_send()
    remote(xr1, xr1, xsend.at[1], xrecv.at[1, 0], x_peer).wait_send()
    final_all(1, mine).wait_send()
    pltpu.make_async_copy(res.at[1], out_ref, osem.at[0]).wait()


def fused_shards(
    n, n_tp, tokens, gate_weight, up_weight, down_weight, pool_weight, pool_bias, pool_scale,
    gain_first, gain_mix, gain_second,
):
    n_rows, width = tokens.shape
    d_loc, f_loc = gate_weight.shape
    groups = pool_weight.shape[1]
    pool = jnp.swapaxes(pool_weight, 0, 1)
    bf16, dma, vmem = jnp.bfloat16, pltpu.SemaphoreType.DMA, pltpu.VMEM
    in_vmem, anywhere = pl.BlockSpec(memory_space=pltpu.VMEM), pl.BlockSpec(memory_space=pl.ANY)
    half, quarter, block, blocks = n_rows // 2, n_rows // n_tp, d_loc // 2, 2 * n
    return pl.pallas_call(
        functools.partial(fused_kernel, (n, n_tp)),
        out_shape=jax.ShapeDtypeStruct((n_rows, width), bf16),
        in_specs=[in_vmem] + [anywhere] * 4 + [in_vmem] * 5,
        out_specs=anywhere,
        scratch_shapes=[
            vmem((2, n * d_loc, f_loc), bf16),
            vmem((n, 2, f_loc, block), bf16),
            vmem((groups, n * pool.shape[1], n_tp * pool.shape[2]), bf16),
            vmem((2, 2 * n_rows, f_loc), jnp.float32),
            vmem((2 * n_rows, width), bf16),
            vmem((2 * n_rows, f_loc), bf16),
            vmem((n_rows, width), bf16),
            vmem((2, n_rows, width), bf16),
            vmem((n_rows, width), bf16),
            vmem((blocks, 2, 2, half, block), bf16),
            vmem((blocks, 2, half, block), bf16),
            vmem((blocks, 2, half, block), bf16),
            vmem((blocks, half, block), bf16),
            vmem((blocks, quarter, block), bf16),
            vmem((blocks, quarter, block), bf16),
            vmem((blocks, n_rows, block), bf16),
            vmem((blocks, half, block), bf16),
            vmem((blocks, half, block), bf16),
            vmem((blocks, half, block), bf16),
            dma((n, 3)), dma((3,)), dma((n - 1, 17)), dma((n, 3)), dma((n - 1, 4)),
            dma((n_tp - 1,)), dma((n_tp - 1,)), dma((5,)),
            dma((2,)), dma((1 + blocks,)), dma((6,)), dma((5 + blocks,)),
            dma((2,)), dma((2, blocks)), dma((2,)), dma((2, blocks)), dma((1,)), dma((blocks,)),
            dma((2,)), dma((1 + blocks,)), dma((1,)),
        ],
        compiler_params=pltpu.CompilerParams(
            collective_id=0, has_side_effects=True, vmem_limit_bytes=60 * 1024 * 1024
        ),
    )(
        tokens, gate_weight, up_weight, down_weight, pool, pool_bias, pool_scale.reshape(1, width),
        gain_first.reshape(1, width), gain_mix.reshape(1, width), gain_second.reshape(1, width),
    )


def layer(n_grp, n, n_tp, *args):
    n_rows, width = args[0].shape
    d_loc, f_loc = args[1].shape
    pool_rows, _, pool_cols = args[4].shape
    fits = n_grp == 2 and n_tp == 4 and n == 4 and n_rows % 64 == 0
    fits = fits and d_loc % 512 == 0 and f_loc % 1280 == 0 and pool_rows % 32 == 0 and pool_cols % 128 == 0
    return fused_shards(n, n_tp, *args) if fits else shards(*args)


def solution(mesh):
    return jax.shard_map(
        functools.partial(layer, mesh.shape["grp"], mesh.shape["fs"], mesh.shape["tp"]),
        mesh=mesh,
        in_specs=(
            P(("grp", "fs"), None),
            P("fs", "tp"),
            P("fs", "tp"),
            P("tp", "fs"),
            P("fs", None, "tp"),
            P(),
            P(),
            P(),
            P(),
            P(),
        ),
        out_specs=P(("grp", "fs"), None),
        check_vma=False,
    )
```

```python
import functools

import jax
import jax.numpy as jnp
from jax import lax
from jax.experimental import pallas as pl
from jax.experimental.pallas import tpu as pltpu
from jax.sharding import PartitionSpec as P

eps = 1e-06
pool_spans = (2, 4, 8, 16)
pad_width = 8
MESH = pl.DeviceIdType.MESH


def rms_scale(values, gain_vec):
    fvalues = values.astype(jnp.float32)
    scaled = fvalues * lax.rsqrt(jnp.mean(fvalues * fvalues, axis=-1, keepdims=True) + eps)
    return (scaled * gain_vec).astype(jnp.bfloat16)


def ffn_hidden(normed, gate_full, up_full):
    gate_proj = jnp.dot(normed, gate_full, preferred_element_type=jnp.float32)
    up_proj = jnp.dot(normed, up_full, preferred_element_type=jnp.float32)
    return (jax.nn.silu(gate_proj) * up_proj).astype(jnp.bfloat16)


def pool_block(padded, offset, seq_len, pool_full, pool_bias, pool_scale):
    n_tokens = padded.shape[0] - 2 * pad_width
    group_width = pool_full.shape[0]
    position = offset + lax.iota(jnp.int32, n_tokens)
    column_pos = offset - pad_width + lax.iota(jnp.int32, padded.shape[0])
    center = padded[pad_width : pad_width + n_tokens].astype(jnp.float32)
    outputs = []
    for group_number, window_span in enumerate(pool_spans):
        low_edge = jnp.clip(position - window_span // 2, 0, seq_len)
        high_edge = jnp.clip(position - window_span // 2 + window_span, 0, seq_len)
        band_mask = (
            (column_pos[None, :] >= low_edge[:, None]) & (column_pos[None, :] < high_edge[:, None])
        ).astype(jnp.bfloat16)
        lower_col = group_number * group_width
        columns = padded[:, lower_col : lower_col + group_width]
        window_sum = jnp.dot(band_mask, columns, preferred_element_type=jnp.float32)
        window_mean = window_sum / (high_edge - low_edge).astype(jnp.float32)[:, None]
        deviation = (window_mean - center[:, lower_col : lower_col + group_width]).astype(
            jnp.bfloat16
        )
        mapped = jnp.dot(
            deviation, pool_full[:, group_number, :], preferred_element_type=jnp.float32
        )
        outputs.append(mapped + pool_bias[group_number])
    return jnp.concatenate(outputs, axis=-1) * pool_scale


def shards(
    tokens,
    gate_weight,
    up_weight,
    down_weight,
    pool_weight,
    pool_bias,
    pool_scale,
    gain_first,
    gain_mix,
    gain_second,
):
    gate_full, up_full, pool_half = (
        lax.all_gather(gate_weight, "fs", axis=0, tiled=True),
        lax.all_gather(up_weight, "fs", axis=0, tiled=True),
        lax.all_gather(pool_weight, "fs", axis=0, tiled=True),
    )
    down_full = lax.all_gather(down_weight, "fs", axis=1, tiled=True)
    pool_full = lax.all_gather(pool_half, "tp", axis=2, tiled=True)
    seq_len = tokens.shape[0]
    first_normed = rms_scale(tokens, gain_first)
    first_hidden = ffn_hidden(first_normed, gate_full, up_full)
    second_gate, second_up, second_down = (gate_full, up_full, down_full)
    first_branch = lax.psum(
        jnp.dot(first_hidden, down_full, preferred_element_type=jnp.float32).astype(jnp.bfloat16),
        "tp",
    ).astype(jnp.float32)
    after_first = (tokens.astype(jnp.float32) + 0.5 * first_branch).astype(jnp.bfloat16)
    mix_normed = rms_scale(after_first, gain_mix)
    padded = jnp.pad(mix_normed, ((pad_width, pad_width), (0, 0)))
    mixed = pool_block(padded, 0, seq_len, pool_full, pool_bias, pool_scale)
    after_mix = (after_first.astype(jnp.float32) + mixed).astype(jnp.bfloat16)
    second_normed = rms_scale(after_mix, gain_second)
    second_hidden = ffn_hidden(second_normed, second_gate, second_up)
    second_branch = lax.psum(
        jnp.dot(second_hidden, second_down, preferred_element_type=jnp.float32).astype(
            jnp.bfloat16
        ),
        "tp",
    ).astype(jnp.float32)
    return (after_mix.astype(jnp.float32) + 0.5 * second_branch).astype(jnp.bfloat16)


def fused_kernel(
    sizes, tok_hbm, gate_ref, up_ref, down_ref, pool_hbm, bias_hbm, scale_hbm, gain1_hbm, gainm_hbm, gain2_hbm,
    out_ref,
    gu_full, down_full, pool_full, acc, normed, hidden, amix, res, guest, part0, rbuf0, xs0, xr0, xg0, lent,
    part1, rbuf1, xs1, xr1, tok_ref, pool_ref, bias_ref, scale_ref, gain1_ref, gainm_ref, gain2_ref,
    zsend, zleft, zrecv, ysend, yrecv, tsend, trecv, lsem, asend, arecv, qsend, qrecv,
    csend, crecv, xsend, xrecv, gsend, grecv, fsend, frecv, osem,
):
    n, n_tp = sizes
    g, z, t = lax.axis_index("grp"), lax.axis_index("fs"), lax.axis_index("tp")
    core, side = lax.rem(t, 2), t // 2
    outer = (z == 0) | (z == n - 1)
    inner = (z > 0) & (z < n - 1)
    e = 1 - jnp.minimum(z, 1) * jnp.minimum(n - 1 - z, 1)
    pz = z + 1 - 2 * lax.rem(z, 2)
    mirror, far = n - 1 - z, n - 1 - pz
    y_peer, partner, inward = {"grp": 1 - g}, {"fs": pz}, {"fs": mirror}
    mate, x_peer = {"tp": t + 1 - 2 * core}, {"tp": lax.rem(t + 2, n_tp)}
    n_rows, width = tok_hbm.shape
    d_loc, f_loc = gate_ref.shape
    pool_rows, groups, pool_cols = pool_hbm.shape
    half_rows = n_rows // 2
    quarter = n_rows // n_tp
    block_cols = d_loc // 2
    sub_cols = block_cols // 2
    n_blocks = 2 * n
    f32 = jnp.float32

    def remote(src, dst, s_sem, r_sem, dev):
        return pltpu.make_async_remote_copy(
            src_ref=src, dst_ref=dst, send_sem=s_sem, recv_sem=r_sem, device_id=dev, device_id_type=MESH
        )

    barrier = pltpu.get_barrier_semaphore()

    def greet(dev):
        pl.semaphore_signal(barrier, inc=1, device_id=dev, device_id_type=MESH)

    greet(y_peer)
    greet(partner)
    for off in range(1, n_tp):
        greet({"tp": lax.rem(t + off, n_tp)})

    @pl.when(inner)
    def _():
        greet(inward)

    pl.semaphore_wait(barrier, n_tp + 2 - e)

    counts = {"pool": 1, "gu": 8, "down": 8}
    first_key = {"pool": 0, "gu": 1, "down": 9}

    def each(name, act):
        if counts[name] == 1:
            act(0)
        else:
            pl.loop(0, counts[name])(act)

    kind = {"pool": 0, "gu": 1, "down": 2}

    def key(name, c):
        return first_key[name] + c

    def slot(s, at):
        return lax.rem(s - at + n, n) - 1

    def bulk(name, c):
        return 0 if name == "pool" else (3 if name == "down" else 1) + c // 4

    def region(name, s, half, c):
        if name == "down":
            size = f_loc // 4
            rows = pl.ds(pl.multiple_of(lax.rem(c, 4) * size, 16), size)
            return down_full.at[s, half, rows, pl.ds(pl.multiple_of(c // 4 * sub_cols, 128), sub_cols)]
        if name == "pool":
            size = pool_rows // 2
            rows = pl.ds(pl.multiple_of(s * pool_rows + half * size, 16), size)
            return pool_full.at[:, rows, pl.ds(pl.multiple_of(t * pool_cols, 128), pool_cols)]
        size = d_loc // 8
        rows = pl.ds(pl.multiple_of(s * d_loc + half * (d_loc // 2) + lax.rem(c, 4) * size, 16), size)
        return gu_full.at[c // 4, rows, :]

    def whole(name, s, half):
        if name == "down":
            return down_full.at[s, half]
        if name == "pool":
            return region(name, s, half, 0)
        rows = pl.ds(pl.multiple_of(s * d_loc + half * (d_loc // 2), 16), d_loc // 2)
        return gu_full.at[:, rows, :] if name == "gu" else gu_full.at[0 if name == "gate" else 1, rows, :]

    def source(name, half, c):
        if name == "down":
            size = f_loc // 4
            cols = pl.ds(pl.multiple_of(half * block_cols + c // 4 * sub_cols, 128), sub_cols)
            return down_ref.at[pl.ds(pl.multiple_of(lax.rem(c, 4) * size, 16), size), cols]
        if name == "pool":
            return region(name, z, half, c)
        size = d_loc // 8
        rows = pl.ds(pl.multiple_of(half * (d_loc // 2) + c * size, 16), size)
        return {"gate": gate_ref, "up": up_ref}[name].at[rows, :]

    def own_copy(name, c, half, s_sem, r_sem, dev):
        base = {"gate": 0, "up": 4}.get(name)
        name_of, at = ("gu", base + c) if base is not None else (name, c)
        where = region(name_of, z, half, at)
        return remote(source(name, half, c), where, s_sem.at[kind[name_of]], r_sem(name_of, at), dev)

    def own_partner(name, c):
        return own_copy(name, c, g, zsend.at[z], lambda nm, at: zrecv.at[slot(z, pz), key(nm, at)], partner)

    def own_inward(name, c):
        return own_copy(name, c, g, zleft, lambda nm, at: zrecv.at[slot(z, mirror), key(nm, at)], inward)

    def own_direct(name, c):
        return own_copy(name, c, 1 - g, ysend.at[z], lambda nm, at: yrecv.at[slot(z, pz), bulk(nm, at)], partner)

    def passing(name, s, c, dev):
        there = region(name, s, g, c)
        to = pz if dev is partner else mirror
        return remote(there, there, zsend.at[s, kind[name]], zrecv.at[slot(s, to), key(name, c)], dev)

    def arrival(name, s, c):
        there = region(name, s, g, c)
        return remote(there, there, zsend.at[s, kind[name]], zrecv.at[slot(s, z), key(name, c)], partner)

    def share(name, s, c):
        there = region(name, s, g, c)
        return remote(there, there, ysend.at[s, kind[name]], yrecv.at[slot(s, z), bulk(name, c)], y_peer)

    def settle(name, s):
        if name == "down":
            settle_down(s, 0)
            settle_down(s, 1)
            return
        there = whole(name, s, 1 - g)
        where = {"pool": 0, "gate": 1, "up": 2}[name]
        remote(there, there, ysend.at[s, 0], yrecv.at[slot(s, z), where], y_peer).wait_recv()

    def settle_down(s, part):
        there = down_full.at[s, 1 - g, :, pl.ds(part * sub_cols, sub_cols)]
        remote(there, there, ysend.at[s, 0], yrecv.at[slot(s, z), 3 + part], y_peer).wait_recv()

    def sent(name, s, half, sems, dev):
        there = whole(name, s, half)
        return remote(there, there, sems.at[kind[name]], yrecv.at[0, 0], dev)

    kinds = ("pool", "gu", "down")

    def quarter_rows(tt):
        return pl.ds(pl.multiple_of((lax.rem(tt, 2) * (n_tp // 2) + tt // 2) * quarter, 16), quarter)

    own_counts = {"pool": 1, "gate": 4, "up": 4, "down": 8}

    def start_each(names, make):
        for name in names:
            pl.loop(0, own_counts[name])(lambda c: make(name, c).start())

    tok_copy = remote(
        tok_hbm.at[quarter_rows(t), :], guest.at[quarter_rows(t), :], asend.at[0], arecv.at[0], partner
    )

    own_rows = pl.ds(pl.multiple_of(z * d_loc, 128), d_loc)
    pool_in = pltpu.make_async_copy(pool_hbm, pool_ref, lsem.at[0])
    local = [
        pltpu.make_async_copy(tok_hbm, tok_ref, lsem.at[1]),
        pltpu.make_async_copy(gate_ref, gu_full.at[0, own_rows, :], lsem.at[2]),
        pltpu.make_async_copy(up_ref, gu_full.at[1, own_rows, :], lsem.at[3]),
        pltpu.make_async_copy(down_ref.at[:, pl.ds(0, block_cols)], down_full.at[z, 0], lsem.at[4]),
        pltpu.make_async_copy(down_ref.at[:, pl.ds(block_cols, block_cols)], down_full.at[z, 1], lsem.at[5]),
        pltpu.make_async_copy(bias_hbm, bias_ref, lsem.at[6]),
        pltpu.make_async_copy(scale_hbm, scale_ref, lsem.at[7]),
        pltpu.make_async_copy(gain1_hbm, gain1_ref, lsem.at[8]),
        pltpu.make_async_copy(gainm_hbm, gainm_ref, lsem.at[9]),
        pltpu.make_async_copy(gain2_hbm, gain2_ref, lsem.at[10]),
    ]
    pool_in.start()

    @pl.when(outer)
    def _():
        tok_copy.start()
        start_each(("gate", "up"), own_partner)

    @pl.when(inner)
    def _():
        for name in ("gate", "up"):

            @pl.loop(0, 4)
            def _(c):
                own_inward(name, c).start()
                own_partner(name, c).start()

    for copy in local:
        copy.start()
    pool_in.wait()
    for k in range(groups):
        pool_full[
            k, pl.ds(pl.multiple_of(z * pool_rows, 16), pool_rows), pl.ds(pl.multiple_of(t * pool_cols, 128), pool_cols)
        ] = pool_ref[:, k, :]
    own_partner("pool", 0).start()

    @pl.when(outer)
    def _():
        start_each(("gate", "up", "pool"), own_direct)
        start_each(("down",), own_partner)
        start_each(("down",), own_direct)

    @pl.when(inner)
    def _():
        own_inward("pool", 0).start()

    def norm_rows(src, gain, base=0):
        @pl.loop(0, n_rows // 32)
        def _(r):
            values = src[pl.ds(pl.multiple_of(r * 32, 32), 32), :].astype(f32)
            scaled = values * lax.rsqrt(jnp.mean(values * values, axis=-1, keepdims=True) + eps)
            normed[pl.ds(pl.multiple_of(base + r * 32, 32), 32), :] = (scaled * gain[...]).astype(jnp.bfloat16)

    tile = 256

    def add_shard(w, s, first=False):
        k_cols = pl.ds(pl.multiple_of(s * d_loc, 128), d_loc)

        @pl.loop(0, f_loc // tile)
        def _(i):
            cols = pl.ds(pl.multiple_of(i * tile, tile), tile)
            product = jnp.dot(normed[:, k_cols], gu_full[w, k_cols, cols], preferred_element_type=f32)
            acc[w, :, cols] = product if first else acc[w, :, cols] + product

    def pool_copy(off, s, sender):
        cols = pl.ds(pl.multiple_of(sender * pool_cols, 128), pool_cols)
        there = pool_full.at[:, pl.ds(pl.multiple_of(s * pool_rows, 16), pool_rows), cols]
        return remote(there, there, tsend.at[off - 1], trecv.at[off - 1], {"tp": lax.rem(t + off, n_tp)})

    def pool_all(off, sender):
        there = pool_full.at[:, :, pl.ds(pl.multiple_of(sender * pool_cols, 128), pool_cols)]
        return remote(there, there, tsend.at[off - 1], trecv.at[off - 1], {"tp": lax.rem(t + off, n_tp)})

    def spread_pool(s):
        for off in range(1, n_tp):
            pool_copy(off, s, t).start()

    def activate(gate_proj, up_proj):
        return (gate_proj / (1.0 + jnp.exp(-gate_proj)) * up_proj).astype(jnp.bfloat16)

    def guest_copy(off, sender):
        there = guest.at[quarter_rows(sender), :]
        return remote(there, there, qsend.at[off - 1], qrecv.at[off - 1], {"tp": lax.rem(t + off, n_tp)})

    def columns(place):
        s, half = place
        return pl.ds(pl.multiple_of(s * d_loc + half * block_cols, 128), block_cols)

    def first_place(j, at):
        here = [at, n - 1 - at, at + 1 - 2 * lax.rem(at, 2)]
        here.append(n - 1 - here[2])
        shard, half = ((0, 0), (0, 1), (1, 0), (1, 1), (2, 0), (3, 0), (2, 1), (3, 1))[j]
        return here[shard], g if half == 0 else 1 - g

    def second_place(j):
        here = [z, e * pz + (1 - e) * mirror, e * far + (1 - e) * pz, e * mirror + (1 - e) * far]
        return here[j // 2], g if j % 2 == 0 else 1 - g

    mine = pl.ds(pl.multiple_of(core * half_rows, 16), half_rows)
    other = pl.ds(pl.multiple_of((1 - core) * half_rows, 16), half_rows)

    def final_copy(phase, j, place, rows):
        there = res.at[phase, rows, columns(place)]
        return remote(there, there, fsend.at[phase], frecv.at[0], mate)

    def final_all(phase, rows):
        there = res.at[phase, rows, :]
        return remote(there, there, fsend.at[phase], frecv.at[0], mate)

    def pair_first(j):
        return remote(part0.at[j, 1 - core], rbuf0.at[j], csend.at[0], crecv.at[0, j], mate)

    def x_first(j):
        return remote(xs0.at[j, 0], xr0.at[j], xsend.at[0], xrecv.at[0, j], x_peer)

    kept = pl.ds(pl.multiple_of(side * quarter, 16), quarter)
    given = pl.ds(pl.multiple_of((1 - side) * quarter, 16), quarter)

    def x_guest(j):
        return remote(xs0.at[j, 1, given, :], xg0.at[j], gsend.at[0], grecv.at[j], x_peer)

    def lend_copy(j, at):
        cols = columns(first_place(j, at))
        return remote(lent.at[j], res.at[0, quarter_rows(t), cols], asend.at[1], arecv.at[1 + j], partner)

    def lent_copy(j, lane):
        owner = (t, t, lax.rem(t + 2, n_tp))[lane]
        there = res.at[0, quarter_rows(owner), columns(first_place(j, pz))]
        return remote(
            there, there, qsend.at[3 + lane], qrecv.at[3 + j if lane == 1 else 11 + lane // 2], x_peer if lane == 1 else mate
        )

    def lent_all(lane, owner):
        there = res.at[0, quarter_rows(owner), :]
        return remote(there, there, qsend.at[3 + lane], qrecv.at[11 + lane // 2], mate)

    def lent_arrival(j):
        lane = 1
        owner = lax.rem(t + 2, n_tp)
        there = res.at[0, quarter_rows(owner), columns(first_place(j, pz))]
        return remote(
            there, there, qsend.at[3 + lane], qrecv.at[3 + j if lane == 1 else 11 + lane // 2], x_peer if lane == 1 else mate
        )

    def from_mirror(name, c):
        arrival(name, mirror, c).wait_recv()
        passing(name, mirror, c, partner).start()
        share(name, mirror, c).start()

    def from_far(name, c):
        arrival(name, far, c).wait_recv()
        passing(name, far, c, partner).start()
        share(name, far, c).start()

    def from_partner(name, c):
        arrival(name, pz, c).wait_recv()
        passing(name, pz, c, inward).start()

    def keep_down(s, low):
        for c in range(low, low + 2):
            arrival("down", s, c).wait_recv()
            share("down", s, c).start()

    def down_mirror(c):
        keep_down(mirror, 2 * c)

    def down_far(c):
        keep_down(far, 2 * c)

    def down_partner(c):
        from_partner("down", 2 * c)
        from_partner("down", 2 * c + 1)

    def first_ffn():
        for copy in local:
            copy.wait()
        spread_pool(z)
        norm_rows(tok_ref, gain1_ref)
        tok_copy.wait_recv()
        for off in range(1, n_tp):
            guest_copy(off, t).start()
        from_mirror("gu", 0)
        from_mirror("gu", 1)

        @pl.loop(0, 4)
        def _(m):
            from_mirror("gu", m + 2)
            from_partner("gu", m)

        for off in range(1, n_tp):
            guest_copy(off, lax.rem(t - off + n_tp, n_tp)).wait_recv()
        norm_rows(guest, gain1_ref, n_rows)
        from_mirror("gu", 6)
        from_partner("gu", 4)
        add_shard(0, z, True)
        from_mirror("gu", 7)
        from_partner("gu", 5)
        add_shard(1, z, True)
        from_mirror("pool", 0)
        from_partner("gu", 6)
        from_far("gu", 0)
        settle("gate", mirror)
        add_shard(0, mirror)
        from_partner("gu", 7)
        from_partner("pool", 0)
        pl.loop(0, 8)(lambda c: own_inward("down", c).start())
        from_far("gu", 1)
        settle("up", mirror)
        add_shard(1, mirror)
        from_far("gu", 2)
        settle("pool", mirror)
        spread_pool(mirror)
        from_far("gu", 3)
        from_far("gu", 4)
        from_far("gu", 5)
        settle("gate", far)
        add_shard(0, far)
        from_far("gu", 6)
        settle("gate", pz)
        add_shard(0, pz)
        from_far("gu", 7)
        from_far("pool", 0)
        pl.loop(0, 4)(lambda c: own_partner("down", c).start())
        down_mirror(0)
        down_mirror(1)
        settle("pool", far)
        spread_pool(far)
        settle("up", far)
        add_shard(1, far)
        settle("up", pz)
        down_mirror(2)
        down_partner(0)
        add_shard(1, pz)

        @pl.loop(0, f_loc // tile)
        def _(i):
            cols = pl.ds(pl.multiple_of(i * tile, tile), tile)

            @pl.loop(0, 2 * n_rows // 128)
            def _(r):
                rows = pl.ds(pl.multiple_of(r * 128, 128), 128)
                hidden[rows, cols] = activate(acc[0, rows, cols], acc[1, rows, cols])

        def multiply(j):
            s, half = first_place(j, z)
            product = jnp.dot(hidden[...], down_full[s, half], preferred_element_type=f32).astype(jnp.bfloat16)
            for seq in range(2):
                for part in range(2):
                    row = seq * n_rows + part * half_rows
                    part0[j, part, seq] = product[row : row + half_rows]
            pair_first(j).start()

        def add_pair(j):
            pair_first(j).wait_recv()
            xs0[j] = (part0[j, core].astype(f32) + rbuf0[j].astype(f32)).astype(jnp.bfloat16)
            x_guest(j).start()
            x_first(j).start()

        def lend(j):
            x_guest(j).wait_recv()
            total = xs0[j, 1, kept, :].astype(f32) + xg0[j].astype(f32)
            cols = columns(first_place(j, z))
            lent[j] = (guest[quarter_rows(t), cols].astype(f32) + 0.5 * total).astype(jnp.bfloat16)
            lend_copy(j, z).start()

        def keep(j):
            x_first(j).wait_recv()
            place = first_place(j, z)
            cols = columns(place)
            total = xs0[j, 0].astype(f32) + xr0[j].astype(f32)
            res[0, mine, cols] = (tok_ref[mine, cols].astype(f32) + 0.5 * total).astype(jnp.bfloat16)
            final_copy(0, j, place, mine).start()

        def finish(j):
            lend(j)
            keep(j)

        down_mirror(3)
        down_partner(1)
        multiply(0)
        multiply(1)
        add_pair(0)
        down_far(0)
        down_partner(2)
        add_pair(1)
        settle("down", mirror)
        multiply(2)
        multiply(3)
        add_pair(2)
        down_partner(3)
        down_far(1)
        multiply(4)
        add_pair(3)
        down_far(2)
        add_pair(4)
        finish(0)
        finish(1)
        down_far(3)
        multiply(5)
        finish(2)
        add_pair(5)
        finish(3)
        settle("down", pz)
        multiply(6)
        finish(4)
        pl.loop(4, 6)(lambda c: own_partner("down", c).start())
        add_pair(6)
        settle("down", far)
        multiply(7)
        lend(5)
        add_pair(7)
        settle("pool", pz)
        spread_pool(pz)
        keep(5)
        lend(6)
        lend(7)
        pl.loop(6, 8)(lambda c: own_partner("down", c).start())
        pl.loop(0, 8)(lambda c: passing("down", mirror, c, partner).start())
        pl.loop(0, 8)(lambda c: passing("down", far, c, partner).start())
        keep(6)
        keep(7)
        final_all(0, other).wait_recv()

    def take(name, s, c):
        arrival(name, s, c).wait_recv()
        share(name, s, c).start()

    def collect():
        for copy in local:
            copy.wait()
        spread_pool(z)
        shards_in = (pz, far, mirror)
        for i, s in enumerate(shards_in):
            pl.loop(0, 8)(lambda m: take("gu", s, m))
            take("pool", s, 0)
            if i > 0:
                settle("pool", shards_in[i - 1])
                spread_pool(shards_in[i - 1])

        def hand_out(j):
            lend_copy(j, pz).wait_recv()
            lent_copy(j, 1).start()
            lent_copy(j, 0).start()

        def hand_on(j):
            lent_arrival(j).wait_recv()
            lent_copy(j, 2).start()

        pl.loop(0, 3)(lambda c: take("down", pz, c))
        settle("pool", mirror)
        spread_pool(mirror)
        take("down", pz, 3)
        for j in range(5):
            hand_out(j)
        pl.loop(4, 6)(lambda c: take("down", pz, c))
        for j in range(4):
            hand_on(j)
        hand_out(5)
        hand_on(4)
        hand_out(6)
        hand_out(7)
        hand_on(5)
        hand_on(6)
        take("down", pz, 6)
        hand_on(7)
        take("down", pz, 7)
        t_mate = t + 1 - 2 * core
        lent_all(0, t_mate).wait_recv()
        lent_all(2, lax.rem(t_mate + 2, n_tp)).wait_recv()

    pl.when(inner)(first_ffn)
    pl.when(outer)(collect)

    def when_outer(act):
        pl.when(outer)(act)

    def take_down(s, low, high):
        @pl.when(outer)
        def _():
            for c in range(low, high):
                take("down", s, c)

    norm_rows(res.at[0], gainm_ref)
    take_down(far, 0, 1)
    for off in range(1, n_tp):
        pool_all(off, lax.rem(t - off + n_tp, n_tp)).wait_recv()
    group_width = width // groups
    row_id = lax.broadcasted_iota(jnp.int32, (n_rows, n_rows), 0)
    col_id = lax.broadcasted_iota(jnp.int32, (n_rows, n_rows), 1)
    position = lax.broadcasted_iota(jnp.int32, (n_rows, 1), 0)
    own_seq = pl.ds(0, n_rows)
    for k, span in enumerate(pool_spans):
        low = row_id - span // 2
        band = jnp.where((col_id >= low) & (col_id < low + span), 1.0, 0.0).astype(jnp.bfloat16)
        first = jnp.maximum(position - span // 2, 0)
        last = jnp.minimum(position - span // 2 + span, n_rows)
        inverse = 1.0 / (last - first).astype(f32)
        cols = pl.ds(k * group_width, group_width)
        mean = jnp.dot(band, normed[own_seq, cols], preferred_element_type=f32) * inverse
        deviation = (mean - normed[own_seq, cols].astype(f32)).astype(jnp.bfloat16)
        mapped = jnp.dot(deviation, pool_full[k], preferred_element_type=f32) + bias_ref[pl.ds(k, 1), :]
        amix[:, cols] = (res[0, :, cols].astype(f32) + mapped * scale_ref[:, cols]).astype(jnp.bfloat16)
        if k % 2 == 1:
            take_down(far, 1 + k // 2, 2 + k // 2)

    norm_rows(amix, gain2_ref)

    @pl.when(outer)
    def _():
        for s in (pz, far, mirror):
            settle("gate", s)
            settle("up", s)
        take("down", far, 3)

    @pl.loop(0, f_loc // tile)
    def _(i):
        cols = pl.ds(pl.multiple_of(i * tile, tile), tile)
        gate_proj = jnp.dot(normed[own_seq, :], gu_full[0, :, cols], preferred_element_type=f32)
        up_proj = jnp.dot(normed[own_seq, :], gu_full[1, :, cols], preferred_element_type=f32)
        hidden[own_seq, cols] = activate(gate_proj, up_proj)

        @pl.when(outer & (i % 2 == 1))
        def _():
            take("down", far, 4 + i // 2)

    def spot(b):
        place, wide = second_place(min(b, n_blocks - 1)), b < n_blocks - 1
        off = 0 if wide else (b - n_blocks + 1) * sub_cols
        size = block_cols if wide else sub_cols
        cols = pl.ds(pl.multiple_of(place[0] * d_loc + place[1] * block_cols + off, 128), size)
        return min(b, n_blocks - 1), place, cols, pl.ds(off, size)

    def pair_copy(b):
        j, _, _, lanes = spot(b)
        return remote(part1.at[j, other, lanes], rbuf1.at[j, :, lanes], csend.at[1], crecv.at[1, b], mate)

    def x_copy(b):
        j, _, _, lanes = spot(b)
        return remote(xs1.at[j, :, lanes], xr1.at[j, :, lanes], xsend.at[1], xrecv.at[1, b], x_peer)

    def last_copy(b, rows):
        there = res.at[1, rows, spot(b)[2]]
        return remote(there, there, fsend.at[1], frecv.at[1 + b], mate)

    def multiply(b):
        j, (s, half), _, lanes = spot(b)
        product = jnp.dot(hidden[own_seq, :], down_full[s, half, :, lanes], preferred_element_type=f32)
        part1[j, :, lanes] = product.astype(jnp.bfloat16)
        pair_copy(b).start()

    def add_pair(b):
        j, _, _, lanes = spot(b)
        pair_copy(b).wait_recv()
        xs1[j, :, lanes] = (part1[j, mine, lanes].astype(f32) + rbuf1[j, :, lanes].astype(f32)).astype(jnp.bfloat16)
        x_copy(b).start()

    def finish(b):
        j, _, cols, lanes = spot(b)
        x_copy(b).wait_recv()
        total = xs1[j, :, lanes].astype(f32) + xr1[j, :, lanes].astype(f32)
        res[1, mine, cols] = (amix[mine, cols].astype(f32) + 0.5 * total).astype(jnp.bfloat16)
        last_copy(b, mine).start()

    def emit(b):
        cols = spot(b)[2]
        last_copy(b, other).wait_recv()
        pltpu.make_async_copy(res.at[1, :, cols], out_ref.at[:, cols], osem.at[0]).start()

    def drain_early():
        for off in range(1, n_tp):
            pool_all(off, t).wait_send()
        for name in kinds:
            sent(name, z, g, zsend.at[z], partner).wait_send()

        @pl.when(outer)
        def _():
            tok_copy.wait_send()
            for name in kinds:
                sent(name, z, 1 - g, ysend.at[z], partner).wait_send()
                for s in (pz, far, mirror):
                    if name != "down":
                        sent(name, s, g, ysend.at[s], y_peer).wait_send()
            sent("down", pz, g, ysend.at[pz], y_peer).wait_send()
            for lane in range(3):
                lent_all(lane, t).wait_send()

        @pl.when(inner)
        def _():
            for off in range(1, n_tp):
                guest_copy(off, t).wait_send()
            for name in kinds:
                sent(name, z, g, zleft, inward).wait_send()
                sent(name, pz, g, zsend.at[pz], inward).wait_send()
                for s in (mirror, far):
                    sent(name, s, g, ysend.at[s], y_peer).wait_send()
                    if name != "down":
                        sent(name, s, g, zsend.at[s], partner).wait_send()
            remote(rbuf0, rbuf0, csend.at[0], crecv.at[0, 0], mate).wait_send()
            remote(xr0, xr0, xsend.at[0], xrecv.at[0, 0], x_peer).wait_send()
            remote(xg0, xg0, gsend.at[0], grecv.at[0], x_peer).wait_send()
            remote(lent, lent, asend.at[1], arecv.at[1], partner).wait_send()
            final_all(0, mine).wait_send()

    multiply(0)
    take_down(far, 6, 7)
    multiply(1)
    add_pair(0)
    multiply(2)
    add_pair(1)
    take_down(far, 7, 8)
    when_outer(lambda: settle("down", pz))
    multiply(3)
    add_pair(2)
    multiply(4)
    add_pair(3)
    take_down(mirror, 0, 1)
    add_pair(4)
    take_down(mirror, 1, 3)
    when_outer(lambda: settle("down", far))
    multiply(5)
    take_down(mirror, 3, 4)
    add_pair(5)
    finish(0)
    take_down(mirror, 4, 5)
    drain_early()
    finish(1)
    emit(0)
    take_down(mirror, 5, 6)
    finish(2)
    emit(1)
    take_down(mirror, 6, 7)
    finish(3)
    emit(2)
    take_down(mirror, 7, 8)
    multiply(6)
    emit(3)
    add_pair(6)
    finish(4)
    when_outer(lambda: settle_down(mirror, 0))
    multiply(7)
    finish(5)
    add_pair(7)
    emit(4)
    when_outer(lambda: settle_down(mirror, 1))
    multiply(8)
    finish(6)
    add_pair(8)
    emit(5)
    finish(7)
    emit(6)
    finish(8)
    emit(7)
    emit(8)

    @pl.when(outer)
    def _():
        for s in (far, mirror):
            sent("down", s, g, ysend.at[s], y_peer).wait_send()

    @pl.when(inner)
    def _():
        for s in (mirror, far):
            sent("down", s, g, zsend.at[s], partner).wait_send()

    remote(xr1, xr1, csend.at[1], crecv.at[1, 0], mate).wait_send()
    remote(xr1, xr1, xsend.at[1], xrecv.at[1, 0], x_peer).wait_send()
    final_all(1, mine).wait_send()
    pltpu.make_async_copy(res.at[1], out_ref, osem.at[0]).wait()


def fused_shards(
    n, n_tp, tokens, gate_weight, up_weight, down_weight, pool_weight, pool_bias, pool_scale,
    gain_first, gain_mix, gain_second,
):
    n_rows, width = tokens.shape
    d_loc, f_loc = gate_weight.shape
    pool_rows, groups, pool_cols = pool_weight.shape
    bf16, dma, vmem = jnp.bfloat16, pltpu.SemaphoreType.DMA, pltpu.VMEM
    anywhere = pl.BlockSpec(memory_space=pl.ANY)
    half, quarter, block, blocks = n_rows // 2, n_rows // n_tp, d_loc // 2, 2 * n
    return pl.pallas_call(
        functools.partial(fused_kernel, (n, n_tp)),
        out_shape=jax.ShapeDtypeStruct((n_rows, width), bf16),
        in_specs=[anywhere] * 10,
        out_specs=anywhere,
        scratch_shapes=[
            vmem((2, n * d_loc, f_loc), bf16),
            vmem((n, 2, f_loc, block), bf16),
            vmem((groups, n * pool_rows, n_tp * pool_cols), bf16),
            vmem((2, 2 * n_rows, f_loc), jnp.float32),
            vmem((2 * n_rows, width), bf16),
            vmem((2 * n_rows, f_loc), bf16),
            vmem((n_rows, width), bf16),
            vmem((2, n_rows, width), bf16),
            vmem((n_rows, width), bf16),
            vmem((blocks, 2, 2, half, block), bf16),
            vmem((blocks, 2, half, block), bf16),
            vmem((blocks, 2, half, block), bf16),
            vmem((blocks, half, block), bf16),
            vmem((blocks, quarter, block), bf16),
            vmem((blocks, quarter, block), bf16),
            vmem((blocks, n_rows, block), bf16),
            vmem((blocks, half, block), bf16),
            vmem((blocks, half, block), bf16),
            vmem((blocks, half, block), bf16),
            vmem((n_rows, width), bf16),
            vmem((pool_rows, groups, pool_cols), bf16),
            vmem(pool_bias.shape, jnp.float32),
            vmem((1, width), jnp.float32),
            vmem((1, width), jnp.float32),
            vmem((1, width), jnp.float32),
            vmem((1, width), jnp.float32),
            dma((n, 3)), dma((3,)), dma((n - 1, 17)), dma((n, 3)), dma((n - 1, 5)),
            dma((n_tp - 1,)), dma((n_tp - 1,)), dma((11,)),
            dma((2,)), dma((1 + blocks,)), dma((6,)), dma((5 + blocks,)),
            dma((2,)), dma((2, blocks + 1)), dma((2,)), dma((2, blocks + 1)), dma((1,)), dma((blocks,)),
            dma((2,)), dma((2 + blocks,)), dma((1,)),
        ],
        compiler_params=pltpu.CompilerParams(
            collective_id=0, has_side_effects=True, vmem_limit_bytes=60 * 1024 * 1024
        ),
    )(
        tokens, gate_weight, up_weight, down_weight, pool_weight, pool_bias, pool_scale.reshape(1, width),
        gain_first.reshape(1, width), gain_mix.reshape(1, width), gain_second.reshape(1, width),
    )


def layer(n_grp, n, n_tp, *args):
    n_rows, width = args[0].shape
    d_loc, f_loc = args[1].shape
    pool_rows, _, pool_cols = args[4].shape
    fits = n_grp == 2 and n_tp == 4 and n == 4 and n_rows % 64 == 0
    fits = fits and d_loc % 512 == 0 and f_loc % 1280 == 0 and pool_rows % 32 == 0 and pool_cols % 128 == 0
    return fused_shards(n, n_tp, *args) if fits else shards(*args)


def solution(mesh):
    return jax.shard_map(
        functools.partial(layer, mesh.shape["grp"], mesh.shape["fs"], mesh.shape["tp"]),
        mesh=mesh,
        in_specs=(
            P(("grp", "fs"), None),
            P("fs", "tp"),
            P("fs", "tp"),
            P("tp", "fs"),
            P("fs", None, "tp"),
            P(),
            P(),
            P(),
            P(),
            P(),
        ),
        out_specs=P(("grp", "fs"), None),
        check_vma=False,
    )
```

```python
import functools

import jax
import jax.numpy as jnp
from jax import lax
from jax.experimental import pallas as pl
from jax.experimental.pallas import tpu as pltpu
from jax.sharding import PartitionSpec as P

eps = 1e-06
pool_spans = (2, 4, 8, 16)
pad_width = 8
MESH = pl.DeviceIdType.MESH


def rms_scale(values, gain_vec):
    fvalues = values.astype(jnp.float32)
    scaled = fvalues * lax.rsqrt(jnp.mean(fvalues * fvalues, axis=-1, keepdims=True) + eps)
    return (scaled * gain_vec).astype(jnp.bfloat16)


def ffn_hidden(normed, gate_full, up_full):
    gate_proj = jnp.dot(normed, gate_full, preferred_element_type=jnp.float32)
    up_proj = jnp.dot(normed, up_full, preferred_element_type=jnp.float32)
    return (jax.nn.silu(gate_proj) * up_proj).astype(jnp.bfloat16)


def pool_block(padded, offset, seq_len, pool_full, pool_bias, pool_scale):
    n_tokens = padded.shape[0] - 2 * pad_width
    group_width = pool_full.shape[0]
    position = offset + lax.iota(jnp.int32, n_tokens)
    column_pos = offset - pad_width + lax.iota(jnp.int32, padded.shape[0])
    center = padded[pad_width : pad_width + n_tokens].astype(jnp.float32)
    outputs = []
    for group_number, window_span in enumerate(pool_spans):
        low_edge = jnp.clip(position - window_span // 2, 0, seq_len)
        high_edge = jnp.clip(position - window_span // 2 + window_span, 0, seq_len)
        band_mask = (
            (column_pos[None, :] >= low_edge[:, None]) & (column_pos[None, :] < high_edge[:, None])
        ).astype(jnp.bfloat16)
        lower_col = group_number * group_width
        columns = padded[:, lower_col : lower_col + group_width]
        window_sum = jnp.dot(band_mask, columns, preferred_element_type=jnp.float32)
        window_mean = window_sum / (high_edge - low_edge).astype(jnp.float32)[:, None]
        deviation = (window_mean - center[:, lower_col : lower_col + group_width]).astype(
            jnp.bfloat16
        )
        mapped = jnp.dot(
            deviation, pool_full[:, group_number, :], preferred_element_type=jnp.float32
        )
        outputs.append(mapped + pool_bias[group_number])
    return jnp.concatenate(outputs, axis=-1) * pool_scale


def shards(
    tokens,
    gate_weight,
    up_weight,
    down_weight,
    pool_weight,
    pool_bias,
    pool_scale,
    gain_first,
    gain_mix,
    gain_second,
):
    gate_full, up_full, pool_half = (
        lax.all_gather(gate_weight, "fs", axis=0, tiled=True),
        lax.all_gather(up_weight, "fs", axis=0, tiled=True),
        lax.all_gather(pool_weight, "fs", axis=0, tiled=True),
    )
    down_full = lax.all_gather(down_weight, "fs", axis=1, tiled=True)
    pool_full = lax.all_gather(pool_half, "tp", axis=2, tiled=True)
    seq_len = tokens.shape[0]
    first_normed = rms_scale(tokens, gain_first)
    first_hidden = ffn_hidden(first_normed, gate_full, up_full)
    second_gate, second_up, second_down = (gate_full, up_full, down_full)
    first_branch = lax.psum(
        jnp.dot(first_hidden, down_full, preferred_element_type=jnp.float32).astype(jnp.bfloat16),
        "tp",
    ).astype(jnp.float32)
    after_first = (tokens.astype(jnp.float32) + 0.5 * first_branch).astype(jnp.bfloat16)
    mix_normed = rms_scale(after_first, gain_mix)
    padded = jnp.pad(mix_normed, ((pad_width, pad_width), (0, 0)))
    mixed = pool_block(padded, 0, seq_len, pool_full, pool_bias, pool_scale)
    after_mix = (after_first.astype(jnp.float32) + mixed).astype(jnp.bfloat16)
    second_normed = rms_scale(after_mix, gain_second)
    second_hidden = ffn_hidden(second_normed, second_gate, second_up)
    second_branch = lax.psum(
        jnp.dot(second_hidden, second_down, preferred_element_type=jnp.float32).astype(
            jnp.bfloat16
        ),
        "tp",
    ).astype(jnp.float32)
    return (after_mix.astype(jnp.float32) + 0.5 * second_branch).astype(jnp.bfloat16)


def fused_kernel(
    sizes, tok_hbm, gate_ref, up_ref, down_ref, pool_hbm, bias_hbm, scale_hbm, gain1_hbm, gainm_hbm, gain2_hbm,
    out_ref,
    gu_full, down_full, pool_full, acc, normed, hidden, amix, res, guest, part0, rbuf0, xs0, xr0, xg0, lent,
    part1, rbuf1, xs1, xr1, tok_ref, pool_ref, bias_ref, scale_ref, gain1_ref, gainm_ref, gain2_ref,
    zsend, zleft, zrecv, ysend, yrecv, tsend, trecv, lsem, asend, arecv, qsend, qrecv,
    csend, crecv, xsend, xrecv, gsend, grecv, fsend, frecv, osem,
):
    n, n_tp = sizes
    g, z, t = lax.axis_index("grp"), lax.axis_index("fs"), lax.axis_index("tp")
    core, side = lax.rem(t, 2), t // 2
    outer = (z == 0) | (z == n - 1)
    inner = (z > 0) & (z < n - 1)
    e = 1 - jnp.minimum(z, 1) * jnp.minimum(n - 1 - z, 1)
    pz = z + 1 - 2 * lax.rem(z, 2)
    mirror, far = n - 1 - z, n - 1 - pz
    y_peer, partner, inward = {"grp": 1 - g}, {"fs": pz}, {"fs": mirror}
    mate, x_peer = {"tp": t + 1 - 2 * core}, {"tp": lax.rem(t + 2, n_tp)}
    n_rows, width = tok_hbm.shape
    d_loc, f_loc = gate_ref.shape
    pool_rows, groups, pool_cols = pool_hbm.shape
    half_rows = n_rows // 2
    quarter = n_rows // n_tp
    block_cols = d_loc // 2
    sub_cols = block_cols // 2
    n_blocks = 2 * n
    f32 = jnp.float32

    def remote(src, dst, s_sem, r_sem, dev):
        return pltpu.make_async_remote_copy(
            src_ref=src, dst_ref=dst, send_sem=s_sem, recv_sem=r_sem, device_id=dev, device_id_type=MESH
        )

    barrier = pltpu.get_barrier_semaphore()

    def greet(dev):
        pl.semaphore_signal(barrier, inc=1, device_id=dev, device_id_type=MESH)

    greet(y_peer)
    greet(partner)
    for off in range(1, n_tp):
        greet({"tp": lax.rem(t + off, n_tp)})

    @pl.when(inner)
    def _():
        greet(inward)

    pl.semaphore_wait(barrier, n_tp + 2 - e)

    counts = {"pool": 1, "gu": 8, "down": 8}
    first_key = {"pool": 0, "gu": 1, "down": 9}

    def each(name, act):
        if counts[name] == 1:
            act(0)
        else:
            pl.loop(0, counts[name])(act)

    kind = {"pool": 0, "gu": 1, "down": 2}

    def key(name, c):
        return first_key[name] + c

    def slot(s, at):
        return lax.rem(s - at + n, n) - 1

    def bulk(name, c):
        return 0 if name == "pool" else (3 if name == "down" else 1) + c // 4

    def region(name, s, half, c):
        if name == "down":
            size = f_loc // 4
            rows = pl.ds(pl.multiple_of(lax.rem(c, 4) * size, 16), size)
            return down_full.at[s, half, rows, pl.ds(pl.multiple_of(c // 4 * sub_cols, 128), sub_cols)]
        if name == "pool":
            size = pool_rows // 2
            rows = pl.ds(pl.multiple_of(s * pool_rows + half * size, 16), size)
            return pool_full.at[:, rows, pl.ds(pl.multiple_of(t * pool_cols, 128), pool_cols)]
        size = d_loc // 8
        rows = pl.ds(pl.multiple_of(s * d_loc + half * (d_loc // 2) + lax.rem(c, 4) * size, 16), size)
        return gu_full.at[c // 4, rows, :]

    def whole(name, s, half):
        if name == "down":
            return down_full.at[s, half]
        if name == "pool":
            return region(name, s, half, 0)
        rows = pl.ds(pl.multiple_of(s * d_loc + half * (d_loc // 2), 16), d_loc // 2)
        return gu_full.at[:, rows, :] if name == "gu" else gu_full.at[0 if name == "gate" else 1, rows, :]

    def source(name, half, c):
        if name == "down":
            size = f_loc // 4
            cols = pl.ds(pl.multiple_of(half * block_cols + c // 4 * sub_cols, 128), sub_cols)
            return down_ref.at[pl.ds(pl.multiple_of(lax.rem(c, 4) * size, 16), size), cols]
        if name == "pool":
            return region(name, z, half, c)
        size = d_loc // 8
        rows = pl.ds(pl.multiple_of(half * (d_loc // 2) + c * size, 16), size)
        return {"gate": gate_ref, "up": up_ref}[name].at[rows, :]

    def own_copy(name, c, half, s_sem, r_sem, dev):
        base = {"gate": 0, "up": 4}.get(name)
        name_of, at = ("gu", base + c) if base is not None else (name, c)
        where = region(name_of, z, half, at)
        return remote(source(name, half, c), where, s_sem.at[kind[name_of]], r_sem(name_of, at), dev)

    def own_partner(name, c):
        return own_copy(name, c, g, zsend.at[z], lambda nm, at: zrecv.at[slot(z, pz), key(nm, at)], partner)

    def own_inward(name, c):
        return own_copy(name, c, g, zleft, lambda nm, at: zrecv.at[slot(z, mirror), key(nm, at)], inward)

    def own_direct(name, c):
        return own_copy(name, c, 1 - g, ysend.at[z], lambda nm, at: yrecv.at[slot(z, pz), bulk(nm, at)], partner)

    def passing(name, s, c, dev):
        there = region(name, s, g, c)
        to = pz if dev is partner else mirror
        return remote(there, there, zsend.at[s, kind[name]], zrecv.at[slot(s, to), key(name, c)], dev)

    def arrival(name, s, c):
        there = region(name, s, g, c)
        return remote(there, there, zsend.at[s, kind[name]], zrecv.at[slot(s, z), key(name, c)], partner)

    def share(name, s, c):
        there = region(name, s, g, c)
        where = kind[name] + (c // 4 if name == "down" else 0)
        return remote(there, there, ysend.at[s, where], yrecv.at[slot(s, z), bulk(name, c)], y_peer)

    def shared(name, s, rows=None):
        if name != "down":
            sent(name, s, g, ysend.at[s], y_peer).wait_send()
            return
        for part in range(2):
            size = f_loc if part == 0 or rows is None else rows
            there = down_full.at[s, g, pl.ds(0, size), pl.ds(part * sub_cols, sub_cols)]
            remote(there, there, ysend.at[s, 2 + part], yrecv.at[0, 0], y_peer).wait_send()

    def settle(name, s):
        if name == "down":
            settle_down(s, 0)
            settle_down(s, 1)
            return
        there = whole(name, s, 1 - g)
        where = {"pool": 0, "gate": 1, "up": 2}[name]
        remote(there, there, ysend.at[s, 0], yrecv.at[slot(s, z), where], y_peer).wait_recv()

    def settle_down(s, part, rows=None):
        there = down_full.at[s, 1 - g, pl.ds(0, rows or f_loc), pl.ds(part * sub_cols, sub_cols)]
        remote(there, there, ysend.at[s, 0], yrecv.at[slot(s, z), 3 + part], y_peer).wait_recv()

    def sent(name, s, half, sems, dev):
        there = whole(name, s, half)
        return remote(there, there, sems.at[kind[name]], yrecv.at[0, 0], dev)

    def extra_copy(s, at, dev):
        there = region("down", s, 1 - g, 7)
        return remote(there, there, zsend.at[s, 3], yrecv.at[slot(s, at), 5], dev)

    kinds = ("pool", "gu", "down")

    def quarter_rows(tt):
        return pl.ds(pl.multiple_of((lax.rem(tt, 2) * (n_tp // 2) + tt // 2) * quarter, 16), quarter)

    own_counts = {"pool": 1, "gate": 4, "up": 4, "down": 8}

    def start_each(names, make):
        for name in names:
            pl.loop(0, own_counts[name])(lambda c: make(name, c).start())

    tok_copy = remote(
        tok_hbm.at[quarter_rows(t), :], guest.at[quarter_rows(t), :], asend.at[0], arecv.at[0], partner
    )

    own_rows = pl.ds(pl.multiple_of(z * d_loc, 128), d_loc)
    pool_in = pltpu.make_async_copy(pool_hbm, pool_ref, lsem.at[0])
    local = [
        pltpu.make_async_copy(tok_hbm, tok_ref, lsem.at[1]),
        pltpu.make_async_copy(gate_ref, gu_full.at[0, own_rows, :], lsem.at[2]),
        pltpu.make_async_copy(up_ref, gu_full.at[1, own_rows, :], lsem.at[3]),
        pltpu.make_async_copy(down_ref.at[:, pl.ds(0, block_cols)], down_full.at[z, 0], lsem.at[4]),
        pltpu.make_async_copy(down_ref.at[:, pl.ds(block_cols, block_cols)], down_full.at[z, 1], lsem.at[5]),
        pltpu.make_async_copy(bias_hbm, bias_ref, lsem.at[6]),
        pltpu.make_async_copy(scale_hbm, scale_ref, lsem.at[7]),
        pltpu.make_async_copy(gain1_hbm, gain1_ref, lsem.at[8]),
        pltpu.make_async_copy(gainm_hbm, gainm_ref, lsem.at[9]),
        pltpu.make_async_copy(gain2_hbm, gain2_ref, lsem.at[10]),
    ]
    pool_in.start()

    @pl.when(outer)
    def _():
        tok_copy.start()
        start_each(("gate", "up"), own_partner)

    @pl.when(inner)
    def _():
        for name in ("gate", "up"):

            @pl.loop(0, 4)
            def _(c):
                own_inward(name, c).start()
                own_partner(name, c).start()

    for copy in local:
        copy.start()
    pool_in.wait()
    for k in range(groups):
        pool_full[
            k, pl.ds(pl.multiple_of(z * pool_rows, 16), pool_rows), pl.ds(pl.multiple_of(t * pool_cols, 128), pool_cols)
        ] = pool_ref[:, k, :]
    own_partner("pool", 0).start()

    @pl.when(outer)
    def _():
        start_each(("gate", "up", "pool"), own_direct)
        start_each(("down",), own_partner)
        start_each(("down",), own_direct)

    @pl.when(inner)
    def _():
        own_inward("pool", 0).start()

    def norm_rows(src, gain, base=0):
        @pl.loop(0, n_rows // 32)
        def _(r):
            values = src[pl.ds(pl.multiple_of(r * 32, 32), 32), :].astype(f32)
            scaled = values * lax.rsqrt(jnp.mean(values * values, axis=-1, keepdims=True) + eps)
            normed[pl.ds(pl.multiple_of(base + r * 32, 32), 32), :] = (scaled * gain[...]).astype(jnp.bfloat16)

    tile = 256

    def add_shard(w, s, first=False):
        k_cols = pl.ds(pl.multiple_of(s * d_loc, 128), d_loc)

        @pl.loop(0, f_loc // tile)
        def _(i):
            cols = pl.ds(pl.multiple_of(i * tile, tile), tile)
            product = jnp.dot(normed[:, k_cols], gu_full[w, k_cols, cols], preferred_element_type=f32)
            acc[w, :, cols] = product if first else acc[w, :, cols] + product

    def pool_copy(off, s, sender):
        cols = pl.ds(pl.multiple_of(sender * pool_cols, 128), pool_cols)
        there = pool_full.at[:, pl.ds(pl.multiple_of(s * pool_rows, 16), pool_rows), cols]
        return remote(there, there, tsend.at[off - 1], trecv.at[off - 1], {"tp": lax.rem(t + off, n_tp)})

    def pool_all(off, sender):
        there = pool_full.at[:, :, pl.ds(pl.multiple_of(sender * pool_cols, 128), pool_cols)]
        return remote(there, there, tsend.at[off - 1], trecv.at[off - 1], {"tp": lax.rem(t + off, n_tp)})

    def spread_pool(s):
        for off in range(1, n_tp):
            pool_copy(off, s, t).start()

    def activate(gate_proj, up_proj):
        return (gate_proj / (1.0 + jnp.exp(-gate_proj)) * up_proj).astype(jnp.bfloat16)

    def guest_copy(off, sender):
        there = guest.at[quarter_rows(sender), :]
        return remote(there, there, qsend.at[off - 1], qrecv.at[off - 1], {"tp": lax.rem(t + off, n_tp)})

    def columns(place):
        s, half = place
        return pl.ds(pl.multiple_of(s * d_loc + half * block_cols, 128), block_cols)

    def first_place(j, at):
        here = [at, n - 1 - at, at + 1 - 2 * lax.rem(at, 2)]
        here.append(n - 1 - here[2])
        shard, half = ((0, 0), (0, 1), (1, 0), (1, 1), (2, 0), (3, 0), (2, 1), (3, 1))[j]
        return here[shard], g if half == 0 else 1 - g

    def second_place(j):
        here = [z, e * pz + (1 - e) * mirror, e * far + (1 - e) * pz, e * mirror + (1 - e) * far]
        return here[j // 2], g if j % 2 == 0 else 1 - g

    mine = pl.ds(pl.multiple_of(core * half_rows, 16), half_rows)
    other = pl.ds(pl.multiple_of((1 - core) * half_rows, 16), half_rows)

    def final_copy(phase, j, place, rows):
        there = res.at[phase, rows, columns(place)]
        return remote(there, there, fsend.at[phase], frecv.at[0], mate)

    def final_all(phase, rows):
        there = res.at[phase, rows, :]
        return remote(there, there, fsend.at[phase], frecv.at[0], mate)

    def pair_first(j):
        return remote(part0.at[j, 1 - core], rbuf0.at[j], csend.at[0], crecv.at[0, j], mate)

    def x_first(j):
        return remote(xs0.at[j, 0], xr0.at[j], xsend.at[0], xrecv.at[0, j], x_peer)

    kept = pl.ds(pl.multiple_of(side * quarter, 16), quarter)
    given = pl.ds(pl.multiple_of((1 - side) * quarter, 16), quarter)

    def x_guest(j):
        return remote(xs0.at[j, 1, given, :], xg0.at[j], gsend.at[0], grecv.at[j], x_peer)

    def lend_copy(j, at):
        cols = columns(first_place(j, at))
        return remote(lent.at[j], res.at[0, quarter_rows(t), cols], asend.at[1], arecv.at[1 + j], partner)

    def lent_copy(j, lane):
        owner = (t, t, lax.rem(t + 2, n_tp))[lane]
        there = res.at[0, quarter_rows(owner), columns(first_place(j, pz))]
        return remote(
            there, there, qsend.at[3 + lane], qrecv.at[3 + j if lane == 1 else 11 + lane // 2], x_peer if lane == 1 else mate
        )

    def lent_all(lane, owner):
        there = res.at[0, quarter_rows(owner), :]
        return remote(there, there, qsend.at[3 + lane], qrecv.at[11 + lane // 2], mate)

    def lent_arrival(j):
        lane = 1
        owner = lax.rem(t + 2, n_tp)
        there = res.at[0, quarter_rows(owner), columns(first_place(j, pz))]
        return remote(
            there, there, qsend.at[3 + lane], qrecv.at[3 + j if lane == 1 else 11 + lane // 2], x_peer if lane == 1 else mate
        )

    def from_mirror(name, c):
        arrival(name, mirror, c).wait_recv()
        passing(name, mirror, c, partner).start()
        share(name, mirror, c).start()

    def from_far(name, c):
        arrival(name, far, c).wait_recv()
        passing(name, far, c, partner).start()
        share(name, far, c).start()

    def from_partner(name, c):
        arrival(name, pz, c).wait_recv()
        passing(name, pz, c, inward).start()

    def keep_down(s, low):
        for c in range(low, low + 2):
            arrival("down", s, c).wait_recv()
            share("down", s, c).start()

    def down_mirror(c):
        keep_down(mirror, 2 * c)

    def down_far(c):
        keep_down(far, 2 * c)

    def down_partner(c):
        from_partner("down", 2 * c)
        from_partner("down", 2 * c + 1)

    def first_ffn():
        for copy in local:
            copy.wait()
        spread_pool(z)
        norm_rows(tok_ref, gain1_ref)
        tok_copy.wait_recv()
        for off in range(1, n_tp):
            guest_copy(off, t).start()
        from_mirror("gu", 0)
        from_mirror("gu", 1)

        @pl.loop(0, 4)
        def _(m):
            from_mirror("gu", m + 2)
            from_partner("gu", m)

        for off in range(1, n_tp):
            guest_copy(off, lax.rem(t - off + n_tp, n_tp)).wait_recv()
        norm_rows(guest, gain1_ref, n_rows)
        from_mirror("gu", 6)
        from_partner("gu", 4)
        add_shard(0, z, True)
        from_mirror("gu", 7)
        from_partner("gu", 5)
        add_shard(1, z, True)
        from_mirror("pool", 0)
        from_partner("gu", 6)
        from_far("gu", 0)
        settle("gate", mirror)
        add_shard(0, mirror)
        from_partner("gu", 7)
        from_partner("pool", 0)
        pl.loop(0, 8)(lambda c: own_inward("down", c).start())
        from_far("gu", 1)
        settle("up", mirror)
        add_shard(1, mirror)
        from_far("gu", 2)
        settle("pool", mirror)
        spread_pool(mirror)
        from_far("gu", 3)
        from_far("gu", 4)
        from_far("gu", 5)
        settle("gate", far)
        add_shard(0, far)
        from_far("gu", 6)
        settle("gate", pz)
        add_shard(0, pz)
        from_far("gu", 7)
        from_far("pool", 0)
        pl.loop(0, 4)(lambda c: own_partner("down", c).start())
        down_mirror(0)
        down_mirror(1)
        settle("pool", far)
        spread_pool(far)
        settle("up", far)
        add_shard(1, far)
        settle("up", pz)
        down_mirror(2)
        down_partner(0)
        add_shard(1, pz)

        @pl.loop(0, f_loc // tile)
        def _(i):
            cols = pl.ds(pl.multiple_of(i * tile, tile), tile)

            @pl.loop(0, 2 * n_rows // 128)
            def _(r):
                rows = pl.ds(pl.multiple_of(r * 128, 128), 128)
                hidden[rows, cols] = activate(acc[0, rows, cols], acc[1, rows, cols])

        def multiply(j):
            s, half = first_place(j, z)
            product = jnp.dot(hidden[...], down_full[s, half], preferred_element_type=f32).astype(jnp.bfloat16)
            for seq in range(2):
                for part in range(2):
                    row = seq * n_rows + part * half_rows
                    part0[j, part, seq] = product[row : row + half_rows]
            pair_first(j).start()

        def add_pair(j):
            pair_first(j).wait_recv()
            xs0[j] = (part0[j, core].astype(f32) + rbuf0[j].astype(f32)).astype(jnp.bfloat16)
            x_guest(j).start()
            x_first(j).start()

        def lend(j):
            x_guest(j).wait_recv()
            total = xs0[j, 1, kept, :].astype(f32) + xg0[j].astype(f32)
            cols = columns(first_place(j, z))
            lent[j] = (guest[quarter_rows(t), cols].astype(f32) + 0.5 * total).astype(jnp.bfloat16)
            lend_copy(j, z).start()

        def keep(j):
            x_first(j).wait_recv()
            place = first_place(j, z)
            cols = columns(place)
            total = xs0[j, 0].astype(f32) + xr0[j].astype(f32)
            res[0, mine, cols] = (tok_ref[mine, cols].astype(f32) + 0.5 * total).astype(jnp.bfloat16)
            final_copy(0, j, place, mine).start()

        def finish(j):
            lend(j)
            keep(j)

        down_mirror(3)
        down_partner(1)
        multiply(0)
        multiply(1)
        add_pair(0)
        down_far(0)
        down_partner(2)
        add_pair(1)
        settle("down", mirror)
        multiply(2)
        multiply(3)
        add_pair(2)
        down_partner(3)
        down_far(1)
        multiply(4)
        add_pair(3)
        down_far(2)
        add_pair(4)
        finish(0)
        finish(1)
        down_far(3)
        multiply(5)
        finish(2)
        add_pair(5)
        finish(3)
        settle("down", pz)
        multiply(6)
        finish(4)
        pl.loop(4, 6)(lambda c: own_partner("down", c).start())
        add_pair(6)
        settle("down", far)
        multiply(7)
        lend(5)
        add_pair(7)
        settle("pool", pz)
        spread_pool(pz)
        keep(5)
        lend(6)
        lend(7)
        pl.loop(6, 8)(lambda c: own_partner("down", c).start())
        pl.loop(0, 8)(lambda c: passing("down", mirror, c, partner).start())
        pl.loop(0, 8)(lambda c: passing("down", far, c, partner).start())
        extra_copy(far, pz, partner).start()
        keep(6)
        keep(7)
        final_all(0, other).wait_recv()

    def take(name, s, c):
        arrival(name, s, c).wait_recv()
        share(name, s, c).start()

    def collect():
        for copy in local:
            copy.wait()
        spread_pool(z)
        shards_in = (pz, far, mirror)
        for i, s in enumerate(shards_in):
            pl.loop(0, 8)(lambda m: take("gu", s, m))
            take("pool", s, 0)
            if i > 0:
                settle("pool", shards_in[i - 1])
                spread_pool(shards_in[i - 1])

        def hand_out(j):
            lend_copy(j, pz).wait_recv()
            lent_copy(j, 1).start()
            lent_copy(j, 0).start()

        def hand_on(j):
            lent_arrival(j).wait_recv()
            lent_copy(j, 2).start()

        pl.loop(0, 3)(lambda c: take("down", pz, c))
        settle("pool", mirror)
        spread_pool(mirror)
        take("down", pz, 3)
        for j in range(5):
            hand_out(j)
        pl.loop(4, 6)(lambda c: take("down", pz, c))
        for j in range(4):
            hand_on(j)
        hand_out(5)
        hand_on(4)
        hand_out(6)
        hand_out(7)
        hand_on(5)
        hand_on(6)
        take("down", pz, 6)
        hand_on(7)
        take("down", pz, 7)
        t_mate = t + 1 - 2 * core
        lent_all(0, t_mate).wait_recv()
        lent_all(2, lax.rem(t_mate + 2, n_tp)).wait_recv()

    pl.when(inner)(first_ffn)
    pl.when(outer)(collect)

    def when_outer(act):
        pl.when(outer)(act)

    def take_down(s, low, high):
        @pl.when(outer)
        def _():
            for c in range(low, high):
                take("down", s, c)

    norm_rows(res.at[0], gainm_ref)
    take_down(far, 0, 1)
    for off in range(1, n_tp):
        pool_all(off, lax.rem(t - off + n_tp, n_tp)).wait_recv()
    group_width = width // groups
    row_id = lax.broadcasted_iota(jnp.int32, (n_rows, n_rows), 0)
    col_id = lax.broadcasted_iota(jnp.int32, (n_rows, n_rows), 1)
    position = lax.broadcasted_iota(jnp.int32, (n_rows, 1), 0)
    own_seq = pl.ds(0, n_rows)
    for k, span in enumerate(pool_spans):
        low = row_id - span // 2
        band = jnp.where((col_id >= low) & (col_id < low + span), 1.0, 0.0).astype(jnp.bfloat16)
        first = jnp.maximum(position - span // 2, 0)
        last = jnp.minimum(position - span // 2 + span, n_rows)
        inverse = 1.0 / (last - first).astype(f32)
        cols = pl.ds(k * group_width, group_width)
        mean = jnp.dot(band, normed[own_seq, cols], preferred_element_type=f32) * inverse
        deviation = (mean - normed[own_seq, cols].astype(f32)).astype(jnp.bfloat16)
        mapped = jnp.dot(deviation, pool_full[k], preferred_element_type=f32) + bias_ref[pl.ds(k, 1), :]
        amix[:, cols] = (res[0, :, cols].astype(f32) + mapped * scale_ref[:, cols]).astype(jnp.bfloat16)
        if k % 2 == 1:
            take_down(far, 1 + k // 2, 2 + k // 2)

    norm_rows(amix, gain2_ref)

    @pl.when(outer)
    def _():
        for s in (pz, far, mirror):
            settle("gate", s)
            settle("up", s)
        take("down", far, 3)

    @pl.loop(0, f_loc // tile)
    def _(i):
        cols = pl.ds(pl.multiple_of(i * tile, tile), tile)
        gate_proj = jnp.dot(normed[own_seq, :], gu_full[0, :, cols], preferred_element_type=f32)
        up_proj = jnp.dot(normed[own_seq, :], gu_full[1, :, cols], preferred_element_type=f32)
        hidden[own_seq, cols] = activate(gate_proj, up_proj)

        @pl.when(outer & (i % 2 == 1))
        def _():
            take("down", far, 4 + i // 2)

    def spot(b):
        wide = b < n_blocks - 2
        j = b if wide else n_blocks - 2 + b % 2
        place = second_place(j)
        off, size = (0, block_cols) if wide else ((b - n_blocks + 2) // 2 * sub_cols, sub_cols)
        cols = pl.ds(pl.multiple_of(place[0] * d_loc + place[1] * block_cols + off, 128), size)
        return j, place, cols, pl.ds(off, size)

    def pair_copy(b):
        j, _, _, lanes = spot(b)
        return remote(part1.at[j, other, lanes], rbuf1.at[j, :, lanes], csend.at[1], crecv.at[1, b], mate)

    def x_copy(b):
        j, _, _, lanes = spot(b)
        return remote(xs1.at[j, :, lanes], xr1.at[j, :, lanes], xsend.at[1], xrecv.at[1, b], x_peer)

    def last_copy(b, rows):
        there = res.at[1, rows, spot(b)[2]]
        return remote(there, there, fsend.at[1], frecv.at[1 + b], mate)

    def multiply(b):
        j, (s, half), _, lanes = spot(b)
        product = jnp.dot(hidden[own_seq, :], down_full[s, half, :, lanes], preferred_element_type=f32)
        part1[j, :, lanes] = product.astype(jnp.bfloat16)
        pair_copy(b).start()

    early_rows = f_loc // 4 * 3 // 128 * 128

    def multiply_last(b):
        j, (s, half), _, lanes = spot(b)
        early, late = pl.ds(0, early_rows), pl.ds(early_rows, f_loc - early_rows)
        when_outer(lambda: settle_down(mirror, 1, f_loc // 4 * 3))
        held = acc.at[0, own_seq, pl.ds(0, sub_cols)]
        held[...] = jnp.dot(hidden[own_seq, early], down_full[s, half, early, lanes], preferred_element_type=f32)
        when_outer(lambda: extra_copy(mirror, z, partner).wait_recv())
        product = jnp.dot(hidden[own_seq, late], down_full[s, half, late, lanes], preferred_element_type=f32)
        part1[j, :, lanes] = (held[...] + product).astype(jnp.bfloat16)
        pair_copy(b).start()

    def add_pair(b):
        j, _, _, lanes = spot(b)
        pair_copy(b).wait_recv()
        xs1[j, :, lanes] = (part1[j, mine, lanes].astype(f32) + rbuf1[j, :, lanes].astype(f32)).astype(jnp.bfloat16)
        x_copy(b).start()

    def finish(b):
        j, _, cols, lanes = spot(b)
        x_copy(b).wait_recv()
        total = xs1[j, :, lanes].astype(f32) + xr1[j, :, lanes].astype(f32)
        res[1, mine, cols] = (amix[mine, cols].astype(f32) + 0.5 * total).astype(jnp.bfloat16)
        last_copy(b, mine).start()

    def emit(b):
        cols = spot(b)[2]
        last_copy(b, other).wait_recv()
        pltpu.make_async_copy(res.at[1, :, cols], out_ref.at[:, cols], osem.at[0]).start()

    def drain_early():
        for off in range(1, n_tp):
            pool_all(off, t).wait_send()
        for name in kinds:
            sent(name, z, g, zsend.at[z], partner).wait_send()

        @pl.when(outer)
        def _():
            tok_copy.wait_send()
            for name in kinds:
                sent(name, z, 1 - g, ysend.at[z], partner).wait_send()
                for s in (pz, far, mirror):
                    if name != "down":
                        shared(name, s)
            shared("down", pz)
            for lane in range(3):
                lent_all(lane, t).wait_send()

        @pl.when(inner)
        def _():
            for off in range(1, n_tp):
                guest_copy(off, t).wait_send()
            for name in kinds:
                sent(name, z, g, zleft, inward).wait_send()
                sent(name, pz, g, zsend.at[pz], inward).wait_send()
                for s in (mirror, far):
                    shared(name, s)
                    if name != "down":
                        sent(name, s, g, zsend.at[s], partner).wait_send()
            remote(rbuf0, rbuf0, csend.at[0], crecv.at[0, 0], mate).wait_send()
            remote(xr0, xr0, xsend.at[0], xrecv.at[0, 0], x_peer).wait_send()
            remote(xg0, xg0, gsend.at[0], grecv.at[0], x_peer).wait_send()
            remote(lent, lent, asend.at[1], arecv.at[1], partner).wait_send()
            final_all(0, mine).wait_send()

    multiply(0)
    take_down(far, 6, 7)
    multiply(1)
    add_pair(0)
    multiply(2)
    add_pair(1)
    take_down(far, 7, 8)
    when_outer(lambda: settle("down", pz))
    multiply(3)
    add_pair(2)
    multiply(4)
    add_pair(3)
    take_down(mirror, 0, 1)
    add_pair(4)
    take_down(mirror, 1, 3)
    when_outer(lambda: settle("down", far))
    multiply(5)
    take_down(mirror, 3, 4)
    multiply(6)
    add_pair(5)
    finish(0)
    add_pair(6)
    take_down(mirror, 4, 5)
    drain_early()
    finish(1)
    emit(0)
    take_down(mirror, 5, 6)
    when_outer(lambda: settle_down(mirror, 0))
    multiply(7)
    finish(2)
    emit(1)
    add_pair(7)
    take_down(mirror, 6, 7)
    finish(3)
    emit(2)
    when_outer(lambda: arrival("down", mirror, 7).wait_recv())
    multiply(8)
    finish(4)
    emit(3)
    add_pair(8)
    multiply_last(9)
    finish(5)
    emit(4)
    add_pair(9)
    finish(6)
    emit(5)
    finish(7)
    emit(6)
    finish(8)
    emit(7)
    finish(9)
    emit(8)
    emit(9)

    @pl.when(outer)
    def _():
        shared("down", far)
        shared("down", mirror, f_loc // 4 * 3)

    @pl.when(inner)
    def _():
        for s in (mirror, far):
            sent("down", s, g, zsend.at[s], partner).wait_send()
        extra_copy(far, pz, partner).wait_send()

    remote(xr1, xr1, csend.at[1], crecv.at[1, 0], mate).wait_send()
    remote(xr1, xr1, xsend.at[1], xrecv.at[1, 0], x_peer).wait_send()
    final_all(1, mine).wait_send()
    pltpu.make_async_copy(res.at[1], out_ref, osem.at[0]).wait()


def fused_shards(
    n, n_tp, tokens, gate_weight, up_weight, down_weight, pool_weight, pool_bias, pool_scale,
    gain_first, gain_mix, gain_second,
):
    n_rows, width = tokens.shape
    d_loc, f_loc = gate_weight.shape
    pool_rows, groups, pool_cols = pool_weight.shape
    bf16, dma, vmem = jnp.bfloat16, pltpu.SemaphoreType.DMA, pltpu.VMEM
    anywhere = pl.BlockSpec(memory_space=pl.ANY)
    half, quarter, block, blocks = n_rows // 2, n_rows // n_tp, d_loc // 2, 2 * n
    return pl.pallas_call(
        functools.partial(fused_kernel, (n, n_tp)),
        out_shape=jax.ShapeDtypeStruct((n_rows, width), bf16),
        in_specs=[anywhere] * 10,
        out_specs=anywhere,
        scratch_shapes=[
            vmem((2, n * d_loc, f_loc), bf16),
            vmem((n, 2, f_loc, block), bf16),
            vmem((groups, n * pool_rows, n_tp * pool_cols), bf16),
            vmem((2, 2 * n_rows, f_loc), jnp.float32),
            vmem((2 * n_rows, width), bf16),
            vmem((2 * n_rows, f_loc), bf16),
            vmem((n_rows, width), bf16),
            vmem((2, n_rows, width), bf16),
            vmem((n_rows, width), bf16),
            vmem((blocks, 2, 2, half, block), bf16),
            vmem((blocks, 2, half, block), bf16),
            vmem((blocks, 2, half, block), bf16),
            vmem((blocks, half, block), bf16),
            vmem((blocks, quarter, block), bf16),
            vmem((blocks, quarter, block), bf16),
            vmem((blocks, n_rows, block), bf16),
            vmem((blocks, half, block), bf16),
            vmem((blocks, half, block), bf16),
            vmem((blocks, half, block), bf16),
            vmem((n_rows, width), bf16),
            vmem((pool_rows, groups, pool_cols), bf16),
            vmem(pool_bias.shape, jnp.float32),
            vmem((1, width), jnp.float32),
            vmem((1, width), jnp.float32),
            vmem((1, width), jnp.float32),
            vmem((1, width), jnp.float32),
            dma((n, 4)), dma((3,)), dma((n - 1, 17)), dma((n, 4)), dma((n - 1, 6)),
            dma((n_tp - 1,)), dma((n_tp - 1,)), dma((11,)),
            dma((2,)), dma((1 + blocks,)), dma((6,)), dma((5 + blocks,)),
            dma((2,)), dma((2, blocks + 2)), dma((2,)), dma((2, blocks + 2)), dma((1,)), dma((blocks,)),
            dma((2,)), dma((3 + blocks,)), dma((1,)),
        ],
        compiler_params=pltpu.CompilerParams(
            collective_id=0, has_side_effects=True, vmem_limit_bytes=60 * 1024 * 1024
        ),
    )(
        tokens, gate_weight, up_weight, down_weight, pool_weight, pool_bias, pool_scale.reshape(1, width),
        gain_first.reshape(1, width), gain_mix.reshape(1, width), gain_second.reshape(1, width),
    )


def layer(n_grp, n, n_tp, *args):
    n_rows, width = args[0].shape
    d_loc, f_loc = args[1].shape
    pool_rows, _, pool_cols = args[4].shape
    fits = n_grp == 2 and n_tp == 4 and n == 4 and n_rows % 64 == 0
    fits = fits and d_loc % 512 == 0 and f_loc % 1280 == 0 and pool_rows % 32 == 0 and pool_cols % 128 == 0
    return fused_shards(n, n_tp, *args) if fits else shards(*args)


def solution(mesh):
    return jax.shard_map(
        functools.partial(layer, mesh.shape["grp"], mesh.shape["fs"], mesh.shape["tp"]),
        mesh=mesh,
        in_specs=(
            P(("grp", "fs"), None),
            P("fs", "tp"),
            P("fs", "tp"),
            P("tp", "fs"),
            P("fs", None, "tp"),
            P(),
            P(),
            P(),
            P(),
            P(),
        ),
        out_specs=P(("grp", "fs"), None),
        check_vma=False,
    )
```

```python
import functools

import jax
import jax.numpy as jnp
from jax import lax
from jax.experimental import pallas as pl
from jax.experimental.pallas import tpu as pltpu
from jax.sharding import PartitionSpec as P

eps = 1e-06
pool_spans = (2, 4, 8, 16)
pad_width = 8
MESH = pl.DeviceIdType.MESH


def rms_scale(values, gain_vec):
    fvalues = values.astype(jnp.float32)
    scaled = fvalues * lax.rsqrt(jnp.mean(fvalues * fvalues, axis=-1, keepdims=True) + eps)
    return (scaled * gain_vec).astype(jnp.bfloat16)


def ffn_hidden(normed, gate_full, up_full):
    gate_proj = jnp.dot(normed, gate_full, preferred_element_type=jnp.float32)
    up_proj = jnp.dot(normed, up_full, preferred_element_type=jnp.float32)
    return (jax.nn.silu(gate_proj) * up_proj).astype(jnp.bfloat16)


def pool_block(padded, offset, seq_len, pool_full, pool_bias, pool_scale):
    n_tokens = padded.shape[0] - 2 * pad_width
    group_width = pool_full.shape[0]
    position = offset + lax.iota(jnp.int32, n_tokens)
    column_pos = offset - pad_width + lax.iota(jnp.int32, padded.shape[0])
    center = padded[pad_width : pad_width + n_tokens].astype(jnp.float32)
    outputs = []
    for group_number, window_span in enumerate(pool_spans):
        low_edge = jnp.clip(position - window_span // 2, 0, seq_len)
        high_edge = jnp.clip(position - window_span // 2 + window_span, 0, seq_len)
        band_mask = (
            (column_pos[None, :] >= low_edge[:, None]) & (column_pos[None, :] < high_edge[:, None])
        ).astype(jnp.bfloat16)
        lower_col = group_number * group_width
        columns = padded[:, lower_col : lower_col + group_width]
        window_sum = jnp.dot(band_mask, columns, preferred_element_type=jnp.float32)
        window_mean = window_sum / (high_edge - low_edge).astype(jnp.float32)[:, None]
        deviation = (window_mean - center[:, lower_col : lower_col + group_width]).astype(
            jnp.bfloat16
        )
        mapped = jnp.dot(
            deviation, pool_full[:, group_number, :], preferred_element_type=jnp.float32
        )
        outputs.append(mapped + pool_bias[group_number])
    return jnp.concatenate(outputs, axis=-1) * pool_scale


def shards(
    tokens,
    gate_weight,
    up_weight,
    down_weight,
    pool_weight,
    pool_bias,
    pool_scale,
    gain_first,
    gain_mix,
    gain_second,
):
    gate_full, up_full, pool_half = (
        lax.all_gather(gate_weight, "fs", axis=0, tiled=True),
        lax.all_gather(up_weight, "fs", axis=0, tiled=True),
        lax.all_gather(pool_weight, "fs", axis=0, tiled=True),
    )
    down_full = lax.all_gather(down_weight, "fs", axis=1, tiled=True)
    pool_full = lax.all_gather(pool_half, "tp", axis=2, tiled=True)
    seq_len = tokens.shape[0]
    first_normed = rms_scale(tokens, gain_first)
    first_hidden = ffn_hidden(first_normed, gate_full, up_full)
    second_gate, second_up, second_down = (gate_full, up_full, down_full)
    first_branch = lax.psum(
        jnp.dot(first_hidden, down_full, preferred_element_type=jnp.float32).astype(jnp.bfloat16),
        "tp",
    ).astype(jnp.float32)
    after_first = (tokens.astype(jnp.float32) + 0.5 * first_branch).astype(jnp.bfloat16)
    mix_normed = rms_scale(after_first, gain_mix)
    padded = jnp.pad(mix_normed, ((pad_width, pad_width), (0, 0)))
    mixed = pool_block(padded, 0, seq_len, pool_full, pool_bias, pool_scale)
    after_mix = (after_first.astype(jnp.float32) + mixed).astype(jnp.bfloat16)
    second_normed = rms_scale(after_mix, gain_second)
    second_hidden = ffn_hidden(second_normed, second_gate, second_up)
    second_branch = lax.psum(
        jnp.dot(second_hidden, second_down, preferred_element_type=jnp.float32).astype(
            jnp.bfloat16
        ),
        "tp",
    ).astype(jnp.float32)
    return (after_mix.astype(jnp.float32) + 0.5 * second_branch).astype(jnp.bfloat16)


def fused_kernel(
    sizes, tok_hbm, gate_ref, up_ref, down_ref, pool_hbm, bias_hbm, scale_hbm, gain1_hbm, gainm_hbm, gain2_hbm,
    out_ref,
    gu_full, down_full, pool_full, acc, normed, hidden, amix, res, guest, part0, rbuf0, xs0, xr0, xg0, lent,
    part1, rbuf1, xs1, xr1, tok_ref, pool_ref, bias_ref, scale_ref, gain1_ref, gainm_ref, gain2_ref,
    zsend, zleft, zrecv, ysend, yrecv, tsend, trecv, lsem, asend, arecv, qsend, qrecv,
    csend, crecv, xsend, xrecv, gsend, grecv, fsend, frecv,
):
    n, n_tp = sizes
    g, z, t = lax.axis_index("grp"), lax.axis_index("fs"), lax.axis_index("tp")
    core, side = lax.rem(t, 2), t // 2
    outer = (z == 0) | (z == n - 1)
    inner = (z > 0) & (z < n - 1)
    e = 1 - jnp.minimum(z, 1) * jnp.minimum(n - 1 - z, 1)
    pz = z + 1 - 2 * lax.rem(z, 2)
    mirror, far = n - 1 - z, n - 1 - pz
    y_peer, partner, inward = {"grp": 1 - g}, {"fs": pz}, {"fs": mirror}
    mate, x_peer = {"tp": t + 1 - 2 * core}, {"tp": lax.rem(t + 2, n_tp)}
    n_rows, width = tok_hbm.shape
    d_loc, f_loc = gate_ref.shape
    pool_rows, groups, pool_cols = pool_hbm.shape
    half_rows = n_rows // 2
    quarter = n_rows // n_tp
    block_cols = d_loc // 2
    sub_cols = block_cols // 2
    n_blocks = 2 * n
    f32 = jnp.float32

    def remote(src, dst, s_sem, r_sem, dev):
        return pltpu.make_async_remote_copy(
            src_ref=src, dst_ref=dst, send_sem=s_sem, recv_sem=r_sem, device_id=dev, device_id_type=MESH
        )

    barrier = pltpu.get_barrier_semaphore()

    def greet(dev):
        pl.semaphore_signal(barrier, inc=1, device_id=dev, device_id_type=MESH)

    greet(y_peer)
    greet(partner)
    for off in range(1, n_tp):
        greet({"tp": lax.rem(t + off, n_tp)})

    @pl.when(inner)
    def _():
        greet(inward)

    pl.semaphore_wait(barrier, n_tp + 2 - e)

    counts = {"pool": 1, "gu": 8, "down": 8}
    first_key = {"pool": 0, "gu": 1, "down": 9}

    def each(name, act):
        if counts[name] == 1:
            act(0)
        else:
            pl.loop(0, counts[name])(act)

    kind = {"pool": 0, "gu": 1, "down": 2}

    def key(name, c):
        return first_key[name] + c

    def slot(s, at):
        return lax.rem(s - at + n, n) - 1

    def bulk(name, c):
        return 0 if name == "pool" else (3 if name == "down" else 1) + c // 4

    def region(name, s, half, c):
        if name == "down":
            size = f_loc // 4
            rows = pl.ds(pl.multiple_of(lax.rem(c, 4) * size, 16), size)
            return down_full.at[s, half, rows, pl.ds(pl.multiple_of(c // 4 * sub_cols, 128), sub_cols)]
        if name == "pool":
            size = pool_rows // 2
            rows = pl.ds(pl.multiple_of(s * pool_rows + half * size, 16), size)
            return pool_full.at[:, rows, pl.ds(pl.multiple_of(t * pool_cols, 128), pool_cols)]
        size = d_loc // 8
        rows = pl.ds(pl.multiple_of(s * d_loc + half * (d_loc // 2) + lax.rem(c, 4) * size, 16), size)
        return gu_full.at[c // 4, rows, :]

    def whole(name, s, half):
        if name == "down":
            return down_full.at[s, half]
        if name == "pool":
            return region(name, s, half, 0)
        rows = pl.ds(pl.multiple_of(s * d_loc + half * (d_loc // 2), 16), d_loc // 2)
        return gu_full.at[:, rows, :] if name == "gu" else gu_full.at[0 if name == "gate" else 1, rows, :]

    def source(name, half, c):
        if name == "down":
            size = f_loc // 4
            cols = pl.ds(pl.multiple_of(half * block_cols + c // 4 * sub_cols, 128), sub_cols)
            return down_ref.at[pl.ds(pl.multiple_of(lax.rem(c, 4) * size, 16), size), cols]
        if name == "pool":
            return region(name, z, half, c)
        size = d_loc // 8
        rows = pl.ds(pl.multiple_of(half * (d_loc // 2) + c * size, 16), size)
        return {"gate": gate_ref, "up": up_ref}[name].at[rows, :]

    def own_copy(name, c, half, s_sem, r_sem, dev):
        base = {"gate": 0, "up": 4}.get(name)
        name_of, at = ("gu", base + c) if base is not None else (name, c)
        where = region(name_of, z, half, at)
        return remote(source(name, half, c), where, s_sem.at[kind[name_of]], r_sem(name_of, at), dev)

    def own_partner(name, c):
        return own_copy(name, c, g, zsend.at[z], lambda nm, at: zrecv.at[slot(z, pz), key(nm, at)], partner)

    def own_inward(name, c):
        return own_copy(name, c, g, zleft, lambda nm, at: zrecv.at[slot(z, mirror), key(nm, at)], inward)

    def own_direct(name, c):
        return own_copy(name, c, 1 - g, ysend.at[z], lambda nm, at: yrecv.at[slot(z, pz), bulk(nm, at)], partner)

    def passing(name, s, c, dev):
        there = region(name, s, g, c)
        to = pz if dev is partner else mirror
        return remote(there, there, zsend.at[s, kind[name]], zrecv.at[slot(s, to), key(name, c)], dev)

    def arrival(name, s, c):
        there = region(name, s, g, c)
        return remote(there, there, zsend.at[s, kind[name]], zrecv.at[slot(s, z), key(name, c)], partner)

    def share(name, s, c):
        there = region(name, s, g, c)
        where = kind[name] + (c // 4 if name == "down" else 0)
        return remote(there, there, ysend.at[s, where], yrecv.at[slot(s, z), bulk(name, c)], y_peer)

    def shared(name, s, rows=None):
        if name != "down":
            sent(name, s, g, ysend.at[s], y_peer).wait_send()
            return
        for part in range(2):
            size = f_loc if part == 0 or rows is None else rows
            there = down_full.at[s, g, pl.ds(0, size), pl.ds(part * sub_cols, sub_cols)]
            remote(there, there, ysend.at[s, 2 + part], yrecv.at[0, 0], y_peer).wait_send()

    def settle(name, s):
        if name == "down":
            settle_down(s, 0)
            settle_down(s, 1)
            return
        there = whole(name, s, 1 - g)
        where = {"pool": 0, "gate": 1, "up": 2}[name]
        remote(there, there, ysend.at[s, 0], yrecv.at[slot(s, z), where], y_peer).wait_recv()

    def settle_down(s, part, rows=None):
        there = down_full.at[s, 1 - g, pl.ds(0, rows or f_loc), pl.ds(part * sub_cols, sub_cols)]
        remote(there, there, ysend.at[s, 0], yrecv.at[slot(s, z), 3 + part], y_peer).wait_recv()

    def sent(name, s, half, sems, dev):
        there = whole(name, s, half)
        return remote(there, there, sems.at[kind[name]], yrecv.at[0, 0], dev)

    def extra_copy(s, at, dev):
        there = region("down", s, 1 - g, 7)
        return remote(there, there, zsend.at[s, 3], yrecv.at[slot(s, at), 5], dev)

    kinds = ("pool", "gu", "down")

    def quarter_rows(tt):
        return pl.ds(pl.multiple_of((lax.rem(tt, 2) * (n_tp // 2) + tt // 2) * quarter, 16), quarter)

    own_counts = {"pool": 1, "gate": 4, "up": 4, "down": 8}

    def start_each(names, make):
        for name in names:
            pl.loop(0, own_counts[name])(lambda c: make(name, c).start())

    tok_copy = remote(
        tok_hbm.at[quarter_rows(t), :], guest.at[quarter_rows(t), :], asend.at[0], arecv.at[0], partner
    )

    own_rows = pl.ds(pl.multiple_of(z * d_loc, 128), d_loc)
    pool_in = pltpu.make_async_copy(pool_hbm, pool_ref, lsem.at[0])
    local = [
        pltpu.make_async_copy(tok_hbm, tok_ref, lsem.at[1]),
        pltpu.make_async_copy(gate_ref, gu_full.at[0, own_rows, :], lsem.at[2]),
        pltpu.make_async_copy(up_ref, gu_full.at[1, own_rows, :], lsem.at[3]),
        pltpu.make_async_copy(down_ref.at[:, pl.ds(0, block_cols)], down_full.at[z, 0], lsem.at[4]),
        pltpu.make_async_copy(down_ref.at[:, pl.ds(block_cols, block_cols)], down_full.at[z, 1], lsem.at[5]),
        pltpu.make_async_copy(bias_hbm, bias_ref, lsem.at[6]),
        pltpu.make_async_copy(scale_hbm, scale_ref, lsem.at[7]),
        pltpu.make_async_copy(gain1_hbm, gain1_ref, lsem.at[8]),
        pltpu.make_async_copy(gainm_hbm, gainm_ref, lsem.at[9]),
        pltpu.make_async_copy(gain2_hbm, gain2_ref, lsem.at[10]),
    ]
    pool_in.start()

    @pl.when(outer)
    def _():
        tok_copy.start()
        start_each(("gate", "up"), own_partner)

    @pl.when(inner)
    def _():
        for name in ("gate", "up"):

            @pl.loop(0, 4)
            def _(c):
                own_inward(name, c).start()
                own_partner(name, c).start()

    for copy in local:
        copy.start()
    pool_in.wait()
    for k in range(groups):
        pool_full[
            k, pl.ds(pl.multiple_of(z * pool_rows, 16), pool_rows), pl.ds(pl.multiple_of(t * pool_cols, 128), pool_cols)
        ] = pool_ref[:, k, :]
    own_partner("pool", 0).start()

    @pl.when(outer)
    def _():
        start_each(("gate", "up", "pool"), own_direct)
        start_each(("down",), own_partner)
        start_each(("down",), own_direct)

    @pl.when(inner)
    def _():
        own_inward("pool", 0).start()

    def norm_rows(src, gain, base=0):
        @pl.loop(0, n_rows // 32)
        def _(r):
            values = src[pl.ds(pl.multiple_of(r * 32, 32), 32), :].astype(f32)
            scaled = values * lax.rsqrt(jnp.mean(values * values, axis=-1, keepdims=True) + eps)
            normed[pl.ds(pl.multiple_of(base + r * 32, 32), 32), :] = (scaled * gain[...]).astype(jnp.bfloat16)

    tile = 256

    def add_shard(w, s, first=False):
        k_cols = pl.ds(pl.multiple_of(s * d_loc, 128), d_loc)

        @pl.loop(0, f_loc // tile)
        def _(i):
            cols = pl.ds(pl.multiple_of(i * tile, tile), tile)
            product = jnp.dot(normed[:, k_cols], gu_full[w, k_cols, cols], preferred_element_type=f32)
            acc[w, :, cols] = product if first else acc[w, :, cols] + product

    def pool_copy(off, s, sender):
        cols = pl.ds(pl.multiple_of(sender * pool_cols, 128), pool_cols)
        there = pool_full.at[:, pl.ds(pl.multiple_of(s * pool_rows, 16), pool_rows), cols]
        return remote(there, there, tsend.at[off - 1], trecv.at[off - 1], {"tp": lax.rem(t + off, n_tp)})

    def pool_all(off, sender):
        there = pool_full.at[:, :, pl.ds(pl.multiple_of(sender * pool_cols, 128), pool_cols)]
        return remote(there, there, tsend.at[off - 1], trecv.at[off - 1], {"tp": lax.rem(t + off, n_tp)})

    def spread_pool(s):
        for off in range(1, n_tp):
            pool_copy(off, s, t).start()

    def activate(gate_proj, up_proj):
        return (gate_proj / (1.0 + jnp.exp(-gate_proj)) * up_proj).astype(jnp.bfloat16)

    def guest_copy(off, sender):
        there = guest.at[quarter_rows(sender), :]
        return remote(there, there, qsend.at[off - 1], qrecv.at[off - 1], {"tp": lax.rem(t + off, n_tp)})

    def columns(place):
        s, half = place
        return pl.ds(pl.multiple_of(s * d_loc + half * block_cols, 128), block_cols)

    def first_place(j, at):
        here = [at, n - 1 - at, at + 1 - 2 * lax.rem(at, 2)]
        here.append(n - 1 - here[2])
        shard, half = ((0, 0), (0, 1), (1, 0), (1, 1), (2, 0), (3, 0), (2, 1), (3, 1))[j]
        return here[shard], g if half == 0 else 1 - g

    def second_place(j):
        here = [z, e * pz + (1 - e) * mirror, e * far + (1 - e) * pz, e * mirror + (1 - e) * far]
        return here[j // 2], g if j % 2 == 0 else 1 - g

    mine = pl.ds(pl.multiple_of(core * half_rows, 16), half_rows)
    other = pl.ds(pl.multiple_of((1 - core) * half_rows, 16), half_rows)

    def final_copy(phase, j, place, rows):
        there = res.at[phase, rows, columns(place)]
        return remote(there, there, fsend.at[phase], frecv.at[0], mate)

    def final_all(phase, rows):
        there = res.at[phase, rows, :]
        return remote(there, there, fsend.at[phase], frecv.at[0], mate)

    def pair_first(j):
        return remote(part0.at[j, 1 - core], rbuf0.at[j], csend.at[0], crecv.at[0, j], mate)

    def x_first(j):
        return remote(xs0.at[j, 0], xr0.at[j], xsend.at[0], xrecv.at[0, j], x_peer)

    kept = pl.ds(pl.multiple_of(side * quarter, 16), quarter)
    given = pl.ds(pl.multiple_of((1 - side) * quarter, 16), quarter)

    def x_guest(j):
        return remote(xs0.at[j, 1, given, :], xg0.at[j], gsend.at[0], grecv.at[j], x_peer)

    def lend_copy(j, at):
        cols = columns(first_place(j, at))
        return remote(lent.at[j], res.at[0, quarter_rows(t), cols], asend.at[1], arecv.at[1 + j], partner)

    def lent_copy(j, lane):
        owner = (t, t, lax.rem(t + 2, n_tp))[lane]
        there = res.at[0, quarter_rows(owner), columns(first_place(j, pz))]
        return remote(
            there, there, qsend.at[3 + lane], qrecv.at[3 + j if lane == 1 else 11 + lane // 2], x_peer if lane == 1 else mate
        )

    def lent_all(lane, owner):
        there = res.at[0, quarter_rows(owner), :]
        return remote(there, there, qsend.at[3 + lane], qrecv.at[11 + lane // 2], mate)

    def lent_arrival(j):
        lane = 1
        owner = lax.rem(t + 2, n_tp)
        there = res.at[0, quarter_rows(owner), columns(first_place(j, pz))]
        return remote(
            there, there, qsend.at[3 + lane], qrecv.at[3 + j if lane == 1 else 11 + lane // 2], x_peer if lane == 1 else mate
        )

    def from_mirror(name, c):
        arrival(name, mirror, c).wait_recv()
        passing(name, mirror, c, partner).start()
        share(name, mirror, c).start()

    def from_far(name, c):
        arrival(name, far, c).wait_recv()
        passing(name, far, c, partner).start()
        share(name, far, c).start()

    def from_partner(name, c):
        arrival(name, pz, c).wait_recv()
        passing(name, pz, c, inward).start()

    def keep_down(s, low):
        for c in range(low, low + 2):
            arrival("down", s, c).wait_recv()
            share("down", s, c).start()

    def down_mirror(c):
        keep_down(mirror, 2 * c)

    def down_far(c):
        keep_down(far, 2 * c)

    def down_partner(c):
        from_partner("down", 2 * c)
        from_partner("down", 2 * c + 1)

    def first_ffn():
        for copy in local:
            copy.wait()
        spread_pool(z)
        norm_rows(tok_ref, gain1_ref)
        tok_copy.wait_recv()
        for off in range(1, n_tp):
            guest_copy(off, t).start()
        from_mirror("gu", 0)
        from_mirror("gu", 1)

        @pl.loop(0, 4)
        def _(m):
            from_mirror("gu", m + 2)
            from_partner("gu", m)

        for off in range(1, n_tp):
            guest_copy(off, lax.rem(t - off + n_tp, n_tp)).wait_recv()
        norm_rows(guest, gain1_ref, n_rows)
        from_mirror("gu", 6)
        from_partner("gu", 4)
        add_shard(0, z, True)
        from_mirror("gu", 7)
        from_partner("gu", 5)
        add_shard(1, z, True)
        from_mirror("pool", 0)
        from_partner("gu", 6)
        from_far("gu", 0)
        settle("gate", mirror)
        add_shard(0, mirror)
        from_partner("gu", 7)
        from_partner("pool", 0)
        pl.loop(0, 8)(lambda c: own_inward("down", c).start())
        from_far("gu", 1)
        settle("up", mirror)
        add_shard(1, mirror)
        from_far("gu", 2)
        settle("pool", mirror)
        spread_pool(mirror)
        from_far("gu", 3)
        from_far("gu", 4)
        from_far("gu", 5)
        settle("gate", far)
        add_shard(0, far)
        from_far("gu", 6)
        settle("gate", pz)
        add_shard(0, pz)
        from_far("gu", 7)
        from_far("pool", 0)
        pl.loop(0, 4)(lambda c: own_partner("down", c).start())
        down_mirror(0)
        down_mirror(1)
        settle("pool", far)
        spread_pool(far)
        settle("up", far)
        add_shard(1, far)
        settle("up", pz)
        down_mirror(2)
        down_partner(0)
        add_shard(1, pz)

        @pl.loop(0, f_loc // tile)
        def _(i):
            cols = pl.ds(pl.multiple_of(i * tile, tile), tile)

            @pl.loop(0, 2 * n_rows // 128)
            def _(r):
                rows = pl.ds(pl.multiple_of(r * 128, 128), 128)
                hidden[rows, cols] = activate(acc[0, rows, cols], acc[1, rows, cols])

        def multiply(j):
            s, half = first_place(j, z)
            product = jnp.dot(hidden[...], down_full[s, half], preferred_element_type=f32).astype(jnp.bfloat16)
            for seq in range(2):
                for part in range(2):
                    row = seq * n_rows + part * half_rows
                    part0[j, part, seq] = product[row : row + half_rows]
            pair_first(j).start()

        def add_pair(j):
            pair_first(j).wait_recv()
            xs0[j] = (part0[j, core].astype(f32) + rbuf0[j].astype(f32)).astype(jnp.bfloat16)
            x_guest(j).start()
            x_first(j).start()

        def lend(j):
            x_guest(j).wait_recv()
            total = xs0[j, 1, kept, :].astype(f32) + xg0[j].astype(f32)
            cols = columns(first_place(j, z))
            lent[j] = (guest[quarter_rows(t), cols].astype(f32) + 0.5 * total).astype(jnp.bfloat16)
            lend_copy(j, z).start()

        def keep(j):
            x_first(j).wait_recv()
            place = first_place(j, z)
            cols = columns(place)
            total = xs0[j, 0].astype(f32) + xr0[j].astype(f32)
            res[0, mine, cols] = (tok_ref[mine, cols].astype(f32) + 0.5 * total).astype(jnp.bfloat16)
            final_copy(0, j, place, mine).start()

        def finish(j):
            lend(j)
            keep(j)

        down_mirror(3)
        down_partner(1)
        multiply(0)
        multiply(1)
        add_pair(0)
        down_far(0)
        down_partner(2)
        add_pair(1)
        settle("down", mirror)
        multiply(2)
        multiply(3)
        add_pair(2)
        down_partner(3)
        down_far(1)
        multiply(4)
        add_pair(3)
        down_far(2)
        add_pair(4)
        finish(0)
        finish(1)
        down_far(3)
        multiply(5)
        finish(2)
        add_pair(5)
        finish(3)
        settle("down", pz)
        multiply(6)
        finish(4)
        pl.loop(4, 6)(lambda c: own_partner("down", c).start())
        add_pair(6)
        settle("down", far)
        multiply(7)
        lend(5)
        add_pair(7)
        settle("pool", pz)
        spread_pool(pz)
        keep(5)
        lend(6)
        lend(7)
        pl.loop(6, 8)(lambda c: own_partner("down", c).start())
        pl.loop(0, 8)(lambda c: passing("down", mirror, c, partner).start())
        pl.loop(0, 8)(lambda c: passing("down", far, c, partner).start())
        extra_copy(far, pz, partner).start()
        keep(6)
        keep(7)
        final_all(0, other).wait_recv()

    def take(name, s, c):
        arrival(name, s, c).wait_recv()
        share(name, s, c).start()

    def collect():
        for copy in local:
            copy.wait()
        spread_pool(z)
        shards_in = (pz, far, mirror)
        for i, s in enumerate(shards_in):
            pl.loop(0, 8)(lambda m: take("gu", s, m))
            take("pool", s, 0)
            if i > 0:
                settle("pool", shards_in[i - 1])
                spread_pool(shards_in[i - 1])

        def hand_out(j):
            lend_copy(j, pz).wait_recv()
            lent_copy(j, 1).start()
            lent_copy(j, 0).start()

        def hand_on(j):
            lent_arrival(j).wait_recv()
            lent_copy(j, 2).start()

        pl.loop(0, 3)(lambda c: take("down", pz, c))
        settle("pool", mirror)
        spread_pool(mirror)
        take("down", pz, 3)
        for j in range(5):
            hand_out(j)
        pl.loop(4, 6)(lambda c: take("down", pz, c))
        for j in range(4):
            hand_on(j)
        hand_out(5)
        hand_on(4)
        hand_out(6)
        hand_out(7)
        hand_on(5)
        hand_on(6)
        take("down", pz, 6)
        hand_on(7)
        take("down", pz, 7)
        t_mate = t + 1 - 2 * core
        lent_all(0, t_mate).wait_recv()
        lent_all(2, lax.rem(t_mate + 2, n_tp)).wait_recv()

    pl.when(inner)(first_ffn)
    pl.when(outer)(collect)

    def when_outer(act):
        pl.when(outer)(act)

    def take_down(s, low, high):
        @pl.when(outer)
        def _():
            for c in range(low, high):
                take("down", s, c)

    norm_rows(res.at[0], gainm_ref)
    take_down(far, 0, 1)
    for off in range(1, n_tp):
        pool_all(off, lax.rem(t - off + n_tp, n_tp)).wait_recv()
    group_width = width // groups
    row_id = lax.broadcasted_iota(jnp.int32, (n_rows, n_rows), 0)
    col_id = lax.broadcasted_iota(jnp.int32, (n_rows, n_rows), 1)
    position = lax.broadcasted_iota(jnp.int32, (n_rows, 1), 0)
    own_seq = pl.ds(0, n_rows)
    for k, span in enumerate(pool_spans):
        low = row_id - span // 2
        band = jnp.where((col_id >= low) & (col_id < low + span), 1.0, 0.0).astype(jnp.bfloat16)
        first = jnp.maximum(position - span // 2, 0)
        last = jnp.minimum(position - span // 2 + span, n_rows)
        inverse = 1.0 / (last - first).astype(f32)
        cols = pl.ds(k * group_width, group_width)
        mean = jnp.dot(band, normed[own_seq, cols], preferred_element_type=f32) * inverse
        deviation = (mean - normed[own_seq, cols].astype(f32)).astype(jnp.bfloat16)
        mapped = jnp.dot(deviation, pool_full[k], preferred_element_type=f32) + bias_ref[pl.ds(k, 1), :]
        amix[:, cols] = (res[0, :, cols].astype(f32) + mapped * scale_ref[:, cols]).astype(jnp.bfloat16)
        if k % 2 == 1:
            take_down(far, 1 + k // 2, 2 + k // 2)

    norm_rows(amix, gain2_ref)

    @pl.when(outer)
    def _():
        for s in (pz, far, mirror):
            settle("gate", s)
            settle("up", s)
        take("down", far, 3)

    @pl.loop(0, f_loc // tile)
    def _(i):
        cols = pl.ds(pl.multiple_of(i * tile, tile), tile)
        gate_proj = jnp.dot(normed[own_seq, :], gu_full[0, :, cols], preferred_element_type=f32)
        up_proj = jnp.dot(normed[own_seq, :], gu_full[1, :, cols], preferred_element_type=f32)
        hidden[own_seq, cols] = activate(gate_proj, up_proj)

        @pl.when(outer & ((i == 1) | (i == 2) | (i == 4)))
        def _():
            take("down", far, 3 + i - i // 4)

    def spot(b):
        wide = b < n_blocks - 2
        j = b if wide else n_blocks - 2 + b % 2
        place = second_place(j)
        off, size = (0, block_cols) if wide else ((b - n_blocks + 2) // 2 * sub_cols, sub_cols)
        cols = pl.ds(pl.multiple_of(place[0] * d_loc + place[1] * block_cols + off, 128), size)
        return j, place, cols, pl.ds(off, size)

    def pair_copy(b):
        j, _, _, lanes = spot(b)
        return remote(part1.at[j, other, lanes], rbuf1.at[j, :, lanes], csend.at[1], crecv.at[1, b], mate)

    def x_copy(b):
        j, _, _, lanes = spot(b)
        return remote(xs1.at[j, :, lanes], xr1.at[j, :, lanes], xsend.at[1], xrecv.at[1, b], x_peer)

    def last_copy(b, rows):
        there = res.at[1, rows, spot(b)[2]]
        return remote(there, there, fsend.at[1], frecv.at[1 + b], mate)

    def multiply(b):
        j, (s, half), _, lanes = spot(b)
        product = jnp.dot(hidden[own_seq, :], down_full[s, half, :, lanes], preferred_element_type=f32)
        part1[j, :, lanes] = product.astype(jnp.bfloat16)
        pair_copy(b).start()

    early_rows = f_loc // 4 * 3 // 128 * 128

    def multiply_last(b):
        j, (s, half), _, lanes = spot(b)
        early, late = pl.ds(0, early_rows), pl.ds(early_rows, f_loc - early_rows)
        when_outer(lambda: settle_down(mirror, 1, f_loc // 4 * 3))
        held = acc.at[0, own_seq, pl.ds(0, sub_cols)]
        held[...] = jnp.dot(hidden[own_seq, early], down_full[s, half, early, lanes], preferred_element_type=f32)
        when_outer(lambda: extra_copy(mirror, z, partner).wait_recv())
        product = jnp.dot(hidden[own_seq, late], down_full[s, half, late, lanes], preferred_element_type=f32)
        part1[j, :, lanes] = (held[...] + product).astype(jnp.bfloat16)
        pair_copy(b).start()

    def add_pair(b):
        j, _, _, lanes = spot(b)
        pair_copy(b).wait_recv()
        xs1[j, :, lanes] = (part1[j, mine, lanes].astype(f32) + rbuf1[j, :, lanes].astype(f32)).astype(jnp.bfloat16)
        x_copy(b).start()

    def finish(b):
        j, _, cols, lanes = spot(b)
        x_copy(b).wait_recv()
        total = xs1[j, :, lanes].astype(f32) + xr1[j, :, lanes].astype(f32)
        res[1, mine, cols] = (amix[mine, cols].astype(f32) + 0.5 * total).astype(jnp.bfloat16)
        last_copy(b, mine).start()
        out_ref[mine, cols] = res[1, mine, cols]

    def emit(b):
        cols = spot(b)[2]
        last_copy(b, other).wait_recv()
        out_ref[other, cols] = res[1, other, cols]

    def drain_early():
        for off in range(1, n_tp):
            pool_all(off, t).wait_send()
        for name in kinds:
            sent(name, z, g, zsend.at[z], partner).wait_send()

        @pl.when(outer)
        def _():
            tok_copy.wait_send()
            for name in kinds:
                sent(name, z, 1 - g, ysend.at[z], partner).wait_send()
                for s in (pz, far, mirror):
                    if name != "down":
                        shared(name, s)
            shared("down", pz)
            for lane in range(3):
                lent_all(lane, t).wait_send()

        @pl.when(inner)
        def _():
            for off in range(1, n_tp):
                guest_copy(off, t).wait_send()
            for name in kinds:
                sent(name, z, g, zleft, inward).wait_send()
                sent(name, pz, g, zsend.at[pz], inward).wait_send()
                for s in (mirror, far):
                    shared(name, s)
                    if name != "down":
                        sent(name, s, g, zsend.at[s], partner).wait_send()
            remote(rbuf0, rbuf0, csend.at[0], crecv.at[0, 0], mate).wait_send()
            remote(xr0, xr0, xsend.at[0], xrecv.at[0, 0], x_peer).wait_send()
            remote(xg0, xg0, gsend.at[0], grecv.at[0], x_peer).wait_send()
            remote(lent, lent, asend.at[1], arecv.at[1], partner).wait_send()
            final_all(0, mine).wait_send()

    multiply(0)
    multiply(1)
    add_pair(0)
    multiply(2)
    add_pair(1)
    take_down(far, 7, 8)
    when_outer(lambda: settle("down", pz))
    multiply(3)
    add_pair(2)
    multiply(4)
    add_pair(3)
    take_down(mirror, 0, 1)
    add_pair(4)
    take_down(mirror, 1, 3)
    when_outer(lambda: settle("down", far))
    multiply(5)
    take_down(mirror, 3, 4)
    multiply(6)
    add_pair(5)
    finish(0)
    add_pair(6)
    take_down(mirror, 4, 5)
    drain_early()
    finish(1)
    emit(0)
    take_down(mirror, 5, 6)
    when_outer(lambda: settle_down(mirror, 0))
    multiply(7)
    finish(2)
    emit(1)
    take_down(mirror, 6, 7)
    add_pair(7)
    finish(3)
    emit(2)
    when_outer(lambda: arrival("down", mirror, 7).wait_recv())
    multiply(8)
    finish(4)
    emit(3)
    add_pair(8)
    multiply_last(9)
    finish(5)
    emit(4)
    add_pair(9)
    finish(6)
    emit(5)
    finish(7)
    emit(6)
    finish(8)
    emit(7)
    finish(9)
    emit(8)
    emit(9)

    @pl.when(outer)
    def _():
        shared("down", far)
        shared("down", mirror, f_loc // 4 * 3)

    @pl.when(inner)
    def _():
        for s in (mirror, far):
            sent("down", s, g, zsend.at[s], partner).wait_send()
        extra_copy(far, pz, partner).wait_send()

    remote(xr1, xr1, csend.at[1], crecv.at[1, 0], mate).wait_send()
    remote(xr1, xr1, xsend.at[1], xrecv.at[1, 0], x_peer).wait_send()
    final_all(1, mine).wait_send()


def fused_shards(
    n, n_tp, tokens, gate_weight, up_weight, down_weight, pool_weight, pool_bias, pool_scale,
    gain_first, gain_mix, gain_second,
):
    n_rows, width = tokens.shape
    d_loc, f_loc = gate_weight.shape
    pool_rows, groups, pool_cols = pool_weight.shape
    bf16, dma, vmem = jnp.bfloat16, pltpu.SemaphoreType.DMA, pltpu.VMEM
    anywhere = pl.BlockSpec(memory_space=pl.ANY)
    half, quarter, block, blocks = n_rows // 2, n_rows // n_tp, d_loc // 2, 2 * n
    return pl.pallas_call(
        functools.partial(fused_kernel, (n, n_tp)),
        out_shape=pltpu.VMEM((n_rows, width), bf16),
        in_specs=[anywhere] * 10,
        out_specs=pl.BlockSpec(memory_space=pltpu.VMEM),
        scratch_shapes=[
            vmem((2, n * d_loc, f_loc), bf16),
            vmem((n, 2, f_loc, block), bf16),
            vmem((groups, n * pool_rows, n_tp * pool_cols), bf16),
            vmem((2, 2 * n_rows, f_loc), jnp.float32),
            vmem((2 * n_rows, width), bf16),
            vmem((2 * n_rows, f_loc), bf16),
            vmem((n_rows, width), bf16),
            vmem((2, n_rows, width), bf16),
            vmem((n_rows, width), bf16),
            vmem((blocks, 2, 2, half, block), bf16),
            vmem((blocks, 2, half, block), bf16),
            vmem((blocks, 2, half, block), bf16),
            vmem((blocks, half, block), bf16),
            vmem((blocks, quarter, block), bf16),
            vmem((blocks, quarter, block), bf16),
            vmem((blocks, n_rows, block), bf16),
            vmem((blocks, half, block), bf16),
            vmem((blocks, half, block), bf16),
            vmem((blocks, half, block), bf16),
            vmem((n_rows, width), bf16),
            vmem((pool_rows, groups, pool_cols), bf16),
            vmem(pool_bias.shape, jnp.float32),
            vmem((1, width), jnp.float32),
            vmem((1, width), jnp.float32),
            vmem((1, width), jnp.float32),
            vmem((1, width), jnp.float32),
            dma((n, 4)), dma((3,)), dma((n - 1, 17)), dma((n, 4)), dma((n - 1, 6)),
            dma((n_tp - 1,)), dma((n_tp - 1,)), dma((11,)),
            dma((2,)), dma((1 + blocks,)), dma((6,)), dma((5 + blocks,)),
            dma((2,)), dma((2, blocks + 2)), dma((2,)), dma((2, blocks + 2)), dma((1,)), dma((blocks,)),
            dma((2,)), dma((3 + blocks,)),
        ],
        compiler_params=pltpu.CompilerParams(
            collective_id=0, has_side_effects=True, vmem_limit_bytes=60 * 1024 * 1024
        ),
    )(
        tokens, gate_weight, up_weight, down_weight, pool_weight, pool_bias, pool_scale.reshape(1, width),
        gain_first.reshape(1, width), gain_mix.reshape(1, width), gain_second.reshape(1, width),
    )


def layer(n_grp, n, n_tp, *args):
    n_rows, width = args[0].shape
    d_loc, f_loc = args[1].shape
    pool_rows, _, pool_cols = args[4].shape
    fits = n_grp == 2 and n_tp == 4 and n == 4 and n_rows % 64 == 0
    fits = fits and d_loc % 512 == 0 and f_loc % 1280 == 0 and pool_rows % 32 == 0 and pool_cols % 128 == 0
    return fused_shards(n, n_tp, *args) if fits else shards(*args)


def solution(mesh):
    return jax.shard_map(
        functools.partial(layer, mesh.shape["grp"], mesh.shape["fs"], mesh.shape["tp"]),
        mesh=mesh,
        in_specs=(
            P(("grp", "fs"), None),
            P("fs", "tp"),
            P("fs", "tp"),
            P("tp", "fs"),
            P("fs", None, "tp"),
            P(),
            P(),
            P(),
            P(),
            P(),
        ),
        out_specs=P(("grp", "fs"), None),
        check_vma=False,
    )
```

```python
import functools

import jax
import jax.numpy as jnp
from jax import lax
from jax.experimental import pallas as pl
from jax.experimental.pallas import tpu as pltpu
from jax.sharding import PartitionSpec as P

eps = 1e-06
pool_spans = (2, 4, 8, 16)
pad_width = 8
MESH = pl.DeviceIdType.MESH


def rms_scale(values, gain_vec):
    fvalues = values.astype(jnp.float32)
    scaled = fvalues * lax.rsqrt(jnp.mean(fvalues * fvalues, axis=-1, keepdims=True) + eps)
    return (scaled * gain_vec).astype(jnp.bfloat16)


def ffn_hidden(normed, gate_full, up_full):
    gate_proj = jnp.dot(normed, gate_full, preferred_element_type=jnp.float32)
    up_proj = jnp.dot(normed, up_full, preferred_element_type=jnp.float32)
    return (jax.nn.silu(gate_proj) * up_proj).astype(jnp.bfloat16)


def pool_block(padded, offset, seq_len, pool_full, pool_bias, pool_scale):
    n_tokens = padded.shape[0] - 2 * pad_width
    group_width = pool_full.shape[0]
    position = offset + lax.iota(jnp.int32, n_tokens)
    column_pos = offset - pad_width + lax.iota(jnp.int32, padded.shape[0])
    center = padded[pad_width : pad_width + n_tokens].astype(jnp.float32)
    outputs = []
    for group_number, window_span in enumerate(pool_spans):
        low_edge = jnp.clip(position - window_span // 2, 0, seq_len)
        high_edge = jnp.clip(position - window_span // 2 + window_span, 0, seq_len)
        band_mask = (
            (column_pos[None, :] >= low_edge[:, None]) & (column_pos[None, :] < high_edge[:, None])
        ).astype(jnp.bfloat16)
        lower_col = group_number * group_width
        columns = padded[:, lower_col : lower_col + group_width]
        window_sum = jnp.dot(band_mask, columns, preferred_element_type=jnp.float32)
        window_mean = window_sum / (high_edge - low_edge).astype(jnp.float32)[:, None]
        deviation = (window_mean - center[:, lower_col : lower_col + group_width]).astype(
            jnp.bfloat16
        )
        mapped = jnp.dot(
            deviation, pool_full[:, group_number, :], preferred_element_type=jnp.float32
        )
        outputs.append(mapped + pool_bias[group_number])
    return jnp.concatenate(outputs, axis=-1) * pool_scale


def shards(
    tokens,
    gate_weight,
    up_weight,
    down_weight,
    pool_weight,
    pool_bias,
    pool_scale,
    gain_first,
    gain_mix,
    gain_second,
):
    gate_full, up_full, pool_half = (
        lax.all_gather(gate_weight, "fs", axis=0, tiled=True),
        lax.all_gather(up_weight, "fs", axis=0, tiled=True),
        lax.all_gather(pool_weight, "fs", axis=0, tiled=True),
    )
    down_full = lax.all_gather(down_weight, "fs", axis=1, tiled=True)
    pool_full = lax.all_gather(pool_half, "tp", axis=2, tiled=True)
    seq_len = tokens.shape[0]
    first_normed = rms_scale(tokens, gain_first)
    first_hidden = ffn_hidden(first_normed, gate_full, up_full)
    second_gate, second_up, second_down = (gate_full, up_full, down_full)
    first_branch = lax.psum(
        jnp.dot(first_hidden, down_full, preferred_element_type=jnp.float32).astype(jnp.bfloat16),
        "tp",
    ).astype(jnp.float32)
    after_first = (tokens.astype(jnp.float32) + 0.5 * first_branch).astype(jnp.bfloat16)
    mix_normed = rms_scale(after_first, gain_mix)
    padded = jnp.pad(mix_normed, ((pad_width, pad_width), (0, 0)))
    mixed = pool_block(padded, 0, seq_len, pool_full, pool_bias, pool_scale)
    after_mix = (after_first.astype(jnp.float32) + mixed).astype(jnp.bfloat16)
    second_normed = rms_scale(after_mix, gain_second)
    second_hidden = ffn_hidden(second_normed, second_gate, second_up)
    second_branch = lax.psum(
        jnp.dot(second_hidden, second_down, preferred_element_type=jnp.float32).astype(
            jnp.bfloat16
        ),
        "tp",
    ).astype(jnp.float32)
    return (after_mix.astype(jnp.float32) + 0.5 * second_branch).astype(jnp.bfloat16)


def fused_kernel(
    sizes, tok_hbm, gate_ref, up_ref, down_ref, pool_hbm, bias_hbm, scale_hbm, gain1_hbm, gainm_hbm, gain2_hbm,
    out_ref,
    gu_full, down_full, pool_full, acc, normed, hidden, amix, res, guest, part0, rbuf0, xs0, xr0, xg0, lent,
    part1, rbuf1, xs1, xr1, tok_ref, pool_ref, bias_ref, scale_ref, gain1_ref, gainm_ref, gain2_ref,
    zsend, zleft, zrecv, ysend, yrecv, tsend, trecv, lsem, asend, arecv, qsend, qrecv,
    csend, crecv, xsend, xrecv, gsend, fsend, frecv,
):
    n, n_tp = sizes
    g, z, t = lax.axis_index("grp"), lax.axis_index("fs"), lax.axis_index("tp")
    core, side = lax.rem(t, 2), t // 2
    outer = (z == 0) | (z == n - 1)
    inner = (z > 0) & (z < n - 1)
    e = 1 - jnp.minimum(z, 1) * jnp.minimum(n - 1 - z, 1)
    pz = z + 1 - 2 * lax.rem(z, 2)
    mirror, far = n - 1 - z, n - 1 - pz
    y_peer, partner, inward = {"grp": 1 - g}, {"fs": pz}, {"fs": mirror}
    mate, x_peer = {"tp": t + 1 - 2 * core}, {"tp": lax.rem(t + 2, n_tp)}
    n_rows, width = tok_hbm.shape
    d_loc, f_loc = gate_ref.shape
    pool_rows, groups, pool_cols = pool_hbm.shape
    half_rows = n_rows // 2
    quarter = n_rows // n_tp
    block_cols = d_loc // 2
    sub_cols = block_cols // 2
    n_blocks = 2 * n
    f32 = jnp.float32

    def remote(src, dst, s_sem, r_sem, dev):
        return pltpu.make_async_remote_copy(
            src_ref=src, dst_ref=dst, send_sem=s_sem, recv_sem=r_sem, device_id=dev, device_id_type=MESH
        )

    barrier = pltpu.get_barrier_semaphore()

    def greet(dev):
        pl.semaphore_signal(barrier, inc=1, device_id=dev, device_id_type=MESH)

    greet(y_peer)
    greet(partner)
    for off in range(1, n_tp):
        greet({"tp": lax.rem(t + off, n_tp)})

    @pl.when(inner)
    def _():
        greet(inward)

    pl.semaphore_wait(barrier, n_tp + 2 - e)

    counts = {"pool": 1, "gu": 8, "down": 8}
    first_key = {"pool": 0, "gu": 1, "down": 9}

    def each(name, act):
        if counts[name] == 1:
            act(0)
        else:
            pl.loop(0, counts[name])(act)

    kind = {"pool": 0, "gu": 1, "down": 2}

    def key(name, c):
        return first_key[name] + c

    def slot(s, at):
        return lax.rem(s - at + n, n) - 1

    def bulk(name, c):
        return 0 if name == "pool" else (3 if name == "down" else 1) + c // 4

    def region(name, s, half, c):
        if name == "down":
            size = f_loc // 4
            rows = pl.ds(pl.multiple_of(lax.rem(c, 4) * size, 16), size)
            return down_full.at[s, half, rows, pl.ds(pl.multiple_of(c // 4 * sub_cols, 128), sub_cols)]
        if name == "pool":
            size = pool_rows // 2
            rows = pl.ds(pl.multiple_of(s * pool_rows + half * size, 16), size)
            return pool_full.at[:, rows, pl.ds(pl.multiple_of(t * pool_cols, 128), pool_cols)]
        size = d_loc // 8
        rows = pl.ds(pl.multiple_of(s * d_loc + half * (d_loc // 2) + lax.rem(c, 4) * size, 16), size)
        return gu_full.at[c // 4, rows, :]

    def whole(name, s, half):
        if name == "down":
            return down_full.at[s, half]
        if name == "pool":
            return region(name, s, half, 0)
        rows = pl.ds(pl.multiple_of(s * d_loc + half * (d_loc // 2), 16), d_loc // 2)
        return gu_full.at[:, rows, :] if name == "gu" else gu_full.at[0 if name == "gate" else 1, rows, :]

    def source(name, half, c):
        if name == "down":
            size = f_loc // 4
            cols = pl.ds(pl.multiple_of(half * block_cols + c // 4 * sub_cols, 128), sub_cols)
            return down_ref.at[pl.ds(pl.multiple_of(lax.rem(c, 4) * size, 16), size), cols]
        if name == "pool":
            return region(name, z, half, c)
        size = d_loc // 8
        rows = pl.ds(pl.multiple_of(half * (d_loc // 2) + c * size, 16), size)
        return {"gate": gate_ref, "up": up_ref}[name].at[rows, :]

    def own_copy(name, c, half, s_sem, r_sem, dev):
        base = {"gate": 0, "up": 4}.get(name)
        name_of, at = ("gu", base + c) if base is not None else (name, c)
        where = region(name_of, z, half, at)
        return remote(source(name, half, c), where, s_sem.at[kind[name_of]], r_sem(name_of, at), dev)

    def own_partner(name, c):
        return own_copy(name, c, g, zsend.at[z], lambda nm, at: zrecv.at[slot(z, pz), key(nm, at)], partner)

    def own_inward(name, c):
        return own_copy(name, c, g, zleft, lambda nm, at: zrecv.at[slot(z, mirror), key(nm, at)], inward)

    def own_direct(name, c):
        return own_copy(name, c, 1 - g, ysend.at[z], lambda nm, at: yrecv.at[slot(z, pz), bulk(nm, at)], partner)

    def passing(name, s, c, dev):
        there = region(name, s, g, c)
        to = pz if dev is partner else mirror
        return remote(there, there, zsend.at[s, kind[name]], zrecv.at[slot(s, to), key(name, c)], dev)

    def arrival(name, s, c):
        there = region(name, s, g, c)
        return remote(there, there, zsend.at[s, kind[name]], zrecv.at[slot(s, z), key(name, c)], partner)

    def share(name, s, c):
        there = region(name, s, g, c)
        where = kind[name] + (c // 4 if name == "down" else 0)
        return remote(there, there, ysend.at[s, where], yrecv.at[slot(s, z), bulk(name, c)], y_peer)

    def shared(name, s, rows=None):
        if name != "down":
            sent(name, s, g, ysend.at[s], y_peer).wait_send()
            return
        for part in range(2):
            size = f_loc if part == 0 or rows is None else rows
            there = down_full.at[s, g, pl.ds(0, size), pl.ds(part * sub_cols, sub_cols)]
            remote(there, there, ysend.at[s, 2 + part], yrecv.at[0, 0], y_peer).wait_send()

    def settle(name, s):
        if name == "down":
            settle_down(s, 0)
            settle_down(s, 1)
            return
        there = whole(name, s, 1 - g)
        where = {"pool": 0, "gate": 1, "up": 2}[name]
        remote(there, there, ysend.at[s, 0], yrecv.at[slot(s, z), where], y_peer).wait_recv()

    def settle_down(s, part, rows=None):
        there = down_full.at[s, 1 - g, pl.ds(0, rows or f_loc), pl.ds(part * sub_cols, sub_cols)]
        remote(there, there, ysend.at[s, 0], yrecv.at[slot(s, z), 3 + part], y_peer).wait_recv()

    def sent(name, s, half, sems, dev):
        there = whole(name, s, half)
        return remote(there, there, sems.at[kind[name]], yrecv.at[0, 0], dev)

    def extra_copy(s, at, dev):
        there = region("down", s, 1 - g, 7)
        return remote(there, there, zsend.at[s, 3], yrecv.at[slot(s, at), 5], dev)

    kinds = ("pool", "gu", "down")

    def quarter_rows(tt):
        return pl.ds(pl.multiple_of((lax.rem(tt, 2) * (n_tp // 2) + tt // 2) * quarter, 16), quarter)

    own_counts = {"pool": 1, "gate": 4, "up": 4, "down": 8}

    def start_each(names, make):
        for name in names:
            pl.loop(0, own_counts[name])(lambda c: make(name, c).start())

    tok_copy = remote(
        tok_hbm.at[quarter_rows(t), :], guest.at[quarter_rows(t), :], asend.at[0], arecv.at[0], partner
    )

    own_rows = pl.ds(pl.multiple_of(z * d_loc, 128), d_loc)
    pool_in = pltpu.make_async_copy(pool_hbm, pool_ref, lsem.at[0])
    local = [
        pltpu.make_async_copy(tok_hbm, tok_ref, lsem.at[1]),
        pltpu.make_async_copy(gate_ref, gu_full.at[0, own_rows, :], lsem.at[2]),
        pltpu.make_async_copy(up_ref, gu_full.at[1, own_rows, :], lsem.at[3]),
        pltpu.make_async_copy(down_ref.at[:, pl.ds(0, block_cols)], down_full.at[z, 0], lsem.at[4]),
        pltpu.make_async_copy(down_ref.at[:, pl.ds(block_cols, block_cols)], down_full.at[z, 1], lsem.at[5]),
        pltpu.make_async_copy(bias_hbm, bias_ref, lsem.at[6]),
        pltpu.make_async_copy(scale_hbm, scale_ref, lsem.at[7]),
        pltpu.make_async_copy(gain1_hbm, gain1_ref, lsem.at[8]),
        pltpu.make_async_copy(gainm_hbm, gainm_ref, lsem.at[9]),
        pltpu.make_async_copy(gain2_hbm, gain2_ref, lsem.at[10]),
    ]
    pool_in.start()

    @pl.when(outer)
    def _():
        tok_copy.start()
        start_each(("gate", "up"), own_partner)

    @pl.when(inner)
    def _():
        for name in ("gate", "up"):

            @pl.loop(0, 4)
            def _(c):
                own_inward(name, c).start()
                own_partner(name, c).start()

    for copy in local:
        copy.start()
    pool_in.wait()
    for k in range(groups):
        pool_full[
            k, pl.ds(pl.multiple_of(z * pool_rows, 16), pool_rows), pl.ds(pl.multiple_of(t * pool_cols, 128), pool_cols)
        ] = pool_ref[:, k, :]
    own_partner("pool", 0).start()

    @pl.when(outer)
    def _():
        start_each(("gate", "up", "pool"), own_direct)
        start_each(("down",), own_partner)
        start_each(("down",), own_direct)

    @pl.when(inner)
    def _():
        own_inward("pool", 0).start()

    def norm_rows(src, gain, base=0):
        @pl.loop(0, n_rows // 32)
        def _(r):
            values = src[pl.ds(pl.multiple_of(r * 32, 32), 32), :].astype(f32)
            scaled = values * lax.rsqrt(jnp.mean(values * values, axis=-1, keepdims=True) + eps)
            normed[pl.ds(pl.multiple_of(base + r * 32, 32), 32), :] = (scaled * gain[...]).astype(jnp.bfloat16)

    tile = 256

    def add_shard(w, s, first=False):
        k_cols = pl.ds(pl.multiple_of(s * d_loc, 128), d_loc)

        @pl.loop(0, f_loc // tile)
        def _(i):
            cols = pl.ds(pl.multiple_of(i * tile, tile), tile)
            product = jnp.dot(normed[:, k_cols], gu_full[w, k_cols, cols], preferred_element_type=f32)
            acc[w, :, cols] = product if first else acc[w, :, cols] + product

    def pool_copy(off, s, sender):
        cols = pl.ds(pl.multiple_of(sender * pool_cols, 128), pool_cols)
        there = pool_full.at[:, pl.ds(pl.multiple_of(s * pool_rows, 16), pool_rows), cols]
        return remote(there, there, tsend.at[off - 1], trecv.at[off - 1], {"tp": lax.rem(t + off, n_tp)})

    def pool_all(off, sender):
        there = pool_full.at[:, :, pl.ds(pl.multiple_of(sender * pool_cols, 128), pool_cols)]
        return remote(there, there, tsend.at[off - 1], trecv.at[off - 1], {"tp": lax.rem(t + off, n_tp)})

    def spread_pool(s):
        for off in range(1, n_tp):
            pool_copy(off, s, t).start()

    def activate(gate_proj, up_proj):
        return (gate_proj / (1.0 + jnp.exp(-gate_proj)) * up_proj).astype(jnp.bfloat16)

    def guest_copy(off, sender):
        there = guest.at[quarter_rows(sender), :]
        return remote(there, there, qsend.at[off - 1], qrecv.at[off - 1], {"tp": lax.rem(t + off, n_tp)})

    def columns(place):
        s, half = place
        return pl.ds(pl.multiple_of(s * d_loc + half * block_cols, 128), block_cols)

    def first_place(j, at):
        here = [at, n - 1 - at, at + 1 - 2 * lax.rem(at, 2)]
        here.append(n - 1 - here[2])
        shard, half = ((0, 0), (0, 1), (1, 0), (1, 1), (2, 0), (3, 0), (2, 1), (3, 1))[j]
        return here[shard], g if half == 0 else 1 - g

    def second_place(j):
        here = [z, e * pz + (1 - e) * mirror, e * far + (1 - e) * pz, e * mirror + (1 - e) * far]
        return here[j // 2], g if j % 2 == 0 else 1 - g

    mine = pl.ds(pl.multiple_of(core * half_rows, 16), half_rows)
    other = pl.ds(pl.multiple_of((1 - core) * half_rows, 16), half_rows)

    def final_copy(phase, j, place, rows):
        there = res.at[phase, rows, columns(place)]
        return remote(there, there, fsend.at[phase], frecv.at[0], mate)

    def final_all(phase, rows):
        there = res.at[phase, rows, :]
        return remote(there, there, fsend.at[phase], frecv.at[0], mate)

    def pair_first(j):
        return remote(part0.at[j, 1 - core], rbuf0.at[j], csend.at[0], crecv.at[0, j], mate)

    def x_first(j):
        return remote(xs0.at[j, 0], xr0.at[j], xsend.at[0], xrecv.at[0, j], x_peer)

    kept = pl.ds(pl.multiple_of(side * quarter, 16), quarter)
    given = pl.ds(pl.multiple_of((1 - side) * quarter, 16), quarter)

    def x_guest(j):
        return remote(xs0.at[j, 1, given, :], xg0.at[j], gsend.at[0], arecv.at[1 + j], x_peer)

    def lend_copy(j, at):
        cols = columns(first_place(j, at))
        return remote(lent.at[j], res.at[0, quarter_rows(t), cols], asend.at[1], arecv.at[1 + j], partner)

    def lent_copy(j, lane):
        owner = (t, t, lax.rem(t + 2, n_tp))[lane]
        there = res.at[0, quarter_rows(owner), columns(first_place(j, pz))]
        return remote(
            there, there, qsend.at[3 + lane], crecv.at[0, j] if lane == 1 else qrecv.at[3 + lane // 2], x_peer if lane == 1 else mate
        )

    def lent_all(lane, owner):
        there = res.at[0, quarter_rows(owner), :]
        return remote(there, there, qsend.at[3 + lane], qrecv.at[3 + lane // 2], mate)

    def lent_arrival(j):
        lane = 1
        owner = lax.rem(t + 2, n_tp)
        there = res.at[0, quarter_rows(owner), columns(first_place(j, pz))]
        return remote(
            there, there, qsend.at[3 + lane], crecv.at[0, j] if lane == 1 else qrecv.at[3 + lane // 2], x_peer if lane == 1 else mate
        )

    def from_mirror(name, c):
        arrival(name, mirror, c).wait_recv()
        passing(name, mirror, c, partner).start()
        share(name, mirror, c).start()

    def from_far(name, c):
        arrival(name, far, c).wait_recv()
        passing(name, far, c, partner).start()
        share(name, far, c).start()

    def from_partner(name, c):
        arrival(name, pz, c).wait_recv()
        passing(name, pz, c, inward).start()

    def keep_down(s, low):
        for c in range(low, low + 2):
            arrival("down", s, c).wait_recv()
            share("down", s, c).start()

    def down_mirror(c):
        keep_down(mirror, 2 * c)

    def down_far(c):
        keep_down(far, 2 * c)

    def down_partner(c):
        from_partner("down", 2 * c)
        from_partner("down", 2 * c + 1)

    def first_ffn():
        for copy in local:
            copy.wait()
        spread_pool(z)
        norm_rows(tok_ref, gain1_ref)
        tok_copy.wait_recv()
        for off in range(1, n_tp):
            guest_copy(off, t).start()
        from_mirror("gu", 0)
        from_mirror("gu", 1)

        @pl.loop(0, 4)
        def _(m):
            from_mirror("gu", m + 2)
            from_partner("gu", m)

        for off in range(1, n_tp):
            guest_copy(off, lax.rem(t - off + n_tp, n_tp)).wait_recv()
        norm_rows(guest, gain1_ref, n_rows)
        from_mirror("gu", 6)
        from_partner("gu", 4)
        add_shard(0, z, True)
        from_mirror("gu", 7)
        from_partner("gu", 5)
        add_shard(1, z, True)
        from_mirror("pool", 0)
        from_partner("gu", 6)
        from_far("gu", 0)
        settle("gate", mirror)
        add_shard(0, mirror)
        from_partner("gu", 7)
        from_partner("pool", 0)
        pl.loop(0, 8)(lambda c: own_inward("down", c).start())
        from_far("gu", 1)
        settle("up", mirror)
        add_shard(1, mirror)
        from_far("gu", 2)
        settle("pool", mirror)
        spread_pool(mirror)
        from_far("gu", 3)
        from_far("gu", 4)
        from_far("gu", 5)
        settle("gate", far)
        add_shard(0, far)
        from_far("gu", 6)
        settle("gate", pz)
        add_shard(0, pz)
        from_far("gu", 7)
        from_far("pool", 0)
        pl.loop(0, 4)(lambda c: own_partner("down", c).start())
        down_mirror(0)
        down_mirror(1)
        settle("pool", far)
        spread_pool(far)
        settle("up", far)
        add_shard(1, far)
        settle("up", pz)
        down_mirror(2)
        down_partner(0)
        add_shard(1, pz)

        @pl.loop(0, f_loc // tile)
        def _(i):
            cols = pl.ds(pl.multiple_of(i * tile, tile), tile)

            @pl.loop(0, 2 * n_rows // 128)
            def _(r):
                rows = pl.ds(pl.multiple_of(r * 128, 128), 128)
                hidden[rows, cols] = activate(acc[0, rows, cols], acc[1, rows, cols])

        def multiply(j):
            s, half = first_place(j, z)
            product = jnp.dot(hidden[...], down_full[s, half], preferred_element_type=f32).astype(jnp.bfloat16)
            for seq in range(2):
                for part in range(2):
                    row = seq * n_rows + part * half_rows
                    part0[j, part, seq] = product[row : row + half_rows]
            pair_first(j).start()

        def add_pair(j):
            pair_first(j).wait_recv()
            xs0[j] = (part0[j, core].astype(f32) + rbuf0[j].astype(f32)).astype(jnp.bfloat16)
            x_guest(j).start()
            x_first(j).start()

        def lend(j):
            x_guest(j).wait_recv()
            total = xs0[j, 1, kept, :].astype(f32) + xg0[j].astype(f32)
            cols = columns(first_place(j, z))
            lent[j] = (guest[quarter_rows(t), cols].astype(f32) + 0.5 * total).astype(jnp.bfloat16)
            lend_copy(j, z).start()

        def keep(j):
            x_first(j).wait_recv()
            place = first_place(j, z)
            cols = columns(place)
            total = xs0[j, 0].astype(f32) + xr0[j].astype(f32)
            res[0, mine, cols] = (tok_ref[mine, cols].astype(f32) + 0.5 * total).astype(jnp.bfloat16)
            final_copy(0, j, place, mine).start()

        def finish(j):
            lend(j)
            keep(j)

        down_mirror(3)
        down_partner(1)
        multiply(0)
        multiply(1)
        add_pair(0)
        down_far(0)
        down_partner(2)
        add_pair(1)
        settle("down", mirror)
        multiply(2)
        multiply(3)
        add_pair(2)
        down_partner(3)
        down_far(1)
        multiply(4)
        add_pair(3)
        down_far(2)
        add_pair(4)
        finish(0)
        finish(1)
        down_far(3)
        multiply(5)
        finish(2)
        add_pair(5)
        finish(3)
        settle("down", pz)
        multiply(6)
        finish(4)
        pl.loop(4, 6)(lambda c: own_partner("down", c).start())
        add_pair(6)
        settle("down", far)
        multiply(7)
        lend(5)
        add_pair(7)
        settle("pool", pz)
        spread_pool(pz)
        keep(5)
        lend(6)
        lend(7)
        pl.loop(6, 8)(lambda c: own_partner("down", c).start())
        pl.loop(0, 8)(lambda c: passing("down", mirror, c, partner).start())
        pl.loop(0, 8)(lambda c: passing("down", far, c, partner).start())
        extra_copy(far, pz, partner).start()
        keep(6)
        keep(7)
        final_all(0, other).wait_recv()

    def take(name, s, c):
        arrival(name, s, c).wait_recv()
        share(name, s, c).start()

    def collect():
        for copy in local:
            copy.wait()
        spread_pool(z)
        shards_in = (pz, far, mirror)
        for i, s in enumerate(shards_in):
            pl.loop(0, 8)(lambda m: take("gu", s, m))
            take("pool", s, 0)
            if i > 0:
                settle("pool", shards_in[i - 1])
                spread_pool(shards_in[i - 1])

        def hand_out(j):
            lend_copy(j, pz).wait_recv()
            lent_copy(j, 1).start()
            lent_copy(j, 0).start()

        def hand_on(j):
            lent_arrival(j).wait_recv()
            lent_copy(j, 2).start()

        pl.loop(0, 3)(lambda c: take("down", pz, c))
        settle("pool", mirror)
        spread_pool(mirror)
        take("down", pz, 3)
        for j in range(5):
            hand_out(j)
        pl.loop(4, 6)(lambda c: take("down", pz, c))
        for j in range(4):
            hand_on(j)
        hand_out(5)
        hand_on(4)
        hand_out(6)
        hand_out(7)
        hand_on(5)
        hand_on(6)
        take("down", pz, 6)
        hand_on(7)
        take("down", pz, 7)
        t_mate = t + 1 - 2 * core
        lent_all(0, t_mate).wait_recv()
        lent_all(2, lax.rem(t_mate + 2, n_tp)).wait_recv()

    pl.when(inner)(first_ffn)
    pl.when(outer)(collect)

    def when_outer(act):
        pl.when(outer)(act)

    def take_down(s, low, high):
        @pl.when(outer)
        def _():
            for c in range(low, high):
                take("down", s, c)

    norm_rows(res.at[0], gainm_ref)
    take_down(far, 0, 1)
    for off in range(1, n_tp):
        pool_all(off, lax.rem(t - off + n_tp, n_tp)).wait_recv()
    group_width = width // groups
    row_id = lax.broadcasted_iota(jnp.int32, (n_rows, n_rows), 0)
    col_id = lax.broadcasted_iota(jnp.int32, (n_rows, n_rows), 1)
    position = lax.broadcasted_iota(jnp.int32, (n_rows, 1), 0)
    own_seq = pl.ds(0, n_rows)
    for k, span in enumerate(pool_spans):
        low = row_id - span // 2
        band = jnp.where((col_id >= low) & (col_id < low + span), 1.0, 0.0).astype(jnp.bfloat16)
        first = jnp.maximum(position - span // 2, 0)
        last = jnp.minimum(position - span // 2 + span, n_rows)
        inverse = 1.0 / (last - first).astype(f32)
        cols = pl.ds(k * group_width, group_width)
        mean = jnp.dot(band, normed[own_seq, cols], preferred_element_type=f32) * inverse
        deviation = (mean - normed[own_seq, cols].astype(f32)).astype(jnp.bfloat16)
        mapped = jnp.dot(deviation, pool_full[k], preferred_element_type=f32) + bias_ref[pl.ds(k, 1), :]
        amix[:, cols] = (res[0, :, cols].astype(f32) + mapped * scale_ref[:, cols]).astype(jnp.bfloat16)
        if k % 2 == 1:
            take_down(far, 1 + k // 2, 2 + k // 2)

    norm_rows(amix, gain2_ref)

    @pl.when(outer)
    def _():
        for s in (pz, far, mirror):
            settle("gate", s)
            settle("up", s)
        take("down", far, 3)

    @pl.loop(0, f_loc // tile)
    def _(i):
        cols = pl.ds(pl.multiple_of(i * tile, tile), tile)
        gate_proj = jnp.dot(normed[own_seq, :], gu_full[0, :, cols], preferred_element_type=f32)
        up_proj = jnp.dot(normed[own_seq, :], gu_full[1, :, cols], preferred_element_type=f32)
        hidden[own_seq, cols] = activate(gate_proj, up_proj)

        @pl.when(outer & ((i == 1) | (i == 2) | (i == 4)))
        def _():
            take("down", far, 3 + i - i // 4)

    def spot(b):
        wide = b < n_blocks - 2
        j = b if wide else n_blocks - 2 + b % 2
        place = second_place(j)
        off, size = (0, block_cols) if wide else ((b - n_blocks + 2) // 2 * sub_cols, sub_cols)
        cols = pl.ds(pl.multiple_of(place[0] * d_loc + place[1] * block_cols + off, 128), size)
        return j, place, cols, pl.ds(off, size)

    def pair_copy(b):
        j, _, _, lanes = spot(b)
        return remote(part1.at[j, other, lanes], rbuf1.at[j, :, lanes], csend.at[1], crecv.at[1, b], mate)

    def x_copy(b):
        j, _, _, lanes = spot(b)
        return remote(xs1.at[j, :, lanes], xr1.at[j, :, lanes], xsend.at[1], xrecv.at[1, b], x_peer)

    def last_copy(b, rows):
        there = res.at[1, rows, spot(b)[2]]
        return remote(there, there, fsend.at[1], frecv.at[1 + b], mate)

    def multiply(b):
        j, (s, half), _, lanes = spot(b)
        product = jnp.dot(hidden[own_seq, :], down_full[s, half, :, lanes], preferred_element_type=f32)
        part1[j, :, lanes] = product.astype(jnp.bfloat16)
        pair_copy(b).start()

    early_rows = f_loc // 4 * 3 // 128 * 128

    def multiply_last(b):
        j, (s, half), _, lanes = spot(b)
        early, late = pl.ds(0, early_rows), pl.ds(early_rows, f_loc - early_rows)
        when_outer(lambda: settle_down(mirror, 1, f_loc // 4 * 3))
        held = acc.at[0, own_seq, pl.ds(0, sub_cols)]
        held[...] = jnp.dot(hidden[own_seq, early], down_full[s, half, early, lanes], preferred_element_type=f32)
        when_outer(lambda: extra_copy(mirror, z, partner).wait_recv())
        product = jnp.dot(hidden[own_seq, late], down_full[s, half, late, lanes], preferred_element_type=f32)
        part1[j, :, lanes] = (held[...] + product).astype(jnp.bfloat16)
        pair_copy(b).start()

    def add_pair(b):
        j, _, _, lanes = spot(b)
        pair_copy(b).wait_recv()
        xs1[j, :, lanes] = (part1[j, mine, lanes].astype(f32) + rbuf1[j, :, lanes].astype(f32)).astype(jnp.bfloat16)
        x_copy(b).start()

    def finish(b):
        j, _, cols, lanes = spot(b)
        x_copy(b).wait_recv()
        total = xs1[j, :, lanes].astype(f32) + xr1[j, :, lanes].astype(f32)
        res[1, mine, cols] = (amix[mine, cols].astype(f32) + 0.5 * total).astype(jnp.bfloat16)
        last_copy(b, mine).start()
        out_ref[mine, cols] = res[1, mine, cols]

    def emit(b):
        cols = spot(b)[2]
        last_copy(b, other).wait_recv()
        out_ref[other, cols] = res[1, other, cols]

    def drain_early():
        for off in range(1, n_tp):
            pool_all(off, t).wait_send()
        for name in kinds:
            sent(name, z, g, zsend.at[z], partner).wait_send()

        @pl.when(outer)
        def _():
            tok_copy.wait_send()
            for name in kinds:
                sent(name, z, 1 - g, ysend.at[z], partner).wait_send()
                for s in (pz, far, mirror):
                    if name != "down":
                        shared(name, s)
            shared("down", pz)
            for lane in range(3):
                lent_all(lane, t).wait_send()

        @pl.when(inner)
        def _():
            for off in range(1, n_tp):
                guest_copy(off, t).wait_send()
            for name in kinds:
                sent(name, z, g, zleft, inward).wait_send()
                sent(name, pz, g, zsend.at[pz], inward).wait_send()
                for s in (mirror, far):
                    shared(name, s)
                    if name != "down":
                        sent(name, s, g, zsend.at[s], partner).wait_send()
            remote(rbuf0, rbuf0, csend.at[0], crecv.at[0, 0], mate).wait_send()
            remote(xr0, xr0, xsend.at[0], xrecv.at[0, 0], x_peer).wait_send()
            remote(xg0, xg0, gsend.at[0], arecv.at[1], x_peer).wait_send()
            remote(lent, lent, asend.at[1], arecv.at[1], partner).wait_send()
            final_all(0, mine).wait_send()

    multiply(0)
    multiply(1)
    add_pair(0)
    multiply(2)
    add_pair(1)
    take_down(far, 7, 8)
    when_outer(lambda: settle("down", pz))
    multiply(3)
    add_pair(2)
    multiply(4)
    add_pair(3)
    take_down(mirror, 0, 1)
    add_pair(4)
    take_down(mirror, 1, 3)
    when_outer(lambda: settle("down", far))
    multiply(5)
    take_down(mirror, 3, 4)
    multiply(6)
    add_pair(5)
    finish(0)
    add_pair(6)
    take_down(mirror, 4, 5)
    drain_early()
    finish(1)
    emit(0)
    take_down(mirror, 5, 6)
    when_outer(lambda: settle_down(mirror, 0))
    multiply(7)
    finish(2)
    emit(1)
    take_down(mirror, 6, 7)
    add_pair(7)
    finish(3)
    emit(2)
    when_outer(lambda: arrival("down", mirror, 7).wait_recv())
    multiply(8)
    finish(4)
    emit(3)
    add_pair(8)
    multiply_last(9)
    finish(5)
    emit(4)
    add_pair(9)
    finish(6)
    emit(5)
    finish(7)
    emit(6)
    finish(8)
    emit(7)
    finish(9)
    emit(8)
    emit(9)

    @pl.when(outer)
    def _():
        shared("down", far)
        shared("down", mirror, f_loc // 4 * 3)

    @pl.when(inner)
    def _():
        for s in (mirror, far):
            sent("down", s, g, zsend.at[s], partner).wait_send()
        extra_copy(far, pz, partner).wait_send()

    remote(xr1, xr1, csend.at[1], crecv.at[1, 0], mate).wait_send()
    remote(xr1, xr1, xsend.at[1], xrecv.at[1, 0], x_peer).wait_send()
    final_all(1, mine).wait_send()


def fused_shards(
    n, n_tp, tokens, gate_weight, up_weight, down_weight, pool_weight, pool_bias, pool_scale,
    gain_first, gain_mix, gain_second,
):
    n_rows, width = tokens.shape
    d_loc, f_loc = gate_weight.shape
    pool_rows, groups, pool_cols = pool_weight.shape
    bf16, dma, vmem = jnp.bfloat16, pltpu.SemaphoreType.DMA, pltpu.VMEM
    anywhere = pl.BlockSpec(memory_space=pl.ANY)
    half, quarter, block, blocks = n_rows // 2, n_rows // n_tp, d_loc // 2, 2 * n
    return pl.pallas_call(
        functools.partial(fused_kernel, (n, n_tp)),
        out_shape=pltpu.VMEM((n_rows, width), bf16),
        in_specs=[anywhere] * 10,
        out_specs=pl.BlockSpec(memory_space=pltpu.VMEM),
        scratch_shapes=[
            vmem((2, n * d_loc, f_loc), bf16),
            vmem((n, 2, f_loc, block), bf16),
            vmem((groups, n * pool_rows, n_tp * pool_cols), bf16),
            vmem((2, 2 * n_rows, f_loc), jnp.float32),
            vmem((2 * n_rows, width), bf16),
            vmem((2 * n_rows, f_loc), bf16),
            vmem((n_rows, width), bf16),
            vmem((2, n_rows, width), bf16),
            vmem((n_rows, width), bf16),
            vmem((blocks, 2, 2, half, block), bf16),
            vmem((blocks, 2, half, block), bf16),
            vmem((blocks, 2, half, block), bf16),
            vmem((blocks, half, block), bf16),
            vmem((blocks, quarter, block), bf16),
            vmem((blocks, quarter, block), bf16),
            vmem((blocks, n_rows, block), bf16),
            vmem((blocks, half, block), bf16),
            vmem((blocks, half, block), bf16),
            vmem((blocks, half, block), bf16),
            vmem((n_rows, width), bf16),
            vmem((pool_rows, groups, pool_cols), bf16),
            vmem(pool_bias.shape, jnp.float32),
            vmem((1, width), jnp.float32),
            vmem((1, width), jnp.float32),
            vmem((1, width), jnp.float32),
            vmem((1, width), jnp.float32),
            dma((n, 4)), dma((3,)), dma((n - 1, 17)), dma((n, 4)), dma((n - 1, 6)),
            dma((n_tp - 1,)), dma((n_tp - 1,)), dma((11,)),
            dma((2,)), dma((1 + blocks,)), dma((6,)), dma((5,)),
            dma((2,)), dma((2, blocks + 2)), dma((2,)), dma((2, blocks + 2)), dma((1,)),
            dma((2,)), dma((3 + blocks,)),
        ],
        compiler_params=pltpu.CompilerParams(
            collective_id=0, has_side_effects=True, vmem_limit_bytes=60 * 1024 * 1024
        ),
    )(
        tokens, gate_weight, up_weight, down_weight, pool_weight, pool_bias, pool_scale.reshape(1, width),
        gain_first.reshape(1, width), gain_mix.reshape(1, width), gain_second.reshape(1, width),
    )


def layer(n_grp, n, n_tp, *args):
    n_rows, width = args[0].shape
    d_loc, f_loc = args[1].shape
    pool_rows, _, pool_cols = args[4].shape
    fits = n_grp == 2 and n_tp == 4 and n == 4 and n_rows % 64 == 0
    fits = fits and d_loc % 512 == 0 and f_loc % 1280 == 0 and pool_rows % 32 == 0 and pool_cols % 128 == 0
    return fused_shards(n, n_tp, *args) if fits else shards(*args)


def solution(mesh):
    return jax.shard_map(
        functools.partial(layer, mesh.shape["grp"], mesh.shape["fs"], mesh.shape["tp"]),
        mesh=mesh,
        in_specs=(
            P(("grp", "fs"), None),
            P("fs", "tp"),
            P("fs", "tp"),
            P("tp", "fs"),
            P("fs", None, "tp"),
            P(),
            P(),
            P(),
            P(),
            P(),
        ),
        out_specs=P(("grp", "fs"), None),
        check_vma=False,
    )
```
